256 devices in a mesh: sp: 64 (over z, y, core), tp: 4 (over x).
Axes of the slice: x: 4, y: 4, z: 8, core: 2. Of those that a mesh axis runs over, the one named last changes fastest.
Arguments:
- cotangent: bfloat16 [10240, 2048], P('sp'), may hold values from -16 to 16
- saved_input: bfloat16 [10240, 2048], P('sp'), may hold values from -200 to 200
- routes: int32 [10240, 2], P('sp'), may hold values from 0 to 63, all different within a row; in each aligned block of 160 rows (0 to 159, 160 to 319, ...) at most 10 rows name the same one
- route_weight: float32 [10240, 2], P('sp'), may hold values from 0.2 to 1.5
- gate_proj: bfloat16 [64, 2048, 1024], P('sp', None, 'tp'), may hold values from -0.125 to 0.125
- up_proj: bfloat16 [64, 2048, 1024], P('sp', None, 'tp'), may hold values from -0.125 to 0.125
- down_proj: bfloat16 [64, 1024, 2048], P('sp', 'tp'), may hold values from -0.1875 to 0.1875
- out_proj: bfloat16 [2048, 1024], P(None, 'tp'), may hold values from -0.1875 to 0.1875
- conv_input: bfloat16 [10240, 1024], P('sp', 'tp'), may hold values from -6 to 6
- gate_branch: bfloat16 [10240, 1024], P('sp', 'tp'), may hold values from -6 to 6
- conv_taps: bfloat16 [4, 1024], P(None, 'tp'), may hold values from -3 to 3
- recur_map: bfloat16 [2, 16, 64, 64], P(None, 'tp'), may hold values from -0.75 to 0.75
- input_map: bfloat16 [2, 16, 64, 64], P(None, 'tp'), may hold values from -0.75 to 0.75
- decay_param: float32 [2, 1024], P(None, 'tp'), may hold values from 4 to 30
- decay_shift: float32 [2, 10240, 1024], P(None, 'sp', 'tp'), may hold values from -2 to 0, as said below
Outputs:
- grad_gate_proj: float32 [64, 2048, 1024], P('sp', None, 'tp')
- grad_up_proj: float32 [64, 2048, 1024], P('sp', None, 'tp')
- grad_down_proj: float32 [64, 1024, 2048], P('sp', 'tp')
- grad_out_proj: float32 [2048, 1024], P('sp', 'tp')
- grad_conv_input: bfloat16 [10240, 1024], P('sp', 'tp')
- grad_gate_branch: bfloat16 [10240, 1024], P('sp', 'tp')
The draws below stay inside these ranges and needn't reach their ends.
Inputs may be any that keep to these rules, and one draw needn't show every extreme that they name: Each row names 2 different experts; among the rows of one device no expert is named by more than 10 rows, and in every draw some device routes exactly 10 rows to some expert. `decay_shift`: together with decay_param, -log_decay stays at or above softplus(-decay_param) for every channel and position.
All inputs are finite; a program needn't handle non-finite values.
Results may differ from the reference program's by a relative error of at most 0.013.
Values may be sent and summed in bfloat16 or wider, within the bound.
A program may use at most 128 MiB of HBM per device.

```python
import math
import jax
import jax.numpy as jnp
import numpy as np
from jax import lax

D = 2048
F = 1024
SCAN_CHANNELS = 1024
HW = 64
CONV_W = 4
TOP_K = 2
TOK_DEV = 160
EXPERTS = 64
STEP_COUNT = 10240
CAP = 10
N_SP = 64
N_TP = 4


DECAY_SCALE = 8.0


def decay_rates(key):
    base = jax.random.fold_in(key, 11)
    keys = jax.random.split(base, 3)
    share = 0.5
    fast = jax.random.uniform(keys[0], (2, SCAN_CHANNELS), jnp.float32) < share
    slow_rate = jnp.exp(jax.random.uniform(keys[1], (2, SCAN_CHANNELS), jnp.float32, math.log(0.005), math.log(0.05))) / STEP_COUNT
    fast_rate = jnp.exp(jax.random.uniform(keys[2], (2, SCAN_CHANNELS), jnp.float32, math.log(0.0025), math.log(0.008)))
    return jnp.where(fast, fast_rate, slow_rate)


def draw_decay_param(key, part):
    rate = decay_rates(key)
    return (-jnp.log(jnp.expm1(rate))).astype(jnp.float32)


def draw_decay_shift(key, part):
    rate = decay_rates(key)
    keys = jax.random.split(jax.random.fold_in(key, 12), 3)
    blocks = STEP_COUNT // TOK_DEV
    pace = jnp.exp(jax.random.uniform(keys[0], (2, blocks, SCAN_CHANNELS), jnp.float32, math.log(1.25), math.log(4.0)))
    pace_rows = jnp.repeat(pace, TOK_DEV, axis=1)
    filtered_signal = -DECAY_SCALE * 0.5 * rate[:, None, :] * (pace_rows - 1.0)
    expert_seats = jax.random.randint(keys[1], (2, 2, SCAN_CHANNELS), 0, STEP_COUNT)
    stack_level = jax.random.uniform(keys[2], (2, 2, SCAN_CHANNELS), jnp.float32, 0.2, 0.45)
    step_location = jnp.arange(STEP_COUNT, dtype=jnp.int32)[None, :, None]
    tally_clusters = jnp.zeros((2, STEP_COUNT, SCAN_CHANNELS), jnp.float32)
    for step_number in range(2):
        tally_clusters = tally_clusters + jnp.where(step_location == expert_seats[:, step_number][:, None, :], jnp.log1p(-stack_level[:, step_number])[:, None, :], 0.0)
    return (filtered_signal + tally_clusters).astype(jnp.float32)


def draw_saved_input(key, part):
    keys = jax.random.split(jax.random.fold_in(key, 13), 4)
    noise = jnp.clip(jax.random.normal(keys[0], (STEP_COUNT, D), jnp.float32), -4.0, 4.0)
    mixed = noise
    row_scale = jnp.exp(jax.random.uniform(keys[2], (STEP_COUNT, 1), jnp.float32, math.log(0.5), math.log(5.0)))
    column_scale = jnp.exp(jax.random.uniform(keys[3], (1, D), jnp.float32, math.log(0.3), math.log(3.0)))
    return (mixed * row_scale * column_scale).astype(jnp.bfloat16)


def with_spikes(values, rng, source, target, shards_of, factor):
    def block_of(dim):
        return (jnp.arange(values.shape[dim]) // (values.shape[dim] // shards_of)).reshape((-1,) + (1,) * (values.ndim - 1 - dim))

    near = jax.random.permutation(rng, shards_of)[block_of(target)]
    other_side = (block_of(target) + shards_of // 2) % shards_of
    return jnp.where((block_of(source) == near) | (block_of(source) == other_side), factor * values, values)


def block_scale(own_key, shape, cuts, least, largest):
    def one(axis_at, parts):
        draws = jax.random.uniform(jax.random.fold_in(jax.random.fold_in(own_key, 6), axis_at), (parts,), jnp.float32, least / len(cuts), largest / len(cuts))
        return jnp.repeat(jnp.exp(draws), shape[axis_at] // parts).reshape((-1,) + (1,) * (len(shape) - axis_at - 1))

    loudness = one(*cuts[0])
    for cut in cuts[1:]:
        loudness = loudness * one(*cut)
    return loudness


def shared_out(rng, own, number, rows, amount, top, most, lean):
    sequence = jax.random.permutation(rng, amount)
    crowded, ordinary = load_shares(amount, rows * top, most, lean, True), load_shares(amount, rows * top, most, lean, False)
    places = jnp.arange(amount)

    def named(lengths, rotation):
        used = int((lengths > 0).sum())
        fixed = max(1, used // 4)
        passed = fixed + (places - fixed + rotation * (used - fixed)) % max(1, amount - fixed)
        return jnp.zeros((amount,), jnp.int32).at[sequence[jnp.where(places < fixed, places, passed)]].set(jnp.asarray(lengths, jnp.int32))

    lengths = jnp.where(number % 4 == 0, named(crowded, number // 4), named(ordinary, number - number // 4 - 1))
    mixed = jax.random.permutation(jax.random.fold_in(own, 3), amount)
    source_of, receiver = mixed[0:amount // 2 * 2:2], mixed[1:amount // 2 * 2:2]
    margin = jnp.minimum(lengths[source_of] - 1, most - lengths[receiver]) // 2
    margin = jnp.where((source_of == sequence[0]) | (receiver == sequence[0]) | (lengths[receiver] == 0), 0, jnp.maximum(margin, 0))
    passed = jax.random.randint(jax.random.fold_in(own, 4), (amount // 2,), 0, 1 << 20) % (margin + 1)
    lengths = lengths.at[source_of].add(-passed).at[receiver].add(passed)
    items = jnp.searchsorted(jnp.cumsum(lengths), jnp.arange(rows * top), side="right").astype(jnp.int32)
    grid = items.reshape(top, rows).T
    grid = grid[jax.random.permutation(jax.random.fold_in(own, 1), rows)]
    rotation = jax.random.randint(jax.random.fold_in(own, 2), (rows, 1), 0, top)
    return jnp.take_along_axis(grid, (jnp.arange(top)[None, :] + rotation) % top, axis=1)


def load_shares(amount, total, bound, skew, full):
    loads = [(1 << 20) // math.isqrt(grade ** skew) + 1 for grade in range(1, amount + 1)]
    largest = bound if full else min(bound, max(-(-total // amount), total * loads[0] // sum(loads)))
    least = 1 if total - largest >= amount - 1 else 0
    given, spare = [largest] + [least] * (amount - 1), total - largest - least * (amount - 1)
    while spare > 0:
        free = [i for i in range(1, amount) if given[i] < largest] or [i for i in range(1, amount) if given[i] < bound]
        pool, left = sum([loads[i] for i in free]), spare
        for i in free:
            more = min(bound - given[i], max(1, left * loads[i] // pool), spare)
            given[i] = given[i] + more
            spare = spare - more
    return np.array(given)


def bell_draw(rng, shape, spread, reach, cuts=(), kind=jnp.bfloat16):
    result = spread * jax.random.normal(rng, shape, jnp.float32)
    if cuts:
        result = result * block_scale(rng, shape, cuts, -0.22, 0.18)
    return jnp.clip(result, -reach, reach).astype(kind)


def bell_draw_with(rng, shape, deviation, most, cuts, heavy, kind=jnp.bfloat16):
    result = deviation * jax.random.normal(rng, shape, jnp.float32)
    if cuts:
        result = result * block_scale(rng, shape, cuts, -0.22, 0.18)
    return jnp.clip(with_spikes(result, jax.random.fold_in(rng, 3), *heavy), -most, most).astype(kind)


def setup_inputs(seed: int = 0) -> dict:
    key_list = jax.random.split(jax.random.key(seed), 16)
    cotangent = bell_draw_with(key_list[0], (STEP_COUNT, D), 1.0, 16.0, ((0, 64),), (0, 1, 64, 4.0))
    saved_input = draw_saved_input(jax.random.fold_in(key_list[15], 71), 0)
    routes_keys = jax.random.split(jax.random.fold_in(key_list[2], 1), STEP_COUNT // TOK_DEV)
    routes_turns = jax.random.permutation(jax.random.fold_in(key_list[2], 3), STEP_COUNT // TOK_DEV)
    routes = jax.vmap(lambda own, number: shared_out(jax.random.fold_in(key_list[2], 2), own, number, TOK_DEV, EXPERTS, TOP_K, CAP, 1))(routes_keys, routes_turns).reshape((STEP_COUNT, TOP_K))
    route_weight = jnp.clip(0.2 + 1.3 * jax.random.uniform(key_list[3], (STEP_COUNT, TOP_K), jnp.float32) ** block_scale(key_list[3], (STEP_COUNT, TOP_K), ((0, 64),), -0.2, 0.2), 0.2, 1.5)
    gate_proj = bell_draw(key_list[4], (EXPERTS, D, F), D ** -0.5, 0.125, ((0, 64), (2, 4)))
    up_proj = bell_draw(key_list[5], (EXPERTS, D, F), D ** -0.5, 0.125, ((0, 64), (2, 4)))
    down_proj = bell_draw(key_list[6], (EXPERTS, F, D), F ** -0.5, 0.1875, ((0, 64), (1, 4)))
    out_proj = bell_draw(key_list[7], (D, SCAN_CHANNELS), SCAN_CHANNELS ** -0.5, 0.1875, ((1, 4),))
    conv_input = bell_draw(key_list[8], (STEP_COUNT, SCAN_CHANNELS), 1.0, 6.0, ((0, 64), (1, 4)))
    gate_branch = bell_draw(key_list[9], (STEP_COUNT, SCAN_CHANNELS), 1.0, 6.0, ((0, 64), (1, 4)))
    conv_taps = bell_draw(key_list[10], (CONV_W, SCAN_CHANNELS), 0.5, 3.0, ((1, 4),))
    recur_map = bell_draw(key_list[11], (2, SCAN_CHANNELS // HW, HW, HW), HW ** -0.5, 0.75, ((1, 4),))
    input_map = bell_draw(key_list[12], (2, SCAN_CHANNELS // HW, HW, HW), HW ** -0.5, 0.75, ((1, 4),))
    decay_param = draw_decay_param(jax.random.fold_in(key_list[15], 71), 0)
    decay_shift = draw_decay_shift(jax.random.fold_in(key_list[15], 71), 0)
    return {"cotangent": cotangent, "saved_input": saved_input, "routes": routes, "route_weight": route_weight, "gate_proj": gate_proj, "up_proj": up_proj, "down_proj": down_proj, "out_proj": out_proj, "conv_input": conv_input, "gate_branch": gate_branch, "conv_taps": conv_taps, "recur_map": recur_map, "input_map": input_map, "decay_param": decay_param, "decay_shift": decay_shift}


EPS = 1e-06
DECAY_SCALE = 8.0

def block_matrix(maps):
    heads = maps.shape[0]
    eye = jnp.eye(heads, dtype=jnp.float32)
    full = jnp.einsum('hij,hg->higj', maps.astype(jnp.float32), eye)
    return full.reshape(heads * maps.shape[1], heads * maps.shape[2])

def gate_terms(conv_out, recur_map, input_map, decay_param, decay_shift):
    recur = jax.nn.sigmoid(jnp.dot(conv_out, block_matrix(recur_map), precision=lax.Precision.HIGHEST))
    inputs = jax.nn.sigmoid(jnp.dot(conv_out, block_matrix(input_map), precision=lax.Precision.HIGHEST))
    log_decay = -DECAY_SCALE * recur * jax.nn.softplus(-decay_param)[None, :] + decay_shift
    decay = jnp.exp(log_decay)
    drive = jnp.sqrt(-jnp.expm1(2.0 * log_decay)) * (inputs * conv_out)
    return (decay, drive)

def link(earlier, later):
    return (earlier[0] * later[0], later[0] * earlier[1] + later[1])

def reference(cotangent, saved_input, routes, route_weight, gate_proj, up_proj, down_proj, out_proj, conv_input, gate_branch, conv_taps, recur_map, input_map, decay_param, decay_shift):
    inputs32 = saved_input.astype(jnp.float32)
    inv_rms = lax.rsqrt(lax.optimization_barrier(jnp.mean(inputs32 * inputs32, axis=1, keepdims=True)) + EPS)
    normed = inputs32 * inv_rms
    expert_input = normed.astype(jnp.bfloat16)
    scaled = (route_weight[:, :, None] * cotangent.astype(jnp.float32)[:, None, :]).astype(jnp.bfloat16)
    scaled = scaled.reshape(STEP_COUNT * TOP_K, D)
    flat_expert = routes.reshape(-1).astype(jnp.int32)
    order = jnp.argsort(flat_expert, stable=True).astype(jnp.int32)
    counts = lax.optimization_barrier(jnp.sum((flat_expert[:, None] == jnp.arange(EXPERTS, dtype=jnp.int32)[None, :]).astype(jnp.int32), axis=0)).astype(jnp.int32)
    starts = (jnp.cumsum(counts) - counts).astype(jnp.int32)
    most_rows = N_SP * CAP
    padded_order = jnp.concatenate([order, jnp.zeros((most_rows,), jnp.int32)])
    block = F // N_TP

    def one_expert(expert):
        picks = lax.dynamic_slice_in_dim(padded_order, starts[expert], most_rows)
        live = jnp.arange(most_rows, dtype=jnp.int32) < counts[expert]
        rows_input = jnp.where(live[:, None], expert_input[picks // TOP_K], 0.0).astype(jnp.bfloat16)
        rows_scaled = jnp.where(live[:, None], scaled[picks], 0.0).astype(jnp.bfloat16)
        w_gate = gate_proj[expert]
        w_up = up_proj[expert]
        w_down = down_proj[expert]
        gate_pre = jnp.dot(rows_input, w_gate, preferred_element_type=jnp.float32)
        up_pre = jnp.dot(rows_input, w_up, preferred_element_type=jnp.float32)
        gate_sig = jax.nn.sigmoid(gate_pre)
        gate_act = gate_pre * gate_sig
        hidden = (gate_act * up_pre).astype(jnp.bfloat16)
        hidden_grad = jnp.dot(rows_scaled, w_down.T, preferred_element_type=jnp.float32)
        gate_grad = (hidden_grad * up_pre * gate_sig * (1.0 + gate_pre * (1.0 - gate_sig))).astype(jnp.bfloat16)
        up_grad = (hidden_grad * gate_act).astype(jnp.bfloat16)
        grad_down = jnp.dot(hidden.T, rows_scaled, preferred_element_type=jnp.float32)
        grad_gate = jnp.dot(rows_input.T, gate_grad, preferred_element_type=jnp.float32)
        grad_up = jnp.dot(rows_input.T, up_grad, preferred_element_type=jnp.float32)
        pieces = jnp.zeros((most_rows, D), jnp.float32)
        for step_number in range(N_TP):
            low = step_number * block
            piece = jnp.dot(gate_grad[:, low:low + block], w_gate[:, low:low + block].T, preferred_element_type=jnp.float32)
            piece = piece + jnp.dot(up_grad[:, low:low + block], w_up[:, low:low + block].T, preferred_element_type=jnp.float32)
            rounded = lax.optimization_barrier(piece.astype(jnp.bfloat16))
            pieces = pieces + rounded.astype(jnp.float32)
        route_rows = pieces.astype(jnp.bfloat16)
        target = jnp.where(live, picks, STEP_COUNT * TOP_K).astype(jnp.int32)
        return (grad_gate, grad_up, grad_down, route_rows, target)
    grad_gate_proj, grad_up_proj, grad_down_proj, route_rows, targets = lax.map(one_expert, jnp.arange(EXPERTS, dtype=jnp.int32))
    assigned = jnp.zeros((STEP_COUNT * TOP_K + 1, D), jnp.bfloat16).at[targets.reshape(-1)].set(route_rows.reshape(-1, D))
    normed_grad = lax.optimization_barrier(jnp.sum(assigned[:STEP_COUNT * TOP_K].reshape(STEP_COUNT, TOP_K, D).astype(jnp.float32), axis=1))
    mixed_grad = cotangent.astype(jnp.float32) + inv_rms * (normed_grad - normed * lax.optimization_barrier(jnp.mean(normed_grad * normed, axis=1, keepdims=True)))
    mixed_grad_b = mixed_grad.astype(jnp.bfloat16)
    taps32 = conv_taps.astype(jnp.float32)

    def mixer(conv_in, branch):
        padded = jnp.pad(conv_in, ((2, 1), (0, 0)))
        conv_out = jnp.zeros((STEP_COUNT, SCAN_CHANNELS), jnp.float32)
        for offset in range(CONV_W):
            conv_out = conv_out + padded[offset:offset + STEP_COUNT] * taps32[offset]
        states = jnp.zeros((STEP_COUNT, SCAN_CHANNELS), jnp.float32)
        for direction in range(2):
            decay, drive = gate_terms(conv_out, recur_map[direction], input_map[direction], decay_param[direction], decay_shift[direction])
            states = states + lax.associative_scan(link, (decay, drive), axis=0, reverse=direction == 1)[1]
        return jax.nn.gelu(branch) * states
    value, pull = jax.vjp(mixer, conv_input.astype(jnp.float32), gate_branch.astype(jnp.float32))
    mixed_out = value.astype(jnp.bfloat16)
    grad_out_proj = lax.dot_general(mixed_grad_b, mixed_out, (((0,), (0,)), ((), ())), preferred_element_type=jnp.float32)
    out_grad = jnp.dot(mixed_grad_b, out_proj, preferred_element_type=jnp.float32)
    conv_grad, branch_grad = pull(out_grad)
    return (grad_gate_proj, grad_up_proj, grad_down_proj, grad_out_proj, conv_grad.astype(jnp.bfloat16), branch_grad.astype(jnp.bfloat16))
```

```python
import functools

import jax
import jax.numpy as jnp
from jax import lax
from jax.experimental import pallas as pl
from jax.experimental.pallas import tpu as pltpu
from jax.sharding import PartitionSpec as P

EPS = 1e-06
DECAY_SCALE = 8.0
MESH = pl.DeviceIdType.MESH
EDGE = 16
BF = jnp.bfloat16
F32 = jnp.float32
VM = pl.BlockSpec(memory_space=pltpu.VMEM)
DMA = pltpu.SemaphoreType.DMA


class Geometry:
    def __init__(self, n_sp, slots):
        self.n = n_sp
        self.nyc = 8 if n_sp == 64 else 2
        self.nz = n_sp // self.nyc
        self.ny = self.nyc // 2
        self.slots = slots
        self.row_a = self.nz * slots
        self.row_b = self.nyc * slots
        self.rows = n_sp * slots

    def place(self):
        sp = lax.axis_index("sp")
        return sp, lax.div(sp, self.nyc), lax.rem(sp, self.nyc), lax.axis_index("tp")


def nearest_first(n):
    order = []
    for k in range(1, n):
        for step in (k, n - k):
            if step not in order and 0 < step < n:
                order.append(step)
    return order


def send(src, dst, send_sem, recv_sem, device):
    copy = pltpu.make_async_remote_copy(
        src_ref=src,
        dst_ref=dst,
        send_sem=send_sem,
        recv_sem=recv_sem,
        device_id=device,
        device_id_type=MESH,
    )
    copy.start()
    return copy


def arrival(dst, send_sem, recv_sem, device):
    return pltpu.make_async_remote_copy(
        src_ref=dst,
        dst_ref=dst,
        send_sem=send_sem,
        recv_sem=recv_sem,
        device_id=device,
        device_id_type=MESH,
    )


def greet(devices):
    barrier = pltpu.get_barrier_semaphore()
    for device in devices:
        pl.semaphore_signal(barrier, inc=1, device_id=device, device_id_type=MESH)
    pl.semaphore_wait(barrier, len(devices))


def block(ref_dim, size):
    return pl.ds(pl.multiple_of(ref_dim * size, size), size)


def group_of(q, slots):
    return lax.shift_right_logical(q * (2048 // slots + 1), 11)


def shuffle_base(count, total, slots, others):
    q = lax.broadcasted_iota(jnp.int32, (count, total), 0)
    col = lax.broadcasted_iota(jnp.int32, (count, total), 1)
    return col - q - group_of(q, slots) * ((others - 1) * slots)


def picked_rows(base, target, slots, rows):
    chosen = jnp.where(base == target * slots, 1.0, 0.0).astype(BF)
    return jnp.dot(chosen, rows, preferred_element_type=F32).astype(BF)


def prep_kernel(geo, cot_ref, x_ref, routes_ref, weight_ref, s_ref, pt_ref):
    length, width = x_ref.shape
    fourth = width // 4
    padded = routes_ref.shape[1]
    x32 = x_ref[...].astype(F32)
    inv_rms = lax.rsqrt(jnp.mean(x32 * x32, axis=1, keepdims=True) + EPS)
    first = pl.multiple_of(lax.axis_index("tp") * fourth, fourth)
    own_x = (x_ref[:, pl.ds(first, fourth)].astype(F32) * inv_rms).astype(BF)
    own_cot = cot_ref[:, pl.ds(first, fourth)].astype(F32)
    filler = jnp.zeros((padded - 2 * length, fourth), BF)
    scaled = [(weight_ref[:, k : k + 1] * own_cot).astype(BF) for k in range(2)]
    all_scaled = jnp.concatenate(scaled + [filler], axis=0)
    all_x = jnp.concatenate([own_x, own_x, filler], axis=0)
    routes = routes_ref[...]
    named = lax.broadcasted_iota(jnp.int32, (geo.n, padded), 0) == routes
    named = jnp.where(named, 1.0, 0.0)
    before = lax.broadcasted_iota(jnp.int32, (padded, padded), 0) < lax.broadcasted_iota(
        jnp.int32, (padded, padded), 1
    )
    before = jnp.where(before, 1.0, 0.0).astype(BF)
    earlier = jnp.dot(named.astype(BF), before, preferred_element_type=F32)
    rank = jnp.sum(earlier * named, axis=0, keepdims=True).astype(jnp.int32)
    shift = geo.nyc.bit_length() - 1
    z = lax.shift_right_arithmetic(routes, shift)
    c = routes & (geo.nyc - 1)
    target = jnp.where(routes < 0, -1, (c * geo.nz + z) * geo.slots + rank)
    place = lax.broadcasted_iota(jnp.int32, (geo.rows, padded), 0) == target
    place = jnp.where(place, 1.0, 0.0)
    chosen = place.astype(BF)
    s_ref[:, :fourth] = jnp.dot(chosen, all_x, preferred_element_type=F32).astype(BF)
    s_ref[:, fourth:] = jnp.dot(chosen, all_scaled, preferred_element_type=F32).astype(BF)
    pt_ref[...] = place.T.astype(BF)


def dispatch_kernel(geo, s_ref, ci_ref, xin_ref, xsc_ref, halo_ref, got, mid, sa, ra, sb, rb, sc, rc, sh, rh):
    nz, nyc, slots, row_a, row_b = geo.nz, geo.nyc, geo.slots, geo.row_a, geo.row_b
    sp, z, c, j = geo.place()
    w = s_ref.shape[1] // 2
    hw = w // 2
    right, left = lax.rem(j + 1, 4), lax.rem(j + 3, 4)
    length = ci_ref.shape[0]
    full = (xin_ref, xsc_ref)
    after, ahead = lax.rem(sp + 1, geo.n), lax.rem(sp + geo.n - 1, geo.n)
    y_order, z_order = nearest_first(nyc), nearest_first(nz)

    def y_peer(k):
        return z * nyc + lax.rem(c + k, nyc)

    def z_at(k):
        return lax.rem(z + k, nz)

    def z_from(k):
        return lax.rem(z + nz - k, nz)

    greet(
        [(y_peer(k), j) for k in y_order]
        + [(z_at(k) * nyc + c, j) for k in z_order]
        + [(sp, right), (sp, left), (after, j), (ahead, j)]
    )
    sent = []
    for h in range(2):
        for k in y_order:
            sent.append(
                send(
                    s_ref.at[block(lax.rem(c + k, nyc), row_a), pl.ds(h * w, w)],
                    got.at[block(c, row_a), pl.ds(h * w, w)],
                    sa.at[h, k],
                    ra.at[h, k],
                    (y_peer(k), j),
                )
            )
    sent.append(
        send(ci_ref.at[pl.ds(length - EDGE, EDGE)], halo_ref.at[pl.ds(0, EDGE)], sh.at[0], rh.at[0], (after, j))
    )
    sent.append(send(ci_ref.at[pl.ds(0, EDGE)], halo_ref.at[pl.ds(EDGE, EDGE)], sh.at[1], rh.at[1], (ahead, j)))
    got[block(c, row_a), :] = s_ref[block(c, row_a), :]
    base = shuffle_base(row_b, geo.rows, slots, nz)

    def exchange_z(h):
        for k in y_order:
            source = lax.rem(c + nyc - k, nyc)
            arrival(
                got.at[block(source, row_a), pl.ds(h * w, w)], sa.at[h, k], ra.at[h, k], (y_peer(k), j)
            ).wait_recv()
        rows = got[:, h * w : (h + 1) * w]
        full[h][block(z, row_b), pl.ds(pl.multiple_of(j * w, w), w)] = picked_rows(base, z, slots, rows)

        def launch(k):
            sent.append(
                send(
                    mid.at[h, k],
                    full[h].at[block(z, row_b), pl.ds(pl.multiple_of(j * w, w), w)],
                    sb.at[h, k],
                    rb.at[h, k],
                    (z_at(k) * nyc + c, j),
                )
            )

        held = None
        for k in z_order:
            mid[h, k] = picked_rows(base, z_at(k), slots, rows)
            if held is not None:
                launch(held)
            held = k
        return lambda: launch(held)

    def part(h, k, column, size, offset=0):
        return full[h].at[block(z_from(k), row_b), pl.ds(pl.multiple_of(column * w + offset, hw), size)]

    def first_hop(h, k):
        if k:
            arrival(part(h, k, j, w), sb.at[h, k], rb.at[h, k], (z_at(k) * nyc + c, j)).wait_recv()
        mine = part(h, k, j, w)
        sent.append(send(mine, mine, sc.at[h, k, 0], rc.at[h, k, 0], (sp, right)))
        sent.append(send(mine, mine, sc.at[h, k, 1], rc.at[h, k, 1], (sp, left)))

    def second_hop(h, k):
        arrival(part(h, k, left, w), sc.at[h, k, 0], rc.at[h, k, 0], (sp, left)).wait_recv()
        low = part(h, k, left, hw)
        sent.append(send(low, low, sc.at[h, k, 2], rc.at[h, k, 2], (sp, right)))
        arrival(part(h, k, right, w), sc.at[h, k, 1], rc.at[h, k, 1], (sp, right)).wait_recv()
        high = part(h, k, right, hw, hw)
        sent.append(send(high, high, sc.at[h, k, 3], rc.at[h, k, 3], (sp, left)))

    lead = z_order[:2]
    rest0, rest1 = z_order[2:], list(z_order)
    later = [(0, k) for k in rest0[:2]] + [(1, k) for k in rest1[:2]]
    later += [(0, k) for k in rest0[2:]] + [(1, k) for k in rest1[2:]]
    plan = [(0, 0)] + [(0, k) for k in lead] + [(1, 0)] + later
    waiting, done = [], []
    for item in plan:
        if item[1] == 0:
            flush = exchange_z(item[0])
            first_hop(*item)
            flush()
        else:
            first_hop(*item)
        waiting.append(item)
        if len(waiting) > 2:
            done.append(waiting.pop(0))
            second_hop(*done[-1])
    for item in waiting:
        second_hop(*item)
    opposite = lax.rem(j + 2, 4)
    for h, k in plan:
        arrival(part(h, k, opposite, hw), sc.at[h, k, 2], rc.at[h, k, 2], (sp, left)).wait_recv()
        arrival(part(h, k, opposite, hw, hw), sc.at[h, k, 3], rc.at[h, k, 3], (sp, right)).wait_recv()
    for e in range(2):
        arrival(halo_ref.at[pl.ds(e * EDGE, EDGE)], sh.at[e], rh.at[e], (after, j)).wait_recv()
    for copy in sent:
        copy.wait_send()


def return_kernel(
    geo, p_ref, pt_ref, ng_ref, thru, direct, comb, fin, share, z_got, y_out, back, sx, rx, sz, rz, sy, ry, sg, rg
):
    nz, nyc, slots, row_a, row_b = geo.nz, geo.nyc, geo.slots, geo.row_a, geo.row_b
    sp, z, c, j = geo.place()
    w = p_ref.shape[1] // 4
    hw = w // 2
    length = ng_ref.shape[0]
    right, left, opposite = lax.rem(j + 1, 4), lax.rem(j + 3, 4), lax.rem(j + 2, 4)
    y_order, z_order = nearest_first(nyc), nearest_first(nz)
    plan = list(reversed(z_order)) + [0]

    def y_peer(k):
        return z * nyc + lax.rem(c + k, nyc)

    def z_at(k):
        return lax.rem(z + k, nz)

    greet(
        [(y_peer(k), j) for k in y_order]
        + [(z_at(k) * nyc + c, j) for k in z_order]
        + [(sp, right), (sp, left)]
    )
    sent = []

    def piece(k, column, offset):
        return p_ref.at[block(z_at(k), row_b), pl.ds(pl.multiple_of(column * w + offset, hw), hw)]

    def go(src, dst, sem, k, device):
        sent.append(send(src, dst, sx.at[k, sem], rx.at[k, sem], (sp, device)))

    def landed(dst, sem, k):
        arrival(dst, sx.at[k, sem], rx.at[k, sem], (sp, left)).wait_recv()

    for k in plan:
        go(piece(k, opposite, 0), thru.at[k, 0], 0, k, right)
        go(piece(k, opposite, hw), thru.at[k, 1], 1, k, left)
        go(piece(k, right, hw), direct.at[k, 0], 2, k, right)
        go(piece(k, left, 0), direct.at[k, 1], 3, k, left)

    def combine(k):
        landed(thru.at[k, 0], 0, k)
        comb[k, 0] = (piece(k, right, 0)[...].astype(F32) + thru[k, 0].astype(F32)).astype(BF)
        landed(thru.at[k, 1], 1, k)
        comb[k, 1] = (piece(k, left, hw)[...].astype(F32) + thru[k, 1].astype(F32)).astype(BF)

    def pass_on(k):
        go(comb.at[k, 0], fin.at[k, 0], 4, k, right)
        go(comb.at[k, 1], fin.at[k, 1], 5, k, left)

    def finish(k):
        for side in range(2):
            landed(direct.at[k, 1 - side], 3 - side, k)
            landed(fin.at[k, side], 4 + side, k)
            total = (
                piece(k, j, side * hw)[...].astype(F32)
                + fin[k, side].astype(F32)
                + direct[k, 1 - side].astype(F32)
            ).astype(BF)
            if k:
                share[k, :, side * hw : (side + 1) * hw] = total
            else:
                z_got[block(z, row_b), side * hw : (side + 1) * hw] = total

    def ship(k):
        if k:
            sent.append(
                send(share.at[k], z_got.at[block(z, row_b)], sz.at[k], rz.at[k], (z_at(k) * nyc + c, j))
            )

    stages = (combine, pass_on, finish, ship)
    lags = (0, 1, 2, 3)
    for step in range(len(plan) + lags[-1]):
        for stage, lag in zip(stages, lags):
            if 0 <= step - lag < len(plan):
                stage(plan[step - lag])
    base = shuffle_base(row_a, geo.rows, slots, nyc)
    for k in z_order:
        source = lax.rem(z + nz - k, nz)
        arrival(z_got.at[block(source, row_b)], sz.at[k], rz.at[k], (z_at(k) * nyc + c, j)).wait_recv()
    rows = z_got[...]

    def ship_y(k):
        sent.append(send(y_out.at[k], back.at[block(c, row_a)], sy.at[k], ry.at[k], (y_peer(k), j)))

    held = None
    for k in y_order:
        y_out[k] = picked_rows(base, lax.rem(c + k, nyc), slots, rows)
        if held is not None:
            ship_y(held)
        held = k
    back[block(c, row_a), :] = picked_rows(base, c, slots, rows)
    ship_y(held)
    for k in y_order:
        source = lax.rem(c + nyc - k, nyc)
        arrival(back.at[block(source, row_a)], sy.at[k], ry.at[k], (y_peer(k), j)).wait_recv()
    picked = jnp.dot(pt_ref[...], back[...], preferred_element_type=F32)
    ng_ref[:, pl.ds(pl.multiple_of(j * w, w), w)] = (picked[:length] + picked[length : 2 * length]).astype(BF)

    def columns(column, size, offset=0):
        return ng_ref.at[:, pl.ds(pl.multiple_of(column * w + offset, hw), size)]

    mine = columns(j, w)
    sent.append(send(mine, mine, sg.at[0], rg.at[0], (sp, right)))
    sent.append(send(mine, mine, sg.at[1], rg.at[1], (sp, left)))
    arrival(columns(left, w), sg.at[0], rg.at[0], (sp, left)).wait_recv()
    sent.append(send(columns(left, hw), columns(left, hw), sg.at[2], rg.at[2], (sp, right)))
    arrival(columns(right, w), sg.at[1], rg.at[1], (sp, right)).wait_recv()
    sent.append(send(columns(right, hw, hw), columns(right, hw, hw), sg.at[3], rg.at[3], (sp, left)))
    arrival(columns(opposite, hw), sg.at[2], rg.at[2], (sp, left)).wait_recv()
    arrival(columns(opposite, hw, hw), sg.at[3], rg.at[3], (sp, right)).wait_recv()
    for copy in sent:
        copy.wait_send()


def minus_expm1(x):
    near = 1.0 + x * (1.0 / 7.0)
    for n in (6.0, 5.0, 4.0, 3.0, 2.0):
        near = 1.0 + x * (1.0 / n) * near
    return jnp.where(x > -0.25, -x * near, 1.0 - jnp.exp(x))


def split_dot(value, matrix, dims):
    high = value.astype(BF)
    low = (value - high.astype(F32)).astype(BF)
    return lax.dot_general(high, matrix, (dims, ((), ())), preferred_element_type=F32) + lax.dot_general(
        low, matrix, (dims, ((), ())), preferred_element_type=F32
    )


def scan_rows(coef, drive, reverse):
    length = coef.shape[0]
    row = lax.broadcasted_iota(jnp.int32, coef.shape, 0)
    step = 1
    while step < length:
        if reverse:
            shift, inside = length - step, row < length - step
        else:
            shift, inside = step, row >= step
        near = jnp.where(inside, pltpu.roll(drive, shift, 0), 0.0)
        drive = coef * near + drive
        coef = coef * jnp.where(inside, pltpu.roll(coef, shift, 0), 1.0)
        step *= 2
    return coef, drive


GELU_C = 0.7978845608028654


def gelu_parts(x):
    inner = GELU_C * (x + 0.044715 * (x * x * x))
    t = jnp.tanh(inner)
    value = 0.5 * x * (1.0 + t)
    slope = 0.5 * (1.0 + t) + 0.5 * x * (1.0 - t * t) * (GELU_C * (1.0 + 3.0 * 0.044715 * (x * x)))
    return value, slope


SAVED = 18


def first_kernel(
    geo, ng_ref, cot_ref, x_ref, op_ref, ci_ref, halo_ref, gb_ref, taps_ref, maps_ref, rate_ref, shift_ref,
    mgb_ref, car_ref, sv_ref, big,
):
    length = ci_ref.shape[0]
    sp = lax.axis_index("sp")
    x32 = x_ref[...].astype(F32)
    inv_rms = lax.rsqrt(jnp.mean(x32 * x32, axis=1, keepdims=True) + EPS)
    normed = x32 * inv_rms
    ng = ng_ref[...].astype(F32)
    mean = jnp.mean(ng * normed, axis=1, keepdims=True)
    mgb = (cot_ref[...].astype(F32) + inv_rms * (ng - normed * mean)).astype(BF)
    mgb_ref[...] = mgb
    out_grad = jnp.dot(mgb, op_ref[...], preferred_element_type=F32)
    value, _ = gelu_parts(gb_ref[...].astype(F32))
    carried = out_grad * value
    has_low = jnp.where(sp > 0, 1.0, 0.0)
    has_high = jnp.where(sp < geo.n - 1, 1.0, 0.0)
    big[0:EDGE] = halo_ref[0:EDGE].astype(F32) * has_low
    big[EDGE : EDGE + length] = ci_ref[...].astype(F32)
    big[EDGE + length :] = halo_ref[EDGE:].astype(F32) * has_high
    conv = jnp.zeros(ci_ref.shape, F32)
    for o in range(4):
        conv = conv + big[EDGE - 2 + o : EDGE - 2 + o + length] * taps_ref[o : o + 1, :]
    sv_ref[0] = out_grad
    sv_ref[1] = carried
    coefs, drives = [], []
    for d in range(2):
        recur = jax.nn.sigmoid(split_dot(conv, maps_ref[2 * d], ((1,), (0,))))
        inputs = jax.nn.sigmoid(split_dot(conv, maps_ref[2 * d + 1], ((1,), (0,))))
        log_decay = -DECAY_SCALE * recur * rate_ref[d : d + 1, :] + shift_ref[d]
        coef = jnp.exp(log_decay)
        root = jnp.sqrt(minus_expm1(2.0 * log_decay))
        sv_ref[2 + 4 * d] = recur
        sv_ref[3 + 4 * d] = inputs
        sv_ref[4 + 4 * d] = coef
        sv_ref[5 + 4 * d] = root
        coefs.append(coef)
        drives.append(root * (inputs * conv))
    cum_f, state_f = scan_rows(coefs[0], drives[0], False)
    sv_ref[10] = cum_f
    sv_ref[11] = state_f
    cum_b, state_b = scan_rows(coefs[1], drives[1], True)
    sv_ref[12] = cum_b
    sv_ref[13] = state_b
    cum_bf, after_b = scan_rows(coefs[1], coefs[1] * carried, False)
    sv_ref[14] = cum_bf
    sv_ref[15] = after_b
    cum_fr, after_f = scan_rows(coefs[0], coefs[0] * carried, True)
    sv_ref[16] = cum_fr
    sv_ref[17] = after_f
    last = length - 1
    car_ref[0:1, :] = cum_f[last:]
    car_ref[1:2, :] = cum_bf[last:]
    car_ref[2:3, :] = cum_b[0:1]
    car_ref[3:4, :] = cum_fr[0:1]
    car_ref[4:5, :] = state_f[last:]
    car_ref[5:6, :] = after_b[last:]
    car_ref[6:7, :] = state_b[0:1]
    car_ref[7:8, :] = after_f[0:1]


def carry_kernel(geo, car_ref, out_ref, near, far, total, s1, r1, s2, r2):
    nz, nyc = geo.nz, geo.nyc
    sp, z, c, j = geo.place()
    y_order, z_order = nearest_first(nyc), nearest_first(nz)

    def y_peer(k):
        return z * nyc + lax.rem(c + k, nyc)

    def z_peer(k):
        return lax.rem(z + k, nz) * nyc + c

    greet([(y_peer(k), j) for k in y_order] + [(z_peer(k), j) for k in z_order])
    sent = [send(car_ref, near.at[c], s1.at[k], r1.at[k], (y_peer(k), j)) for k in y_order]
    near[c] = car_ref[...]
    for k in y_order:
        arrival(near.at[lax.rem(c + nyc - k, nyc)], s1.at[k], r1.at[k], (y_peer(k), j)).wait_recv()

    def combined(ref, count, place):
        shape = (2, car_ref.shape[1])
        ones, zeros = jnp.ones(shape, F32), jnp.zeros(shape, F32)
        results = []
        for side in range(2):
            a, b, ta, tb = ones, zeros, ones, zeros
            for i in range(count):
                at = i if side == 0 else count - 1 - i
                na, nb = ref[at, 2 * side : 2 * side + 2], ref[at, 4 + 2 * side : 6 + 2 * side]
                ta, tb = ta * na, na * tb + nb
                inside = (at < place) if side == 0 else (at > place)
                ma, mb = jnp.where(inside, na, 1.0), jnp.where(inside, nb, 0.0)
                a, b = a * ma, ma * b + mb
            results.append((a, b, ta, tb))
        return results

    first = combined(near, nyc, c)
    for side in range(2):
        total[2 * side : 2 * side + 2] = first[side][2]
        total[4 + 2 * side : 6 + 2 * side] = first[side][3]
    far[z] = total[...]
    sent += [send(total, far.at[z], s2.at[k], r2.at[k], (z_peer(k), j)) for k in z_order]
    for k in z_order:
        arrival(far.at[lax.rem(z + nz - k, nz)], s2.at[k], r2.at[k], (z_peer(k), j)).wait_recv()
    second = combined(far, nz, z)
    out_ref[...] = jnp.zeros_like(out_ref)
    for side in range(2):
        a, b = first[side][:2]
        out_ref[2 * side : 2 * side + 2] = a * second[side][1] + b
    for copy in sent:
        copy.wait_send()


def second_kernel(
    geo, mgb_ref, carry_ref, sv_ref, ci_ref, halo_ref, gb_ref, taps_ref, maps_ref, rate_ref,
    go_ref, cg_ref, cgb_ref, bg_ref, big,
):
    length = ci_ref.shape[0]
    sp = lax.axis_index("sp")
    row = lax.broadcasted_iota(jnp.int32, ci_ref.shape, 0)
    low_f, low_b = carry_ref[0:1], carry_ref[1:2]
    up_b, up_f = carry_ref[2:3], carry_ref[3:4]

    def from_before(value, carry):
        return jnp.where(row == 0, carry, pltpu.roll(value, 1, 0))

    def from_after(value, carry):
        return jnp.where(row == length - 1, carry, pltpu.roll(value, length - 1, 0))

    state_f = sv_ref[11] + sv_ref[10] * low_f
    state_b = sv_ref[13] + sv_ref[12] * up_b
    states = state_f + state_b
    value, slope = gelu_parts(gb_ref[...].astype(F32))
    bg_ref[...] = (sv_ref[0] * states * slope).astype(BF)
    mixed_out = (value * states).astype(BF)
    go = lax.dot_general(mgb_ref[...], mixed_out, (((0,), (0,)), ((), ())), preferred_element_type=F32)
    go_ref[...] = go.astype(BF)
    carried = sv_ref[1]
    after_b = sv_ref[15] + sv_ref[14] * low_b
    after_f = sv_ref[17] + sv_ref[16] * up_f
    adjoints = (carried + from_after(after_f, up_f), carried + from_before(after_b, low_b))
    others = (from_before(state_f, low_f), from_after(state_b, up_b))
    has_low = jnp.where(sp > 0, 1.0, 0.0)
    has_high = jnp.where(sp < geo.n - 1, 1.0, 0.0)
    big[0:EDGE] = halo_ref[0:EDGE].astype(F32) * has_low
    big[EDGE : EDGE + length] = ci_ref[...].astype(F32)
    big[EDGE + length :] = halo_ref[EDGE:].astype(F32) * has_high
    conv = jnp.zeros(ci_ref.shape, F32)
    for o in range(4):
        conv = conv + big[EDGE - 2 + o : EDGE - 2 + o + length] * taps_ref[o : o + 1, :]
    conv_grad = jnp.zeros(ci_ref.shape, F32)
    for d in range(2):
        recur, inputs = sv_ref[2 + 4 * d], sv_ref[3 + 4 * d]
        coef, root = sv_ref[4 + 4 * d], sv_ref[5 + 4 * d]
        adjoint = adjoints[d]
        log_grad = adjoint * others[d] * coef - adjoint * (inputs * conv) * (coef * coef) / root
        recur_grad = log_grad * (-DECAY_SCALE * rate_ref[d : d + 1, :]) * recur * (1.0 - recur)
        input_grad = adjoint * root * conv * inputs * (1.0 - inputs)
        conv_grad = conv_grad + adjoint * root * inputs
        conv_grad = conv_grad + split_dot(recur_grad, maps_ref[2 * d], ((1,), (1,)))
        conv_grad = conv_grad + split_dot(input_grad, maps_ref[2 * d + 1], ((1,), (1,)))
    cg_ref[...] = conv_grad
    cgb_ref[...] = conv_grad.astype(BF)


def last_kernel(
    geo, go_ref, cg_ref, cgb_ref, taps_ref, out_ref, ig_ref, half, quarter, r1, r2, r3, halo, big,
    s1, q1, s2, q2, s3, q3, sh, rh,
):
    nz, ny, nyc = geo.nz, geo.ny, geo.nyc
    sp, z, c, j = geo.place()
    y, core = lax.div(c, 2), lax.rem(c, 2)
    length = cg_ref.shape[0]
    after, ahead = lax.rem(sp + 1, geo.n), lax.rem(sp + geo.n - 1, geo.n)
    y_order, z_order = nearest_first(ny), nearest_first(nz)

    def y_peer(k):
        return z * nyc + lax.rem(y + k, ny) * 2 + core

    def z_peer(k):
        return lax.rem(z + k, nz) * nyc + c

    partner = z * nyc + y * 2 + (1 - core)
    greet(
        [(partner, j), (after, j), (ahead, j)]
        + [(y_peer(k), j) for k in y_order]
        + [(z_peer(k), j) for k in z_order]
    )
    sent = [send(go_ref.at[:, :, 1 - core], r1, s1, q1, (partner, j))]
    sent.append(send(cgb_ref.at[pl.ds(length - EDGE, EDGE)], halo.at[pl.ds(0, EDGE)], sh.at[0], rh.at[0], (after, j)))
    sent.append(send(cgb_ref.at[pl.ds(0, EDGE)], halo.at[pl.ds(EDGE, EDGE)], sh.at[1], rh.at[1], (ahead, j)))
    arrival(r1, s1, q1, (partner, j)).wait_recv()
    for k in y_order + [0]:
        at = lax.rem(y + k, ny)
        half[k] = (go_ref[:, at, core].astype(F32) + r1[:, at].astype(F32)).astype(BF)
    for k in y_order:
        sent.append(send(half.at[k], r2.at[k], s2.at[k], q2.at[k], (y_peer(k), j)))
    for e in range(2):
        arrival(halo.at[pl.ds(e * EDGE, EDGE)], sh.at[e], rh.at[e], (after, j)).wait_recv()
    has_low = jnp.where(sp > 0, 1.0, 0.0)
    has_high = jnp.where(sp < geo.n - 1, 1.0, 0.0)
    big[0:EDGE] = halo[0:EDGE].astype(F32) * has_low
    big[EDGE : EDGE + length] = cg_ref[...]
    big[EDGE + length :] = halo[EDGE:].astype(F32) * has_high
    grad = jnp.zeros(cg_ref.shape, F32)
    for o in range(4):
        grad = grad + big[EDGE + 2 - o : EDGE + 2 - o + length] * taps_ref[o : o + 1, :]
    ig_ref[...] = grad.astype(BF)
    for k in y_order:
        arrival(r2.at[k], s2.at[k], q2.at[k], (y_peer(k), j)).wait_recv()
    total = half[0].astype(F32)
    for k in y_order:
        total = total + r2[k].astype(F32)
    quarter[...] = total.astype(BF)
    for k in z_order:
        sent.append(
            send(quarter.at[lax.rem(z + k, nz)], r3.at[k], s3.at[k], q3.at[k], (z_peer(k), j))
        )
    result = quarter[z].astype(F32)
    for k in z_order:
        arrival(r3.at[k], s3.at[k], q3.at[k], (z_peer(k), j)).wait_recv()
        result = result + r3[k].astype(F32)
    out_ref[...] = result
    for copy in sent:
        copy.wait_send()


def local(body, geo, inputs, outs, scratch=()):
    return pl.pallas_call(
        functools.partial(body, geo),
        out_shape=outs,
        in_specs=[VM] * inputs,
        out_specs=jax.tree.map(lambda _: VM, outs),
        scratch_shapes=list(scratch),
        compiler_params=pltpu.CompilerParams(vmem_limit_bytes=60 * 2**20),
    )


def remote(body, geo, number, inputs, outs, scratch):
    return pl.pallas_call(
        functools.partial(body, geo),
        out_shape=outs,
        in_specs=[VM] * inputs,
        out_specs=jax.tree.map(lambda _: VM, outs),
        scratch_shapes=list(scratch),
        compiler_params=pltpu.CompilerParams(
            collective_id=number, has_side_effects=True, vmem_limit_bytes=60 * 2**20
        ),
    )


def block_matrices(maps):
    heads = maps.shape[1]
    eye = jnp.eye(heads, dtype=maps.dtype)
    full = maps[:, :, :, None, :] * eye[None, :, None, :, None]
    return full.reshape(maps.shape[0], heads * maps.shape[2], heads * maps.shape[3])


def shards(
    cotangent,
    saved_input,
    routes,
    route_weight,
    gate_proj,
    up_proj,
    down_proj,
    out_proj,
    conv_input,
    gate_branch,
    conv_taps,
    recur_map,
    input_map,
    decay_param,
    decay_shift,
):
    length, width = cotangent.shape
    n_sp = lax.axis_size("sp")
    geo = Geometry(n_sp, 4 * length // n_sp)
    nz, ny, nyc, rows = geo.nz, geo.ny, geo.nyc, geo.rows
    w = width // 4
    channels = conv_input.shape[1]
    shape = jax.ShapeDtypeStruct
    padded = -(-2 * length // 128) * 128
    flat_routes = jnp.pad(routes.T.reshape(1, 2 * length), ((0, 0), (0, padded - 2 * length)), constant_values=-1)
    slots, places = local(prep_kernel, geo, 4, (shape((rows, 2 * w), BF), shape((padded, rows), BF)))(
        cotangent, saved_input, flat_routes, route_weight
    )
    rows_input, rows_scaled, halo = remote(
        dispatch_kernel,
        geo,
        1,
        2,
        (shape((rows, width), BF), shape((rows, width), BF), shape((2 * EDGE, channels), BF)),
        [
            pltpu.VMEM((rows, 2 * w), BF),
            pltpu.VMEM((2, nz, geo.row_b, w), BF),
            DMA((2, nyc)),
            DMA((2, nyc)),
            DMA((2, nz)),
            DMA((2, nz)),
            DMA((2, nz, 4)),
            DMA((2, nz, 4)),
            DMA((2,)),
            DMA((2,)),
        ],
    )(slots, conv_input)
    w_gate, w_up, w_down = gate_proj[0], up_proj[0], down_proj[0]
    gate_pre = jnp.dot(rows_input, w_gate, preferred_element_type=F32)
    up_pre = jnp.dot(rows_input, w_up, preferred_element_type=F32)
    gate_sig = jax.nn.sigmoid(gate_pre)
    gate_act = gate_pre * gate_sig
    hidden = (gate_act * up_pre).astype(BF)
    hidden_grad = lax.dot_general(rows_scaled, w_down, (((1,), (1,)), ((), ())), preferred_element_type=F32)
    gate_grad = (hidden_grad * up_pre * gate_sig * (1.0 + gate_pre * (1.0 - gate_sig))).astype(BF)
    up_grad = (hidden_grad * gate_act).astype(BF)
    over_rows = (((0,), (0,)), ((), ()))
    grad_down = lax.dot_general(hidden, rows_scaled, over_rows, preferred_element_type=F32)
    grad_gate = lax.dot_general(rows_input, gate_grad, over_rows, preferred_element_type=F32)
    grad_up = lax.dot_general(rows_input, up_grad, over_rows, preferred_element_type=F32)
    transposed = (((1,), (1,)), ((), ()))
    partial_rows = lax.dot_general(gate_grad, w_gate, transposed, preferred_element_type=F32)
    partial_rows = partial_rows + lax.dot_general(up_grad, w_up, transposed, preferred_element_type=F32)
    half = (nz, 2, geo.row_b, w // 2)
    normed_grad = remote(
        return_kernel,
        geo,
        2,
        2,
        shape((length, width), BF),
        [pltpu.VMEM(half, BF)] * 4
        + [
            pltpu.VMEM((nz, geo.row_b, w), BF),
            pltpu.VMEM((rows, w), BF),
            pltpu.VMEM((nyc, geo.row_a, w), BF),
            pltpu.VMEM((rows, w), BF),
            DMA((nz, 6)),
            DMA((nz, 6)),
            DMA((nz,)),
            DMA((nz,)),
            DMA((nyc,)),
            DMA((nyc,)),
            DMA((4,)),
            DMA((4,)),
        ],
    )(partial_rows.astype(BF), places)
    taps32 = conv_taps.astype(F32)
    maps = block_matrices(jnp.stack([recur_map[0], input_map[0], recur_map[1], input_map[1]]))
    rate = jax.nn.softplus(-decay_param)
    own = (length, channels)
    big = pltpu.VMEM((length + 2 * EDGE, channels), F32)
    mixed_grad_b, carries, saved = local(
        first_kernel,
        geo,
        11,
        (shape((length, width), BF), shape((8, channels), F32), shape((SAVED, *own), F32)),
        [big],
    )(
        normed_grad, cotangent, saved_input, out_proj, conv_input, halo, gate_branch, taps32, maps, rate, decay_shift
    )
    entering = remote(
        carry_kernel,
        geo,
        3,
        1,
        shape((8, channels), F32),
        [
            pltpu.VMEM((nyc, 8, channels), F32),
            pltpu.VMEM((nz, 8, channels), F32),
            pltpu.VMEM((8, channels), F32),
            DMA((nyc,)),
            DMA((nyc,)),
            DMA((nz,)),
            DMA((nz,)),
        ],
    )(carries)
    grad_rows, conv_grad, conv_grad_b, branch_grad = local(
        second_kernel,
        geo,
        9,
        (shape((width, channels), BF), shape(own, F32), shape(own, BF), shape(own, BF)),
        [big],
    )(mixed_grad_b, entering, saved, conv_input, halo, gate_branch, taps32, maps, rate)
    part = width // n_sp
    grad_out, input_grad = remote(
        last_kernel,
        geo,
        4,
        4,
        (shape((part, channels), F32), shape(own, BF)),
        [
            pltpu.VMEM((ny, nz, part, channels), BF),
            pltpu.VMEM((nz, part, channels), BF),
            pltpu.VMEM((nz, ny, part, channels), BF),
            pltpu.VMEM((ny, nz, part, channels), BF),
            pltpu.VMEM((nz, part, channels), BF),
            pltpu.VMEM((2 * EDGE, channels), BF),
            big,
            DMA,
            DMA,
            DMA((ny,)),
            DMA((ny,)),
            DMA((nz,)),
            DMA((nz,)),
            DMA((2,)),
            DMA((2,)),
        ],
    )(grad_rows.reshape(nz, ny, 2, part, channels), conv_grad, conv_grad_b, taps32)
    return (grad_gate[None], grad_up[None], grad_down[None], grad_out, input_grad, branch_grad)


def solution(mesh):
    in_specs = (
        P("sp", None),
        P("sp", None),
        P("sp", None),
        P("sp", None),
        P("sp", None, "tp"),
        P("sp", None, "tp"),
        P("sp", "tp", None),
        P(None, "tp"),
        P("sp", "tp"),
        P("sp", "tp"),
        P(None, "tp"),
        P(None, "tp", None, None),
        P(None, "tp", None, None),
        P(None, "tp"),
        P(None, "sp", "tp"),
    )
    out_specs = (
        P("sp", None, "tp"),
        P("sp", None, "tp"),
        P("sp", "tp", None),
        P("sp", "tp"),
        P("sp", "tp"),
        P("sp", "tp"),
    )
    return jax.shard_map(shards, mesh=mesh, in_specs=in_specs, out_specs=out_specs, check_vma=False)
```

```python
import functools

import jax
import jax.numpy as jnp
from jax import lax
from jax.experimental import pallas as pl
from jax.experimental.pallas import tpu as pltpu
from jax.sharding import PartitionSpec as P

EPS = 1e-06
DECAY_SCALE = 8.0
MESH = pl.DeviceIdType.MESH
EDGE = 16
BF = jnp.bfloat16
F32 = jnp.float32
VM = pl.BlockSpec(memory_space=pltpu.VMEM)
DMA = pltpu.SemaphoreType.DMA


class Geometry:
    def __init__(self, n_sp, slots):
        self.n = n_sp
        self.nyc = 8 if n_sp == 64 else 2
        self.nz = n_sp // self.nyc
        self.ny = self.nyc // 2
        self.slots = slots
        self.row_a = self.nz * slots
        self.row_b = self.nyc * slots
        self.rows = n_sp * slots

    def place(self):
        sp = lax.axis_index("sp")
        return sp, lax.div(sp, self.nyc), lax.rem(sp, self.nyc), lax.axis_index("tp")


def nearest_first(n):
    order = []
    for k in range(1, n):
        for step in (k, n - k):
            if step not in order and 0 < step < n:
                order.append(step)
    return order


def send(src, dst, send_sem, recv_sem, device):
    copy = pltpu.make_async_remote_copy(
        src_ref=src,
        dst_ref=dst,
        send_sem=send_sem,
        recv_sem=recv_sem,
        device_id=device,
        device_id_type=MESH,
    )
    copy.start()
    return copy


def arrival(dst, send_sem, recv_sem, device):
    return pltpu.make_async_remote_copy(
        src_ref=dst,
        dst_ref=dst,
        send_sem=send_sem,
        recv_sem=recv_sem,
        device_id=device,
        device_id_type=MESH,
    )


def greet(devices):
    barrier = pltpu.get_barrier_semaphore()
    for device in devices:
        pl.semaphore_signal(barrier, inc=1, device_id=device, device_id_type=MESH)
    pl.semaphore_wait(barrier, len(devices))


def block(ref_dim, size):
    return pl.ds(pl.multiple_of(ref_dim * size, size), size)


def group_of(q, slots):
    return lax.shift_right_logical(q * (2048 // slots + 1), 11)


def shuffle_base(count, total, slots, others):
    q = lax.broadcasted_iota(jnp.int32, (count, total), 0)
    col = lax.broadcasted_iota(jnp.int32, (count, total), 1)
    return col - q - group_of(q, slots) * ((others - 1) * slots)


def picked_rows(base, target, slots, rows):
    chosen = jnp.where(base == target * slots, 1.0, 0.0).astype(BF)
    return jnp.dot(chosen, rows, preferred_element_type=F32).astype(BF)


def prep_kernel(geo, cot_ref, x_ref, routes_ref, weight_ref, s_ref, pt_ref):
    length, width = x_ref.shape
    fourth = width // 4
    padded = routes_ref.shape[1]
    x32 = x_ref[...].astype(F32)
    inv_rms = lax.rsqrt(jnp.mean(x32 * x32, axis=1, keepdims=True) + EPS)
    first = pl.multiple_of(lax.axis_index("tp") * fourth, fourth)
    own_x = (x_ref[:, pl.ds(first, fourth)].astype(F32) * inv_rms).astype(BF)
    own_cot = cot_ref[:, pl.ds(first, fourth)].astype(F32)
    filler = jnp.zeros((padded - 2 * length, fourth), BF)
    scaled = [(weight_ref[:, k : k + 1] * own_cot).astype(BF) for k in range(2)]
    all_scaled = jnp.concatenate(scaled + [filler], axis=0)
    all_x = jnp.concatenate([own_x, own_x, filler], axis=0)
    routes = routes_ref[...]
    named = lax.broadcasted_iota(jnp.int32, (geo.n, padded), 0) == routes
    named = jnp.where(named, 1.0, 0.0)
    before = lax.broadcasted_iota(jnp.int32, (padded, padded), 0) < lax.broadcasted_iota(
        jnp.int32, (padded, padded), 1
    )
    before = jnp.where(before, 1.0, 0.0).astype(BF)
    earlier = jnp.dot(named.astype(BF), before, preferred_element_type=F32)
    rank = jnp.sum(earlier * named, axis=0, keepdims=True).astype(jnp.int32)
    shift = geo.nyc.bit_length() - 1
    z = lax.shift_right_arithmetic(routes, shift)
    c = routes & (geo.nyc - 1)
    target = jnp.where(routes < 0, -1, (c * geo.nz + z) * geo.slots + rank)
    place = lax.broadcasted_iota(jnp.int32, (geo.rows, padded), 0) == target
    place = jnp.where(place, 1.0, 0.0)
    chosen = place.astype(BF)
    s_ref[:, :fourth] = jnp.dot(chosen, all_x, preferred_element_type=F32).astype(BF)
    s_ref[:, fourth:] = jnp.dot(chosen, all_scaled, preferred_element_type=F32).astype(BF)
    pt_ref[...] = place.T.astype(BF)


def dispatch_kernel(geo, s_ref, ci_ref, xin_ref, xsc_ref, halo_ref, got, mid, sa, ra, sb, rb, sc, rc, sh, rh):
    nz, nyc, slots, row_a, row_b = geo.nz, geo.nyc, geo.slots, geo.row_a, geo.row_b
    sp, z, c, j = geo.place()
    w = s_ref.shape[1] // 2
    hw = w // 2
    right, left = lax.rem(j + 1, 4), lax.rem(j + 3, 4)
    length = ci_ref.shape[0]
    full = (xin_ref, xsc_ref)
    after, ahead = lax.rem(sp + 1, geo.n), lax.rem(sp + geo.n - 1, geo.n)
    y_order, z_order = nearest_first(nyc), nearest_first(nz)

    def y_peer(k):
        return z * nyc + lax.rem(c + k, nyc)

    def z_at(k):
        return lax.rem(z + k, nz)

    def z_from(k):
        return lax.rem(z + nz - k, nz)

    greet(
        [(y_peer(k), j) for k in y_order]
        + [(z_at(k) * nyc + c, j) for k in z_order]
        + [(sp, right), (sp, left), (after, j), (ahead, j)]
    )
    sent = []
    for h in range(2):
        for k in y_order:
            sent.append(
                send(
                    s_ref.at[block(lax.rem(c + k, nyc), row_a), pl.ds(h * w, w)],
                    got.at[block(c, row_a), pl.ds(h * w, w)],
                    sa.at[h, k],
                    ra.at[h, k],
                    (y_peer(k), j),
                )
            )
    sent.append(
        send(ci_ref.at[pl.ds(length - EDGE, EDGE)], halo_ref.at[pl.ds(0, EDGE)], sh.at[0], rh.at[0], (after, j))
    )
    sent.append(send(ci_ref.at[pl.ds(0, EDGE)], halo_ref.at[pl.ds(EDGE, EDGE)], sh.at[1], rh.at[1], (ahead, j)))
    got[block(c, row_a), :] = s_ref[block(c, row_a), :]
    base = shuffle_base(row_b, geo.rows, slots, nz)

    def exchange_z(h):
        for k in y_order:
            source = lax.rem(c + nyc - k, nyc)
            arrival(
                got.at[block(source, row_a), pl.ds(h * w, w)], sa.at[h, k], ra.at[h, k], (y_peer(k), j)
            ).wait_recv()
        rows = got[:, h * w : (h + 1) * w]
        full[h][block(z, row_b), pl.ds(pl.multiple_of(j * w, w), w)] = picked_rows(base, z, slots, rows)

        def launch(k):
            sent.append(
                send(
                    mid.at[h, k],
                    full[h].at[block(z, row_b), pl.ds(pl.multiple_of(j * w, w), w)],
                    sb.at[h, k],
                    rb.at[h, k],
                    (z_at(k) * nyc + c, j),
                )
            )

        held = None
        for k in z_order:
            mid[h, k] = picked_rows(base, z_at(k), slots, rows)
            if held is not None:
                launch(held)
            held = k
        return lambda: launch(held)

    def part(h, k, column, size, offset=0):
        return full[h].at[block(z_from(k), row_b), pl.ds(pl.multiple_of(column * w + offset, hw), size)]

    def first_hop(h, k):
        if k:
            arrival(part(h, k, j, w), sb.at[h, k], rb.at[h, k], (z_at(k) * nyc + c, j)).wait_recv()
        mine = part(h, k, j, w)
        sent.append(send(mine, mine, sc.at[h, k, 0], rc.at[h, k, 0], (sp, right)))
        sent.append(send(mine, mine, sc.at[h, k, 1], rc.at[h, k, 1], (sp, left)))

    def second_hop(h, k):
        arrival(part(h, k, left, w), sc.at[h, k, 0], rc.at[h, k, 0], (sp, left)).wait_recv()
        low = part(h, k, left, hw)
        sent.append(send(low, low, sc.at[h, k, 2], rc.at[h, k, 2], (sp, right)))
        arrival(part(h, k, right, w), sc.at[h, k, 1], rc.at[h, k, 1], (sp, right)).wait_recv()
        high = part(h, k, right, hw, hw)
        sent.append(send(high, high, sc.at[h, k, 3], rc.at[h, k, 3], (sp, left)))

    lead = z_order[:2]
    rest0, rest1 = z_order[2:], list(z_order)
    later = [(0, k) for k in rest0[:2]] + [(1, k) for k in rest1[:2]]
    later += [(0, k) for k in rest0[2:]] + [(1, k) for k in rest1[2:]]
    plan = [(0, 0)] + [(0, k) for k in lead] + [(1, 0)] + later
    waiting, done = [], []
    for item in plan:
        if item[1] == 0:
            flush = exchange_z(item[0])
            first_hop(*item)
            flush()
        else:
            first_hop(*item)
        waiting.append(item)
        if len(waiting) > 2:
            done.append(waiting.pop(0))
            second_hop(*done[-1])
    for item in waiting:
        second_hop(*item)
    opposite = lax.rem(j + 2, 4)
    for h, k in plan:
        arrival(part(h, k, opposite, hw), sc.at[h, k, 2], rc.at[h, k, 2], (sp, left)).wait_recv()
        arrival(part(h, k, opposite, hw, hw), sc.at[h, k, 3], rc.at[h, k, 3], (sp, right)).wait_recv()
    for e in range(2):
        arrival(halo_ref.at[pl.ds(e * EDGE, EDGE)], sh.at[e], rh.at[e], (after, j)).wait_recv()
    for copy in sent:
        copy.wait_send()


def return_kernel(
    geo, p_ref, pt_ref, ng_ref, thru, direct, comb, fin, share, z_got, y_out, back, sx, rx, sz, rz, sy, ry, sg, rg
):
    nz, nyc, slots, row_a, row_b = geo.nz, geo.nyc, geo.slots, geo.row_a, geo.row_b
    sp, z, c, j = geo.place()
    w = p_ref.shape[1] // 4
    hw = w // 2
    length = ng_ref.shape[0]
    right, left, opposite = lax.rem(j + 1, 4), lax.rem(j + 3, 4), lax.rem(j + 2, 4)
    y_order, z_order = nearest_first(nyc), nearest_first(nz)
    plan = list(reversed(z_order)) + [0]

    def y_peer(k):
        return z * nyc + lax.rem(c + k, nyc)

    def z_at(k):
        return lax.rem(z + k, nz)

    greet(
        [(y_peer(k), j) for k in y_order]
        + [(z_at(k) * nyc + c, j) for k in z_order]
        + [(sp, right), (sp, left)]
    )
    sent = []

    def piece(k, column, offset):
        return p_ref.at[block(z_at(k), row_b), pl.ds(pl.multiple_of(column * w + offset, hw), hw)]

    def go(src, dst, sem, k, device):
        sent.append(send(src, dst, sx.at[k, sem], rx.at[k, sem], (sp, device)))

    def landed(dst, sem, k):
        arrival(dst, sx.at[k, sem], rx.at[k, sem], (sp, left)).wait_recv()

    for k in plan:
        go(piece(k, opposite, 0), thru.at[k, 0], 0, k, right)
        go(piece(k, opposite, hw), thru.at[k, 1], 1, k, left)
        go(piece(k, right, hw), direct.at[k, 0], 2, k, right)
        go(piece(k, left, 0), direct.at[k, 1], 3, k, left)

    def combine(k):
        landed(thru.at[k, 0], 0, k)
        comb[k, 0] = (piece(k, right, 0)[...].astype(F32) + thru[k, 0].astype(F32)).astype(BF)
        landed(thru.at[k, 1], 1, k)
        comb[k, 1] = (piece(k, left, hw)[...].astype(F32) + thru[k, 1].astype(F32)).astype(BF)

    def pass_on(k):
        go(comb.at[k, 0], fin.at[k, 0], 4, k, right)
        go(comb.at[k, 1], fin.at[k, 1], 5, k, left)

    def finish(k):
        for side in range(2):
            landed(direct.at[k, 1 - side], 3 - side, k)
            landed(fin.at[k, side], 4 + side, k)
            total = (
                piece(k, j, side * hw)[...].astype(F32)
                + fin[k, side].astype(F32)
                + direct[k, 1 - side].astype(F32)
            ).astype(BF)
            if k:
                share[k, :, side * hw : (side + 1) * hw] = total
            else:
                z_got[block(z, row_b), side * hw : (side + 1) * hw] = total

    def ship(k):
        if k:
            sent.append(
                send(share.at[k], z_got.at[block(z, row_b)], sz.at[k], rz.at[k], (z_at(k) * nyc + c, j))
            )

    stages = (combine, pass_on, finish, ship)
    lags = (0, 1, 2, 3)
    for step in range(len(plan) + lags[-1]):
        for stage, lag in zip(stages, lags):
            if 0 <= step - lag < len(plan):
                stage(plan[step - lag])
    base = shuffle_base(row_a, geo.rows, slots, nyc)
    for k in z_order:
        source = lax.rem(z + nz - k, nz)
        arrival(z_got.at[block(source, row_b)], sz.at[k], rz.at[k], (z_at(k) * nyc + c, j)).wait_recv()
    rows = z_got[...]

    def ship_y(k):
        sent.append(send(y_out.at[k], back.at[block(c, row_a)], sy.at[k], ry.at[k], (y_peer(k), j)))

    held = None
    for k in y_order:
        y_out[k] = picked_rows(base, lax.rem(c + k, nyc), slots, rows)
        if held is not None:
            ship_y(held)
        held = k
    back[block(c, row_a), :] = picked_rows(base, c, slots, rows)
    ship_y(held)
    for k in y_order:
        source = lax.rem(c + nyc - k, nyc)
        arrival(back.at[block(source, row_a)], sy.at[k], ry.at[k], (y_peer(k), j)).wait_recv()
    picked = jnp.dot(pt_ref[...], back[...], preferred_element_type=F32)
    ng_ref[:, pl.ds(pl.multiple_of(j * w, w), w)] = (picked[:length] + picked[length : 2 * length]).astype(BF)

    def columns(column, size, offset=0):
        return ng_ref.at[:, pl.ds(pl.multiple_of(column * w + offset, hw), size)]

    mine = columns(j, w)
    sent.append(send(mine, mine, sg.at[0], rg.at[0], (sp, right)))
    sent.append(send(mine, mine, sg.at[1], rg.at[1], (sp, left)))
    arrival(columns(left, w), sg.at[0], rg.at[0], (sp, left)).wait_recv()
    sent.append(send(columns(left, hw), columns(left, hw), sg.at[2], rg.at[2], (sp, right)))
    arrival(columns(right, w), sg.at[1], rg.at[1], (sp, right)).wait_recv()
    sent.append(send(columns(right, hw, hw), columns(right, hw, hw), sg.at[3], rg.at[3], (sp, left)))
    arrival(columns(opposite, hw), sg.at[2], rg.at[2], (sp, left)).wait_recv()
    arrival(columns(opposite, hw, hw), sg.at[3], rg.at[3], (sp, right)).wait_recv()
    for copy in sent:
        copy.wait_send()


def minus_expm1(x):
    near = 1.0 + x * (1.0 / 7.0)
    for n in (6.0, 5.0, 4.0, 3.0, 2.0):
        near = 1.0 + x * (1.0 / n) * near
    return jnp.where(x > -0.25, -x * near, 1.0 - jnp.exp(x))


def split_dot(value, matrix, dims):
    high = value.astype(BF)
    low = (value - high.astype(F32)).astype(BF)
    return lax.dot_general(high, matrix, (dims, ((), ())), preferred_element_type=F32) + lax.dot_general(
        low, matrix, (dims, ((), ())), preferred_element_type=F32
    )


def scan_rows(coef, drive, reverse):
    length = coef.shape[0]
    row = lax.broadcasted_iota(jnp.int32, coef.shape, 0)
    step = 1
    while step < length:
        if reverse:
            shift, inside = length - step, row < length - step
        else:
            shift, inside = step, row >= step
        near = jnp.where(inside, pltpu.roll(drive, shift, 0), 0.0)
        drive = coef * near + drive
        coef = coef * jnp.where(inside, pltpu.roll(coef, shift, 0), 1.0)
        step *= 2
    return coef, drive


GELU_C = 0.7978845608028654


def gelu_parts(x):
    inner = GELU_C * (x + 0.044715 * (x * x * x))
    t = jnp.tanh(inner)
    value = 0.5 * x * (1.0 + t)
    slope = 0.5 * (1.0 + t) + 0.5 * x * (1.0 - t * t) * (GELU_C * (1.0 + 3.0 * 0.044715 * (x * x)))
    return value, slope


def pre_greet(devices):
    barrier = pltpu.get_barrier_semaphore()
    for device in devices:
        pl.semaphore_signal(barrier, inc=1, device_id=device, device_id_type=MESH)
    return lambda: pl.semaphore_wait(barrier, len(devices))


class Carries:
    def __init__(self, geo, own, near, far, total, sems):
        self.geo, self.own, self.near, self.far, self.total = geo, own, near, far, total
        self.s1, self.r1, self.s2, self.r2 = sems
        self.sp, self.z, self.c, self.j = geo.place()
        self.y_order, self.z_order = nearest_first(geo.nyc), nearest_first(geo.nz)

    def y_peer(self, k):
        return (self.z * self.geo.nyc + lax.rem(self.c + k, self.geo.nyc), self.j)

    def z_peer(self, k):
        return (lax.rem(self.z + k, self.geo.nz) * self.geo.nyc + self.c, self.j)

    def start(self):
        self.near[self.c] = self.own[...]
        return [
            send(self.own, self.near.at[self.c], self.s1.at[k], self.r1.at[k], self.y_peer(k)) for k in self.y_order
        ]

    def combined(self, ref, count, place):
        results = []
        for side in range(2):
            shape = (2, self.own.shape[1])
            a, b = jnp.ones(shape, F32), jnp.zeros(shape, F32)
            ta, tb = a, b
            for i in range(count):
                at = i if side == 0 else count - 1 - i
                na, nb = ref[at, 2 * side : 2 * side + 2], ref[at, 4 + 2 * side : 6 + 2 * side]
                ta, tb = ta * na, na * tb + nb
                inside = (at < place) if side == 0 else (at > place)
                ma, mb = jnp.where(inside, na, 1.0), jnp.where(inside, nb, 0.0)
                a, b = a * ma, ma * b + mb
            results.append((a, b, ta, tb))
        return results

    def middle(self):
        nyc = self.geo.nyc
        for k in self.y_order:
            source = lax.rem(self.c + nyc - k, nyc)
            arrival(self.near.at[source], self.s1.at[k], self.r1.at[k], self.y_peer(k)).wait_recv()
        self.first = self.combined(self.near, nyc, self.c)
        for side in range(2):
            self.total[2 * side : 2 * side + 2] = self.first[side][2]
            self.total[4 + 2 * side : 6 + 2 * side] = self.first[side][3]
        self.far[self.z] = self.total[...]
        return [
            send(self.total, self.far.at[self.z], self.s2.at[k], self.r2.at[k], self.z_peer(k)) for k in self.z_order
        ]

    def end(self):
        nz = self.geo.nz
        for k in self.z_order:
            source = lax.rem(self.z + nz - k, nz)
            arrival(self.far.at[source], self.s2.at[k], self.r2.at[k], self.z_peer(k)).wait_recv()
        second = self.combined(self.far, nz, self.z)
        return [self.first[side][0] * second[side][1] + self.first[side][1] for side in range(2)]


def tail_kernel(
    geo, ng_ref, cot_ref, x_ref, op_ref, ci_ref, halo_ref, gb_ref, taps_ref, maps_ref, rate_ref, shift_ref,
    out_ref, ig_ref, bg_ref,
    big, mgb_ref, go_ref, cgb_ref, half, quarter, r1, r2, r3, halo, car, near, far, total,
    s1, q1, s2, q2, s3, q3, sh, rh, e1, f1, e2, f2,
):
    nz, ny, nyc = geo.nz, geo.ny, geo.nyc
    sp, z, c, j = geo.place()
    y, core = lax.div(c, 2), lax.rem(c, 2)
    length = ci_ref.shape[0]
    part = out_ref.shape[0]
    after, ahead = lax.rem(sp + 1, geo.n), lax.rem(sp + geo.n - 1, geo.n)
    y_order, z_order = nearest_first(ny), nearest_first(nz)
    partner = z * nyc + y * 2 + (1 - core)

    def y_peer(k):
        return (z * nyc + lax.rem(y + k, ny) * 2 + core, j)

    def z_peer(k):
        return (lax.rem(z + k, nz) * nyc + c, j)

    forward, backward = [
        Carries(geo, car.at[i], near.at[i], far.at[i], total.at[i], (e1.at[i], f1.at[i], e2.at[i], f2.at[i]))
        for i in range(2)
    ]
    met = pre_greet(
        [forward.y_peer(k) for k in nearest_first(nyc)] + [z_peer(k) for k in z_order] + [(after, j), (ahead, j)]
    )
    sent = []
    has_low = jnp.where(sp > 0, 1.0, 0.0)
    has_high = jnp.where(sp < geo.n - 1, 1.0, 0.0)

    def surround(low, middle, high):
        big[0:EDGE] = low.astype(F32) * has_low
        big[EDGE : EDGE + length] = middle
        big[EDGE + length :] = high.astype(F32) * has_high

    surround(halo_ref[0:EDGE], ci_ref[...].astype(F32), halo_ref[EDGE:])
    conv = jnp.zeros(ci_ref.shape, F32)
    for o in range(4):
        conv = conv + big[EDGE - 2 + o : EDGE - 2 + o + length] * taps_ref[o : o + 1, :]
    gates = []
    for d in range(2):
        recur = jax.nn.sigmoid(split_dot(conv, maps_ref[2 * d], ((1,), (0,))))
        inputs = jax.nn.sigmoid(split_dot(conv, maps_ref[2 * d + 1], ((1,), (0,))))
        log_decay = -DECAY_SCALE * recur * rate_ref[d : d + 1, :] + shift_ref[d]
        gates.append((recur, inputs, jnp.exp(log_decay), jnp.sqrt(minus_expm1(2.0 * log_decay))))
    last = length - 1
    cum_f, state_f = scan_rows(gates[0][2], gates[0][3] * (gates[0][1] * conv), False)
    cum_b, state_b = scan_rows(gates[1][2], gates[1][3] * (gates[1][1] * conv), True)

    def fill(ref, sums):
        products = (cum_f[last:], cum_b[0:1], cum_b[0:1], cum_f[last:])
        for i, value in enumerate(products + sums):
            ref[i : i + 1, :] = value

    zero = jnp.zeros((1, ci_ref.shape[1]), F32)
    fill(car.at[0], (state_f[last:], zero, state_b[0:1], zero))
    x32 = x_ref[...].astype(F32)
    inv_rms = lax.rsqrt(jnp.mean(x32 * x32, axis=1, keepdims=True) + EPS)
    met()
    sent += forward.start()
    normed = x32 * inv_rms
    ng = ng_ref[...].astype(F32)
    mean = jnp.mean(ng * normed, axis=1, keepdims=True)
    mgb = (cot_ref[...].astype(F32) + inv_rms * (ng - normed * mean)).astype(BF)
    mgb_ref[...] = mgb
    out_grad = jnp.dot(mgb, op_ref[...], preferred_element_type=F32)
    value, slope = gelu_parts(gb_ref[...].astype(F32))
    carried = out_grad * value
    cum_bf, after_b = scan_rows(gates[1][2], gates[1][2] * carried, False)
    cum_fr, after_f = scan_rows(gates[0][2], gates[0][2] * carried, True)
    fill(car.at[1], (zero, after_b[last:], zero, after_f[0:1]))
    sent += forward.middle()
    sent += backward.start()
    low, high = forward.end()
    low_f, up_b = low[0:1], high[0:1]
    sent += backward.middle()
    row = lax.broadcasted_iota(jnp.int32, ci_ref.shape, 0)

    def from_before(value, carry):
        return jnp.where(row == 0, carry, pltpu.roll(value, 1, 0))

    def from_after(value, carry):
        return jnp.where(row == last, carry, pltpu.roll(value, length - 1, 0))

    state_f = state_f + cum_f * low_f
    state_b = state_b + cum_b * up_b
    states = state_f + state_b
    bg_ref[...] = (out_grad * states * slope).astype(BF)
    mixed_out = (value * states).astype(BF)
    go = lax.dot_general(mgb_ref[...], mixed_out, (((0,), (0,)), ((), ())), preferred_element_type=F32)
    go_ref[...] = go.astype(BF).reshape(go_ref.shape)
    low, high = backward.end()
    low_b, up_f = low[1:2], high[1:2]
    sent.append(send(go_ref.at[:, :, 1 - core], r1, s1, q1, (partner, j)))
    after_b = after_b + cum_bf * low_b
    after_f = after_f + cum_fr * up_f
    adjoints = (carried + from_after(after_f, up_f), carried + from_before(after_b, low_b))
    others = (from_before(state_f, low_f), from_after(state_b, up_b))
    conv_grad = jnp.zeros(ci_ref.shape, F32)
    for d in range(2):
        recur, inputs, coef, root = gates[d]
        adjoint = adjoints[d]
        log_grad = adjoint * others[d] * coef - adjoint * (inputs * conv) * (coef * coef) / root
        recur_grad = log_grad * (-DECAY_SCALE * rate_ref[d : d + 1, :]) * recur * (1.0 - recur)
        input_grad = adjoint * root * conv * inputs * (1.0 - inputs)
        conv_grad = conv_grad + adjoint * root * inputs
        conv_grad = conv_grad + split_dot(recur_grad, maps_ref[2 * d], ((1,), (1,)))
        conv_grad = conv_grad + split_dot(input_grad, maps_ref[2 * d + 1], ((1,), (1,)))
    cgb_ref[...] = conv_grad.astype(BF)
    arrival(r1, s1, q1, (partner, j)).wait_recv()
    for k in y_order + [0]:
        at = lax.rem(y + k, ny)
        half[k] = (go_ref[:, at, core].astype(F32) + r1[:, at].astype(F32)).astype(BF)
    sent.append(send(cgb_ref.at[pl.ds(length - EDGE, EDGE)], halo.at[pl.ds(0, EDGE)], sh.at[0], rh.at[0], (after, j)))
    sent.append(send(cgb_ref.at[pl.ds(0, EDGE)], halo.at[pl.ds(EDGE, EDGE)], sh.at[1], rh.at[1], (ahead, j)))
    for k in y_order:
        sent.append(send(half.at[k], r2.at[k], s2.at[k], q2.at[k], y_peer(k)))
    for e in range(2):
        arrival(halo.at[pl.ds(e * EDGE, EDGE)], sh.at[e], rh.at[e], (after, j)).wait_recv()
    surround(halo[0:EDGE], conv_grad, halo[EDGE:])
    grad = jnp.zeros(ci_ref.shape, F32)
    for o in range(4):
        grad = grad + big[EDGE + 2 - o : EDGE + 2 - o + length] * taps_ref[o : o + 1, :]
    ig_ref[...] = grad.astype(BF)
    for k in y_order:
        arrival(r2.at[k], s2.at[k], q2.at[k], y_peer(k)).wait_recv()
    for k in z_order + [0]:
        at = lax.rem(z + k, nz)
        summed = half[0, at].astype(F32)
        for m in y_order:
            summed = summed + r2[m, at].astype(F32)
        quarter[k] = summed.astype(BF)
    for k in z_order:
        sent.append(send(quarter.at[k], r3.at[k], s3.at[k], q3.at[k], z_peer(k)))
    result = quarter[0].astype(F32)
    for k in z_order:
        arrival(r3.at[k], s3.at[k], q3.at[k], z_peer(k)).wait_recv()
        result = result + r3[k].astype(F32)
    out_ref[...] = result
    for copy in sent:
        copy.wait_send()


def local(body, geo, inputs, outs, scratch=()):
    return pl.pallas_call(
        functools.partial(body, geo),
        out_shape=outs,
        in_specs=[VM] * inputs,
        out_specs=jax.tree.map(lambda _: VM, outs),
        scratch_shapes=list(scratch),
        compiler_params=pltpu.CompilerParams(vmem_limit_bytes=60 * 2**20),
    )


def remote(body, geo, number, inputs, outs, scratch):
    return pl.pallas_call(
        functools.partial(body, geo),
        out_shape=outs,
        in_specs=[VM] * inputs,
        out_specs=jax.tree.map(lambda _: VM, outs),
        scratch_shapes=list(scratch),
        compiler_params=pltpu.CompilerParams(
            collective_id=number, has_side_effects=True, vmem_limit_bytes=60 * 2**20
        ),
    )


def block_matrices(maps):
    heads = maps.shape[1]
    eye = jnp.eye(heads, dtype=maps.dtype)
    full = maps[:, :, :, None, :] * eye[None, :, None, :, None]
    return full.reshape(maps.shape[0], heads * maps.shape[2], heads * maps.shape[3])


def shards(
    cotangent,
    saved_input,
    routes,
    route_weight,
    gate_proj,
    up_proj,
    down_proj,
    out_proj,
    conv_input,
    gate_branch,
    conv_taps,
    recur_map,
    input_map,
    decay_param,
    decay_shift,
):
    length, width = cotangent.shape
    n_sp = lax.axis_size("sp")
    geo = Geometry(n_sp, 4 * length // n_sp)
    nz, ny, nyc, rows = geo.nz, geo.ny, geo.nyc, geo.rows
    w = width // 4
    channels = conv_input.shape[1]
    shape = jax.ShapeDtypeStruct
    padded = -(-2 * length // 128) * 128
    flat_routes = jnp.pad(routes.T.reshape(1, 2 * length), ((0, 0), (0, padded - 2 * length)), constant_values=-1)
    slots, places = local(prep_kernel, geo, 4, (shape((rows, 2 * w), BF), shape((padded, rows), BF)))(
        cotangent, saved_input, flat_routes, route_weight
    )
    rows_input, rows_scaled, halo = remote(
        dispatch_kernel,
        geo,
        1,
        2,
        (shape((rows, width), BF), shape((rows, width), BF), shape((2 * EDGE, channels), BF)),
        [
            pltpu.VMEM((rows, 2 * w), BF),
            pltpu.VMEM((2, nz, geo.row_b, w), BF),
            DMA((2, nyc)),
            DMA((2, nyc)),
            DMA((2, nz)),
            DMA((2, nz)),
            DMA((2, nz, 4)),
            DMA((2, nz, 4)),
            DMA((2,)),
            DMA((2,)),
        ],
    )(slots, conv_input)
    w_gate, w_up, w_down = gate_proj[0], up_proj[0], down_proj[0]
    gate_pre = jnp.dot(rows_input, w_gate, preferred_element_type=F32)
    up_pre = jnp.dot(rows_input, w_up, preferred_element_type=F32)
    gate_sig = jax.nn.sigmoid(gate_pre)
    gate_act = gate_pre * gate_sig
    hidden = (gate_act * up_pre).astype(BF)
    hidden_grad = lax.dot_general(rows_scaled, w_down, (((1,), (1,)), ((), ())), preferred_element_type=F32)
    gate_grad = (hidden_grad * up_pre * gate_sig * (1.0 + gate_pre * (1.0 - gate_sig))).astype(BF)
    up_grad = (hidden_grad * gate_act).astype(BF)
    over_rows = (((0,), (0,)), ((), ()))
    grad_down = lax.dot_general(hidden, rows_scaled, over_rows, preferred_element_type=F32)
    grad_gate = lax.dot_general(rows_input, gate_grad, over_rows, preferred_element_type=F32)
    grad_up = lax.dot_general(rows_input, up_grad, over_rows, preferred_element_type=F32)
    transposed = (((1,), (1,)), ((), ()))
    partial_rows = lax.dot_general(gate_grad, w_gate, transposed, preferred_element_type=F32)
    partial_rows = partial_rows + lax.dot_general(up_grad, w_up, transposed, preferred_element_type=F32)
    half = (nz, 2, geo.row_b, w // 2)
    normed_grad = remote(
        return_kernel,
        geo,
        2,
        2,
        shape((length, width), BF),
        [pltpu.VMEM(half, BF)] * 4
        + [
            pltpu.VMEM((nz, geo.row_b, w), BF),
            pltpu.VMEM((rows, w), BF),
            pltpu.VMEM((nyc, geo.row_a, w), BF),
            pltpu.VMEM((rows, w), BF),
            DMA((nz, 6)),
            DMA((nz, 6)),
            DMA((nz,)),
            DMA((nz,)),
            DMA((nyc,)),
            DMA((nyc,)),
            DMA((4,)),
            DMA((4,)),
        ],
    )(partial_rows.astype(BF), places)
    taps32 = conv_taps.astype(F32)
    maps = block_matrices(jnp.stack([recur_map[0], input_map[0], recur_map[1], input_map[1]]))
    rate = jax.nn.softplus(-decay_param)
    own = (length, channels)
    big = pltpu.VMEM((length + 2 * EDGE, channels), F32)
    part = width // n_sp
    carry = (8, channels)
    grad_out, input_grad, branch_grad = remote(
        tail_kernel,
        geo,
        3,
        11,
        (shape((part, channels), F32), shape(own, BF), shape(own, BF)),
        [
            big,
            pltpu.VMEM((length, width), BF),
            pltpu.VMEM((nz, ny, 2, part, channels), BF),
            pltpu.VMEM(own, BF),
            pltpu.VMEM((ny, nz, part, channels), BF),
            pltpu.VMEM((nz, part, channels), BF),
            pltpu.VMEM((nz, ny, part, channels), BF),
            pltpu.VMEM((ny, nz, part, channels), BF),
            pltpu.VMEM((nz, part, channels), BF),
            pltpu.VMEM((2 * EDGE, channels), BF),
            pltpu.VMEM((2, *carry), F32),
            pltpu.VMEM((2, nyc, *carry), F32),
            pltpu.VMEM((2, nz, *carry), F32),
            pltpu.VMEM((2, *carry), F32),
            DMA,
            DMA,
            DMA((ny,)),
            DMA((ny,)),
            DMA((nz,)),
            DMA((nz,)),
            DMA((2,)),
            DMA((2,)),
            DMA((2, nyc)),
            DMA((2, nyc)),
            DMA((2, nz)),
            DMA((2, nz)),
        ],
    )(
        normed_grad, cotangent, saved_input, out_proj, conv_input, halo, gate_branch, taps32, maps, rate, decay_shift
    )
    return (grad_gate[None], grad_up[None], grad_down[None], grad_out, input_grad, branch_grad)


def solution(mesh):
    in_specs = (
        P("sp", None),
        P("sp", None),
        P("sp", None),
        P("sp", None),
        P("sp", None, "tp"),
        P("sp", None, "tp"),
        P("sp", "tp", None),
        P(None, "tp"),
        P("sp", "tp"),
        P("sp", "tp"),
        P(None, "tp"),
        P(None, "tp", None, None),
        P(None, "tp", None, None),
        P(None, "tp"),
        P(None, "sp", "tp"),
    )
    out_specs = (
        P("sp", None, "tp"),
        P("sp", None, "tp"),
        P("sp", "tp", None),
        P("sp", "tp"),
        P("sp", "tp"),
        P("sp", "tp"),
    )
    return jax.shard_map(shards, mesh=mesh, in_specs=in_specs, out_specs=out_specs, check_vma=False)
```

```python
import functools

import jax
import jax.numpy as jnp
from jax import lax
from jax.experimental import pallas as pl
from jax.experimental.pallas import tpu as pltpu
from jax.sharding import PartitionSpec as P

EPS = 1e-06
DECAY_SCALE = 8.0
MESH = pl.DeviceIdType.MESH
EDGE = 16
BF = jnp.bfloat16
F32 = jnp.float32
VM = pl.BlockSpec(memory_space=pltpu.VMEM)
DMA = pltpu.SemaphoreType.DMA


class Geometry:
    def __init__(self, n_sp, slots):
        self.n = n_sp
        self.nyc = 8 if n_sp == 64 else 2
        self.nz = n_sp // self.nyc
        self.ny = self.nyc // 2
        self.slots = slots
        self.row_a = self.nz * slots
        self.row_b = self.nyc * slots
        self.rows = n_sp * slots

    def place(self):
        sp = lax.axis_index("sp")
        return sp, lax.div(sp, self.nyc), lax.rem(sp, self.nyc), lax.axis_index("tp")


def nearest_first(n):
    order = []
    for k in range(1, n):
        for step in (k, n - k):
            if step not in order and 0 < step < n:
                order.append(step)
    return order


def send(src, dst, send_sem, recv_sem, device):
    copy = pltpu.make_async_remote_copy(
        src_ref=src,
        dst_ref=dst,
        send_sem=send_sem,
        recv_sem=recv_sem,
        device_id=device,
        device_id_type=MESH,
    )
    copy.start()
    return copy


def arrival(dst, send_sem, recv_sem, device):
    return pltpu.make_async_remote_copy(
        src_ref=dst,
        dst_ref=dst,
        send_sem=send_sem,
        recv_sem=recv_sem,
        device_id=device,
        device_id_type=MESH,
    )


def greet(devices):
    barrier = pltpu.get_barrier_semaphore()
    for device in devices:
        pl.semaphore_signal(barrier, inc=1, device_id=device, device_id_type=MESH)
    pl.semaphore_wait(barrier, len(devices))


def block(ref_dim, size):
    return pl.ds(pl.multiple_of(ref_dim * size, size), size)


def group_of(q, slots):
    return lax.shift_right_logical(q * (2048 // slots + 1), 11)


def shuffle_base(count, total, slots, others):
    q = lax.broadcasted_iota(jnp.int32, (count, total), 0)
    col = lax.broadcasted_iota(jnp.int32, (count, total), 1)
    return col - q - group_of(q, slots) * ((others - 1) * slots)


def picked_rows(base, target, slots, rows):
    chosen = jnp.where(base == target * slots, 1.0, 0.0).astype(BF)
    return jnp.dot(chosen, rows, preferred_element_type=F32).astype(BF)


def prep_kernel(geo, cot_ref, x_ref, routes_ref, weight_ref, s_ref, pt_ref):
    length, width = x_ref.shape
    fourth = width // 4
    padded = routes_ref.shape[1]
    x32 = x_ref[...].astype(F32)
    inv_rms = lax.rsqrt(jnp.mean(x32 * x32, axis=1, keepdims=True) + EPS)
    first = pl.multiple_of(lax.axis_index("tp") * fourth, fourth)
    own_x = (x_ref[:, pl.ds(first, fourth)].astype(F32) * inv_rms).astype(BF)
    own_cot = cot_ref[:, pl.ds(first, fourth)].astype(F32)
    filler = jnp.zeros((padded - 2 * length, fourth), BF)
    scaled = [(weight_ref[:, k : k + 1] * own_cot).astype(BF) for k in range(2)]
    all_scaled = jnp.concatenate(scaled + [filler], axis=0)
    all_x = jnp.concatenate([own_x, own_x, filler], axis=0)
    routes = routes_ref[...]
    named = lax.broadcasted_iota(jnp.int32, (geo.n, padded), 0) == routes
    named = jnp.where(named, 1.0, 0.0)
    before = lax.broadcasted_iota(jnp.int32, (padded, padded), 0) < lax.broadcasted_iota(
        jnp.int32, (padded, padded), 1
    )
    before = jnp.where(before, 1.0, 0.0).astype(BF)
    earlier = jnp.dot(named.astype(BF), before, preferred_element_type=F32)
    rank = jnp.sum(earlier * named, axis=0, keepdims=True).astype(jnp.int32)
    shift = geo.nyc.bit_length() - 1
    z = lax.shift_right_arithmetic(routes, shift)
    c = routes & (geo.nyc - 1)
    target = jnp.where(routes < 0, -1, (c * geo.nz + z) * geo.slots + rank)
    place = lax.broadcasted_iota(jnp.int32, (geo.rows, padded), 0) == target
    place = jnp.where(place, 1.0, 0.0)
    chosen = place.astype(BF)
    s_ref[:, :fourth] = jnp.dot(chosen, all_x, preferred_element_type=F32).astype(BF)
    s_ref[:, fourth:] = jnp.dot(chosen, all_scaled, preferred_element_type=F32).astype(BF)
    pt_ref[...] = place.T.astype(BF)


def wire(src, dst, send_sem, recv_sem, device):
    return pltpu.make_async_remote_copy(
        src_ref=src, dst_ref=dst, send_sem=send_sem, recv_sem=recv_sem, device_id=device, device_id_type=MESH
    )


def across(a, b):
    return lax.dot_general(a, b, (((1,), (1,)), ((), ())), preferred_element_type=F32)


def experts_kernel(
    geo, s_ref, ci_ref, pt_ref, wg_ref, wu_ref, wd_ref,
    xin_ref, xsc_ref, hid_ref, gg_ref, ug_ref, halo_ref, ng_ref,
    got, mid, p_ref, thru, direct, comb, fin, share, z_got, y_out, back,
    sa, ra, sb, rb, sc, rc, sh, rh, sx, rx, sz, rz, sy, ry, sg, rg,
):
    nz, nyc, slots, row_a, row_b = geo.nz, geo.nyc, geo.slots, geo.row_a, geo.row_b
    sp, z, c, j = geo.place()
    w = s_ref.shape[1] // 2
    hw = w // 2
    right, left, opposite = lax.rem(j + 1, 4), lax.rem(j + 3, 4), lax.rem(j + 2, 4)
    length = ci_ref.shape[0]
    full = (xin_ref, xsc_ref)
    after, ahead = lax.rem(sp + 1, geo.n), lax.rem(sp + geo.n - 1, geo.n)
    y_order, z_order = nearest_first(nyc), nearest_first(nz)

    def turn(i):
        if isinstance(i, int):
            return ([0] + z_order)[i]
        return jnp.where(lax.rem(i, 2) == 1, lax.div(i + 1, 2), lax.rem(nz - lax.div(i, 2), nz))

    def y_peer(k):
        return (z * nyc + lax.rem(c + k, nyc), j)

    def z_at(k):
        return lax.rem(z + k, nz)

    def z_from(k):
        return lax.rem(z + nz - k, nz)

    def z_peer(k):
        return (z_at(k) * nyc + c, j)

    def columns(column, offset=0):
        return pl.multiple_of(column * w + offset, hw)

    greet(
        [y_peer(k) for k in y_order]
        + [z_peer(k) for k in z_order]
        + [(sp, right), (sp, left), (after, j), (ahead, j)]
    )

    def y_copy(h, k):
        return wire(
            s_ref.at[block(lax.rem(c + k, nyc), row_a), pl.ds(h * w, w)],
            got.at[block(c, row_a), pl.ds(h * w, w)],
            sa.at[h, k],
            ra.at[h, k],
            y_peer(k),
        )

    for h in range(2):
        for k in y_order:
            y_copy(h, k).start()
    edges = [
        wire(ci_ref.at[pl.ds(length - EDGE, EDGE)], halo_ref.at[pl.ds(0, EDGE)], sh.at[0], rh.at[0], (after, j)),
        wire(ci_ref.at[pl.ds(0, EDGE)], halo_ref.at[pl.ds(EDGE, EDGE)], sh.at[1], rh.at[1], (ahead, j)),
    ]
    for copy in edges:
        copy.start()
    got[block(c, row_a), :] = s_ref[block(c, row_a), :]
    base = shuffle_base(row_b, geo.rows, slots, nz)

    def z_copy(h, k):
        own = full[h].at[block(z, row_b), pl.ds(columns(j), w)]
        return wire(mid.at[h, k], own, sb.at[h, k], rb.at[h, k], z_peer(k))

    def exchange_z(h):
        for k in y_order:
            source = lax.rem(c + nyc - k, nyc)
            arrival(got.at[block(source, row_a), pl.ds(h * w, w)], sa.at[h, k], ra.at[h, k], y_peer(k)).wait_recv()
        rows = got[:, h * w : (h + 1) * w]
        held = None
        for k in z_order:
            mid[h, k] = picked_rows(base, z_at(k), slots, rows)
            if held is not None:
                z_copy(h, held).start()
            held = k
        full[h][block(z, row_b), pl.ds(columns(j), w)] = picked_rows(base, z, slots, rows)
        z_copy(h, held).start()

    def part(h, i, column, size, offset=0):
        return full[h].at[block(z_from(turn(i)), row_b), pl.ds(columns(column, offset), size)]

    def x_copy(h, i, kind):
        ref = (
            lambda: part(h, i, j, w),
            lambda: part(h, i, j, w),
            lambda: part(h, i, left, hw),
            lambda: part(h, i, right, hw, hw),
        )[kind]()
        return wire(ref, ref, sc.at[h, i, kind], rc.at[h, i, kind], (sp, left if kind % 2 else right))

    def x_landed(h, i, kind):
        ref = (
            lambda: part(h, i, left, w),
            lambda: part(h, i, right, w),
            lambda: part(h, i, opposite, hw),
            lambda: part(h, i, opposite, hw, hw),
        )[kind]()
        arrival(ref, sc.at[h, i, kind], rc.at[h, i, kind], (sp, right)).wait_recv()

    def first_hop(h, i):
        if not (isinstance(i, int) and i == 0):
            k = turn(i)
            arrival(part(h, i, j, w), sb.at[h, k], rb.at[h, k], z_peer(k)).wait_recv()
        x_copy(h, i, 0).start()
        x_copy(h, i, 1).start()

    def second_hop(h, i):
        for side in range(2):
            x_landed(h, i, side)
            x_copy(h, i, 2 + side).start()

    def compute(i):
        for h in range(2):
            for kind in (2, 3):
                x_landed(h, i, kind)
        rows = block(z_from(turn(i)), row_b)
        x = xin_ref[rows, :]
        gate_pre = jnp.dot(x, wg_ref[...], preferred_element_type=F32)
        up_pre = jnp.dot(x, wu_ref[...], preferred_element_type=F32)
        hidden_grad = across(xsc_ref[rows, :], wd_ref[...])
        gate_sig = jax.nn.sigmoid(gate_pre)
        gate_act = gate_pre * gate_sig
        hid_ref[rows, :] = (gate_act * up_pre).astype(BF)
        gate_grad = (hidden_grad * up_pre * gate_sig * (1.0 + gate_pre * (1.0 - gate_sig))).astype(BF)
        up_grad = (hidden_grad * gate_act).astype(BF)
        gg_ref[rows, :] = gate_grad
        ug_ref[rows, :] = up_grad
        for q in range(4):
            cut = pl.ds(q * w, w)
            p_ref[i, :, cut] = (across(gate_grad, wg_ref[cut, :]) + across(up_grad, wu_ref[cut, :])).astype(BF)

    def piece(i, column, offset):
        return p_ref.at[i, :, pl.ds(columns(column, offset), hw)]

    def s_copy(i, kind):
        src, dst = (
            lambda: (piece(i, opposite, 0), thru.at[i, 0]),
            lambda: (piece(i, opposite, hw), thru.at[i, 1]),
            lambda: (piece(i, right, hw), direct.at[i, 0]),
            lambda: (piece(i, left, 0), direct.at[i, 1]),
            lambda: (comb.at[i, 0], fin.at[i, 0]),
            lambda: (comb.at[i, 1], fin.at[i, 1]),
        )[kind]()
        return wire(src, dst, sx.at[i, kind], rx.at[i, kind], (sp, left if kind % 2 else right))

    def s_landed(ref, i, kind):
        arrival(ref, sx.at[i, kind], rx.at[i, kind], (sp, left)).wait_recv()

    def spread(i):
        for kind in range(4):
            s_copy(i, kind).start()

    def combine(i):
        s_landed(thru.at[i, 0], i, 0)
        comb[i, 0] = (piece(i, right, 0)[...].astype(F32) + thru[i, 0].astype(F32)).astype(BF)
        s_landed(thru.at[i, 1], i, 1)
        comb[i, 1] = (piece(i, left, hw)[...].astype(F32) + thru[i, 1].astype(F32)).astype(BF)

    def pass_on(i):
        s_copy(i, 4).start()
        s_copy(i, 5).start()

    def finish(i):
        for side in range(2):
            s_landed(direct.at[i, 1 - side], i, 3 - side)
            s_landed(fin.at[i, side], i, 4 + side)
            total = (
                piece(i, j, side * hw)[...].astype(F32)
                + fin[i, side].astype(F32)
                + direct[i, 1 - side].astype(F32)
            )
            share[i, :, side * hw : (side + 1) * hw] = total.astype(BF)

    def r_copy(i):
        k = turn(i)
        return wire(
            share.at[i], z_got.at[block(z, row_b)], sz.at[k], rz.at[k], (z_from(k) * nyc + c, j)
        )

    exchange_z(0)
    for i in range(min(3, nz)):
        first_hop(0, i)
    exchange_z(1)
    first_hop(1, 0)
    if nz > 3:
        first_hop(0, 3)
    for i in range(min(2, nz)):
        second_hop(0, i)
    second_hop(1, 0)

    def step(t, _):
        @pl.when(t + 4 < nz)
        def _():
            first_hop(0, t + 4)

        @pl.when(t + 1 < nz)
        def _():
            first_hop(1, t + 1)

        @pl.when(t + 2 < nz)
        def _():
            second_hop(0, t + 2)

        @pl.when(t < nz)
        def _():
            compute(t)

        @pl.when(t + 1 < nz)
        def _():
            second_hop(1, t + 1)

        @pl.when(t < nz)
        def _():
            spread(t)

        @pl.when((t >= 1) & (t < nz + 1))
        def _():
            combine(t - 1)

        @pl.when(t >= 2)
        def _():
            finish(t - 2)

        @pl.when((t >= 1) & (t < nz + 1))
        def _():
            pass_on(t - 1)

        @pl.when(t >= 3)
        def _():
            r_copy(t - 2).start()

        return 0

    lax.fori_loop(0, nz + 2, step, 0)
    z_got[block(z, row_b), :] = share[0]
    base = shuffle_base(row_a, geo.rows, slots, nyc)
    for k in z_order:
        arrival(z_got.at[block(z_at(k), row_b)], sz.at[k], rz.at[k], z_peer(k)).wait_recv()
    rows = z_got[...]

    def b_copy(k):
        return wire(y_out.at[k], back.at[block(c, row_a)], sy.at[k], ry.at[k], y_peer(k))

    held = None
    for k in y_order:
        y_out[k] = picked_rows(base, lax.rem(c + k, nyc), slots, rows)
        if held is not None:
            b_copy(held).start()
        held = k
    back[block(c, row_a), :] = picked_rows(base, c, slots, rows)
    b_copy(held).start()
    for k in y_order:
        source = lax.rem(c + nyc - k, nyc)
        arrival(back.at[block(source, row_a)], sy.at[k], ry.at[k], y_peer(k)).wait_recv()
    picked = jnp.dot(pt_ref[...], back[...], preferred_element_type=F32)
    ng_ref[:, pl.ds(columns(j), w)] = (picked[:length] + picked[length : 2 * length]).astype(BF)

    def g_part(column, size, offset=0):
        return ng_ref.at[:, pl.ds(columns(column, offset), size)]

    gathers = [
        wire(g_part(j, w), g_part(j, w), sg.at[0], rg.at[0], (sp, right)),
        wire(g_part(j, w), g_part(j, w), sg.at[1], rg.at[1], (sp, left)),
        wire(g_part(left, hw), g_part(left, hw), sg.at[2], rg.at[2], (sp, right)),
        wire(g_part(right, hw, hw), g_part(right, hw, hw), sg.at[3], rg.at[3], (sp, left)),
    ]
    gathers[0].start()
    gathers[1].start()
    arrival(g_part(left, w), sg.at[0], rg.at[0], (sp, left)).wait_recv()
    gathers[2].start()
    arrival(g_part(right, w), sg.at[1], rg.at[1], (sp, right)).wait_recv()
    gathers[3].start()
    for e in range(2):
        arrival(halo_ref.at[pl.ds(e * EDGE, EDGE)], sh.at[e], rh.at[e], (after, j)).wait_recv()

    def drain(i, _):
        for h in range(2):
            for kind in range(4):
                x_copy(h, i, kind).wait_send()
        for kind in range(6):
            s_copy(i, kind).wait_send()
        return 0

    lax.fori_loop(0, nz, drain, 0)
    for k in y_order:
        y_copy(0, k).wait_send()
        y_copy(1, k).wait_send()
        b_copy(k).wait_send()
    for i in range(1, nz):
        r_copy(i).wait_send()
        z_copy(0, z_order[i - 1]).wait_send()
        z_copy(1, z_order[i - 1]).wait_send()
    arrival(g_part(opposite, hw), sg.at[2], rg.at[2], (sp, left)).wait_recv()
    arrival(g_part(opposite, hw, hw), sg.at[3], rg.at[3], (sp, right)).wait_recv()
    for copy in edges + gathers:
        copy.wait_send()


def minus_expm1(x):
    near = 1.0 + x * (1.0 / 7.0)
    for n in (6.0, 5.0, 4.0, 3.0, 2.0):
        near = 1.0 + x * (1.0 / n) * near
    return jnp.where(x > -0.25, -x * near, 1.0 - jnp.exp(x))


def split_dot(value, matrix, dims):
    high = value.astype(BF)
    low = (value - high.astype(F32)).astype(BF)
    return lax.dot_general(high, matrix, (dims, ((), ())), preferred_element_type=F32) + lax.dot_general(
        low, matrix, (dims, ((), ())), preferred_element_type=F32
    )


def scan_rows(coef, drive, reverse):
    length = coef.shape[0]
    row = lax.broadcasted_iota(jnp.int32, coef.shape, 0)
    step = 1
    while step < length:
        if reverse:
            shift, inside = length - step, row < length - step
        else:
            shift, inside = step, row >= step
        near = jnp.where(inside, pltpu.roll(drive, shift, 0), 0.0)
        drive = coef * near + drive
        coef = coef * jnp.where(inside, pltpu.roll(coef, shift, 0), 1.0)
        step *= 2
    return coef, drive


GELU_C = 0.7978845608028654


def gelu_parts(x):
    inner = GELU_C * (x + 0.044715 * (x * x * x))
    t = jnp.tanh(inner)
    value = 0.5 * x * (1.0 + t)
    slope = 0.5 * (1.0 + t) + 0.5 * x * (1.0 - t * t) * (GELU_C * (1.0 + 3.0 * 0.044715 * (x * x)))
    return value, slope


def pre_greet(devices):
    barrier = pltpu.get_barrier_semaphore()
    for device in devices:
        pl.semaphore_signal(barrier, inc=1, device_id=device, device_id_type=MESH)
    return lambda: pl.semaphore_wait(barrier, len(devices))


class Carries:
    def __init__(self, geo, own, near, far, total, sems):
        self.geo, self.own, self.near, self.far, self.total = geo, own, near, far, total
        self.s1, self.r1, self.s2, self.r2 = sems
        self.sp, self.z, self.c, self.j = geo.place()
        self.y_order, self.z_order = nearest_first(geo.nyc), nearest_first(geo.nz)

    def y_peer(self, k):
        return (self.z * self.geo.nyc + lax.rem(self.c + k, self.geo.nyc), self.j)

    def z_peer(self, k):
        return (lax.rem(self.z + k, self.geo.nz) * self.geo.nyc + self.c, self.j)

    def start(self):
        self.near[self.c] = self.own[...]
        return [
            send(self.own, self.near.at[self.c], self.s1.at[k], self.r1.at[k], self.y_peer(k)) for k in self.y_order
        ]

    def combined(self, ref, count, place):
        results = []
        for side in range(2):
            shape = (2, self.own.shape[1])
            a, b = jnp.ones(shape, F32), jnp.zeros(shape, F32)
            ta, tb = a, b
            for i in range(count):
                at = i if side == 0 else count - 1 - i
                na, nb = ref[at, 2 * side : 2 * side + 2], ref[at, 4 + 2 * side : 6 + 2 * side]
                ta, tb = ta * na, na * tb + nb
                inside = (at < place) if side == 0 else (at > place)
                ma, mb = jnp.where(inside, na, 1.0), jnp.where(inside, nb, 0.0)
                a, b = a * ma, ma * b + mb
            results.append((a, b, ta, tb))
        return results

    def middle(self):
        nyc = self.geo.nyc
        for k in self.y_order:
            source = lax.rem(self.c + nyc - k, nyc)
            arrival(self.near.at[source], self.s1.at[k], self.r1.at[k], self.y_peer(k)).wait_recv()
        self.first = self.combined(self.near, nyc, self.c)
        for side in range(2):
            self.total[2 * side : 2 * side + 2] = self.first[side][2]
            self.total[4 + 2 * side : 6 + 2 * side] = self.first[side][3]
        self.far[self.z] = self.total[...]
        return [
            send(self.total, self.far.at[self.z], self.s2.at[k], self.r2.at[k], self.z_peer(k)) for k in self.z_order
        ]

    def end(self):
        nz = self.geo.nz
        for k in self.z_order:
            source = lax.rem(self.z + nz - k, nz)
            arrival(self.far.at[source], self.s2.at[k], self.r2.at[k], self.z_peer(k)).wait_recv()
        second = self.combined(self.far, nz, self.z)
        return [self.first[side][0] * second[side][1] + self.first[side][1] for side in range(2)]


def tail_kernel(
    geo, ng_ref, cot_ref, x_ref, op_ref, ci_ref, halo_ref, gb_ref, taps_ref, maps_ref, rate_ref, shift_ref,
    out_ref, ig_ref, bg_ref,
    big, mgb_ref, go_ref, cgb_ref, half, quarter, r1, r2, r3, halo, car, near, far, total,
    s1, q1, s2, q2, s3, q3, sh, rh, e1, f1, e2, f2,
):
    nz, ny, nyc = geo.nz, geo.ny, geo.nyc
    sp, z, c, j = geo.place()
    y, core = lax.div(c, 2), lax.rem(c, 2)
    length = ci_ref.shape[0]
    part = out_ref.shape[0]
    after, ahead = lax.rem(sp + 1, geo.n), lax.rem(sp + geo.n - 1, geo.n)
    y_order, z_order = nearest_first(ny), nearest_first(nz)
    partner = z * nyc + y * 2 + (1 - core)

    def y_peer(k):
        return (z * nyc + lax.rem(y + k, ny) * 2 + core, j)

    def z_peer(k):
        return (lax.rem(z + k, nz) * nyc + c, j)

    forward, backward = [
        Carries(geo, car.at[i], near.at[i], far.at[i], total.at[i], (e1.at[i], f1.at[i], e2.at[i], f2.at[i]))
        for i in range(2)
    ]
    met = pre_greet(
        [forward.y_peer(k) for k in nearest_first(nyc)] + [z_peer(k) for k in z_order] + [(after, j), (ahead, j)]
    )
    sent = []
    has_low = jnp.where(sp > 0, 1.0, 0.0)
    has_high = jnp.where(sp < geo.n - 1, 1.0, 0.0)

    def surround(low, middle, high):
        big[0:EDGE] = low.astype(F32) * has_low
        big[EDGE : EDGE + length] = middle
        big[EDGE + length :] = high.astype(F32) * has_high

    surround(halo_ref[0:EDGE], ci_ref[...].astype(F32), halo_ref[EDGE:])
    conv = jnp.zeros(ci_ref.shape, F32)
    for o in range(4):
        conv = conv + big[EDGE - 2 + o : EDGE - 2 + o + length] * taps_ref[o : o + 1, :]
    gates = []
    for d in range(2):
        recur = jax.nn.sigmoid(split_dot(conv, maps_ref[2 * d], ((1,), (0,))))
        inputs = jax.nn.sigmoid(split_dot(conv, maps_ref[2 * d + 1], ((1,), (0,))))
        log_decay = -DECAY_SCALE * recur * rate_ref[d : d + 1, :] + shift_ref[d]
        gates.append((recur, inputs, jnp.exp(log_decay), jnp.sqrt(minus_expm1(2.0 * log_decay))))
    last = length - 1
    cum_f, state_f = scan_rows(gates[0][2], gates[0][3] * (gates[0][1] * conv), False)
    cum_b, state_b = scan_rows(gates[1][2], gates[1][3] * (gates[1][1] * conv), True)

    def fill(ref, sums):
        products = (cum_f[last:], cum_b[0:1], cum_b[0:1], cum_f[last:])
        for i, value in enumerate(products + sums):
            ref[i : i + 1, :] = value

    zero = jnp.zeros((1, ci_ref.shape[1]), F32)
    fill(car.at[0], (state_f[last:], zero, state_b[0:1], zero))
    x32 = x_ref[...].astype(F32)
    inv_rms = lax.rsqrt(jnp.mean(x32 * x32, axis=1, keepdims=True) + EPS)
    met()
    sent += forward.start()
    normed = x32 * inv_rms
    ng = ng_ref[...].astype(F32)
    mean = jnp.mean(ng * normed, axis=1, keepdims=True)
    mgb = (cot_ref[...].astype(F32) + inv_rms * (ng - normed * mean)).astype(BF)
    mgb_ref[...] = mgb
    out_grad = jnp.dot(mgb, op_ref[...], preferred_element_type=F32)
    value, slope = gelu_parts(gb_ref[...].astype(F32))
    carried = out_grad * value
    cum_bf, after_b = scan_rows(gates[1][2], gates[1][2] * carried, False)
    cum_fr, after_f = scan_rows(gates[0][2], gates[0][2] * carried, True)
    fill(car.at[1], (zero, after_b[last:], zero, after_f[0:1]))
    sent += forward.middle()
    sent += backward.start()
    low, high = forward.end()
    low_f, up_b = low[0:1], high[0:1]
    sent += backward.middle()
    row = lax.broadcasted_iota(jnp.int32, ci_ref.shape, 0)

    def from_before(value, carry):
        return jnp.where(row == 0, carry, pltpu.roll(value, 1, 0))

    def from_after(value, carry):
        return jnp.where(row == last, carry, pltpu.roll(value, length - 1, 0))

    state_f = state_f + cum_f * low_f
    state_b = state_b + cum_b * up_b
    states = state_f + state_b
    bg_ref[...] = (out_grad * states * slope).astype(BF)
    mixed_out = (value * states).astype(BF)
    go = lax.dot_general(mgb_ref[...], mixed_out, (((0,), (0,)), ((), ())), preferred_element_type=F32)
    go_ref[...] = go.astype(BF).reshape(go_ref.shape)
    low, high = backward.end()
    low_b, up_f = low[1:2], high[1:2]
    sent.append(send(go_ref.at[:, :, 1 - core], r1, s1, q1, (partner, j)))
    after_b = after_b + cum_bf * low_b
    after_f = after_f + cum_fr * up_f
    adjoints = (carried + from_after(after_f, up_f), carried + from_before(after_b, low_b))
    others = (from_before(state_f, low_f), from_after(state_b, up_b))
    conv_grad = jnp.zeros(ci_ref.shape, F32)
    for d in range(2):
        recur, inputs, coef, root = gates[d]
        adjoint = adjoints[d]
        log_grad = adjoint * others[d] * coef - adjoint * (inputs * conv) * (coef * coef) / root
        recur_grad = log_grad * (-DECAY_SCALE * rate_ref[d : d + 1, :]) * recur * (1.0 - recur)
        input_grad = adjoint * root * conv * inputs * (1.0 - inputs)
        conv_grad = conv_grad + adjoint * root * inputs
        conv_grad = conv_grad + split_dot(recur_grad, maps_ref[2 * d], ((1,), (1,)))
        conv_grad = conv_grad + split_dot(input_grad, maps_ref[2 * d + 1], ((1,), (1,)))
    cgb_ref[...] = conv_grad.astype(BF)
    arrival(r1, s1, q1, (partner, j)).wait_recv()
    for k in y_order + [0]:
        at = lax.rem(y + k, ny)
        half[k] = (go_ref[:, at, core].astype(F32) + r1[:, at].astype(F32)).astype(BF)
    sent.append(send(cgb_ref.at[pl.ds(length - EDGE, EDGE)], halo.at[pl.ds(0, EDGE)], sh.at[0], rh.at[0], (after, j)))
    sent.append(send(cgb_ref.at[pl.ds(0, EDGE)], halo.at[pl.ds(EDGE, EDGE)], sh.at[1], rh.at[1], (ahead, j)))
    for k in y_order:
        sent.append(send(half.at[k], r2.at[k], s2.at[k], q2.at[k], y_peer(k)))
    for e in range(2):
        arrival(halo.at[pl.ds(e * EDGE, EDGE)], sh.at[e], rh.at[e], (after, j)).wait_recv()
    surround(halo[0:EDGE], conv_grad, halo[EDGE:])
    grad = jnp.zeros(ci_ref.shape, F32)
    for o in range(4):
        grad = grad + big[EDGE + 2 - o : EDGE + 2 - o + length] * taps_ref[o : o + 1, :]
    ig_ref[...] = grad.astype(BF)
    for k in y_order:
        arrival(r2.at[k], s2.at[k], q2.at[k], y_peer(k)).wait_recv()
    for k in z_order + [0]:
        at = lax.rem(z + k, nz)
        summed = half[0, at].astype(F32)
        for m in y_order:
            summed = summed + r2[m, at].astype(F32)
        quarter[k] = summed.astype(BF)
    for k in z_order:
        sent.append(send(quarter.at[k], r3.at[k], s3.at[k], q3.at[k], z_peer(k)))
    result = quarter[0].astype(F32)
    for k in z_order:
        arrival(r3.at[k], s3.at[k], q3.at[k], z_peer(k)).wait_recv()
        result = result + r3[k].astype(F32)
    out_ref[...] = result
    for copy in sent:
        copy.wait_send()


def local(body, geo, inputs, outs, scratch=()):
    return pl.pallas_call(
        functools.partial(body, geo),
        out_shape=outs,
        in_specs=[VM] * inputs,
        out_specs=jax.tree.map(lambda _: VM, outs),
        scratch_shapes=list(scratch),
        compiler_params=pltpu.CompilerParams(vmem_limit_bytes=60 * 2**20),
    )


def remote(body, geo, number, inputs, outs, scratch):
    return pl.pallas_call(
        functools.partial(body, geo),
        out_shape=outs,
        in_specs=[VM] * inputs,
        out_specs=jax.tree.map(lambda _: VM, outs),
        scratch_shapes=list(scratch),
        compiler_params=pltpu.CompilerParams(
            collective_id=number, has_side_effects=True, vmem_limit_bytes=60 * 2**20
        ),
    )


def block_matrices(maps):
    heads = maps.shape[1]
    eye = jnp.eye(heads, dtype=maps.dtype)
    full = maps[:, :, :, None, :] * eye[None, :, None, :, None]
    return full.reshape(maps.shape[0], heads * maps.shape[2], heads * maps.shape[3])


def shards(
    cotangent,
    saved_input,
    routes,
    route_weight,
    gate_proj,
    up_proj,
    down_proj,
    out_proj,
    conv_input,
    gate_branch,
    conv_taps,
    recur_map,
    input_map,
    decay_param,
    decay_shift,
):
    length, width = cotangent.shape
    n_sp = lax.axis_size("sp")
    geo = Geometry(n_sp, 4 * length // n_sp)
    nz, ny, nyc, rows = geo.nz, geo.ny, geo.nyc, geo.rows
    w = width // 4
    channels = conv_input.shape[1]
    shape = jax.ShapeDtypeStruct
    padded = -(-2 * length // 128) * 128
    flat_routes = jnp.pad(routes.T.reshape(1, 2 * length), ((0, 0), (0, padded - 2 * length)), constant_values=-1)
    slots, places = local(prep_kernel, geo, 4, (shape((rows, 2 * w), BF), shape((padded, rows), BF)))(
        cotangent, saved_input, flat_routes, route_weight
    )
    half = (nz, 2, geo.row_b, w // 2)
    hidden_shape = shape((rows, gate_proj.shape[2]), BF)
    wide = shape((rows, width), BF)
    rows_input, rows_scaled, hidden, gate_grad, up_grad, halo, normed_grad = remote(
        experts_kernel,
        geo,
        1,
        6,
        (wide, wide, hidden_shape, hidden_shape, hidden_shape, shape((2 * EDGE, channels), BF), shape((length, width), BF)),
        [
            pltpu.VMEM((rows, 2 * w), BF),
            pltpu.VMEM((2, nz, geo.row_b, w), BF),
            pltpu.VMEM((nz, geo.row_b, width), BF),
            pltpu.VMEM(half, BF),
            pltpu.VMEM(half, BF),
            pltpu.VMEM(half, BF),
            pltpu.VMEM(half, BF),
            pltpu.VMEM((nz, geo.row_b, w), BF),
            pltpu.VMEM((rows, w), BF),
            pltpu.VMEM((nyc, geo.row_a, w), BF),
            pltpu.VMEM((rows, w), BF),
            DMA((2, nyc)),
            DMA((2, nyc)),
            DMA((2, nz)),
            DMA((2, nz)),
            DMA((2, nz, 4)),
            DMA((2, nz, 4)),
            DMA((2,)),
            DMA((2,)),
            DMA((nz, 6)),
            DMA((nz, 6)),
            DMA((nz,)),
            DMA((nz,)),
            DMA((nyc,)),
            DMA((nyc,)),
            DMA((4,)),
            DMA((4,)),
        ],
    )(slots, conv_input, places, gate_proj[0], up_proj[0], down_proj[0])
    over_rows = (((0,), (0,)), ((), ()))
    grad_down = lax.dot_general(hidden, rows_scaled, over_rows, preferred_element_type=F32)
    grad_gate = lax.dot_general(rows_input, gate_grad, over_rows, preferred_element_type=F32)
    grad_up = lax.dot_general(rows_input, up_grad, over_rows, preferred_element_type=F32)
    taps32 = conv_taps.astype(F32)
    maps = block_matrices(jnp.stack([recur_map[0], input_map[0], recur_map[1], input_map[1]]))
    rate = jax.nn.softplus(-decay_param)
    own = (length, channels)
    big = pltpu.VMEM((length + 2 * EDGE, channels), F32)
    part = width // n_sp
    carry = (8, channels)
    grad_out, input_grad, branch_grad = remote(
        tail_kernel,
        geo,
        3,
        11,
        (shape((part, channels), F32), shape(own, BF), shape(own, BF)),
        [
            big,
            pltpu.VMEM((length, width), BF),
            pltpu.VMEM((nz, ny, 2, part, channels), BF),
            pltpu.VMEM(own, BF),
            pltpu.VMEM((ny, nz, part, channels), BF),
            pltpu.VMEM((nz, part, channels), BF),
            pltpu.VMEM((nz, ny, part, channels), BF),
            pltpu.VMEM((ny, nz, part, channels), BF),
            pltpu.VMEM((nz, part, channels), BF),
            pltpu.VMEM((2 * EDGE, channels), BF),
            pltpu.VMEM((2, *carry), F32),
            pltpu.VMEM((2, nyc, *carry), F32),
            pltpu.VMEM((2, nz, *carry), F32),
            pltpu.VMEM((2, *carry), F32),
            DMA,
            DMA,
            DMA((ny,)),
            DMA((ny,)),
            DMA((nz,)),
            DMA((nz,)),
            DMA((2,)),
            DMA((2,)),
            DMA((2, nyc)),
            DMA((2, nyc)),
            DMA((2, nz)),
            DMA((2, nz)),
        ],
    )(
        normed_grad, cotangent, saved_input, out_proj, conv_input, halo, gate_branch, taps32, maps, rate, decay_shift
    )
    return (grad_gate[None], grad_up[None], grad_down[None], grad_out, input_grad, branch_grad)


def solution(mesh):
    in_specs = (
        P("sp", None),
        P("sp", None),
        P("sp", None),
        P("sp", None),
        P("sp", None, "tp"),
        P("sp", None, "tp"),
        P("sp", "tp", None),
        P(None, "tp"),
        P("sp", "tp"),
        P("sp", "tp"),
        P(None, "tp"),
        P(None, "tp", None, None),
        P(None, "tp", None, None),
        P(None, "tp"),
        P(None, "sp", "tp"),
    )
    out_specs = (
        P("sp", None, "tp"),
        P("sp", None, "tp"),
        P("sp", "tp", None),
        P("sp", "tp"),
        P("sp", "tp"),
        P("sp", "tp"),
    )
    return jax.shard_map(shards, mesh=mesh, in_specs=in_specs, out_specs=out_specs, check_vma=False)
```

```python
import functools

import jax
import jax.numpy as jnp
from jax import lax
from jax.experimental import pallas as pl
from jax.experimental.pallas import tpu as pltpu
from jax.sharding import PartitionSpec as P

EPS = 1e-06
DECAY_SCALE = 8.0
MESH = pl.DeviceIdType.MESH
EDGE = 16
BF = jnp.bfloat16
F32 = jnp.float32
VM = pl.BlockSpec(memory_space=pltpu.VMEM)
DMA = pltpu.SemaphoreType.DMA


class Geometry:
    def __init__(self, n_sp, slots):
        self.n = n_sp
        self.nyc = 8 if n_sp == 64 else 2
        self.nz = n_sp // self.nyc
        self.ny = self.nyc // 2
        self.slots = slots
        self.row_a = self.nz * slots
        self.row_b = self.nyc * slots
        self.rows = n_sp * slots

    def place(self):
        sp = lax.axis_index("sp")
        return sp, lax.div(sp, self.nyc), lax.rem(sp, self.nyc), lax.axis_index("tp")


def nearest_first(n):
    order = []
    for k in range(1, n):
        for step in (k, n - k):
            if step not in order and 0 < step < n:
                order.append(step)
    return order


def send(src, dst, send_sem, recv_sem, device):
    copy = pltpu.make_async_remote_copy(
        src_ref=src,
        dst_ref=dst,
        send_sem=send_sem,
        recv_sem=recv_sem,
        device_id=device,
        device_id_type=MESH,
    )
    copy.start()
    return copy


def arrival(dst, send_sem, recv_sem, device):
    return pltpu.make_async_remote_copy(
        src_ref=dst,
        dst_ref=dst,
        send_sem=send_sem,
        recv_sem=recv_sem,
        device_id=device,
        device_id_type=MESH,
    )


def greet(devices):
    barrier = pltpu.get_barrier_semaphore()
    for device in devices:
        pl.semaphore_signal(barrier, inc=1, device_id=device, device_id_type=MESH)
    return lambda: pl.semaphore_wait(barrier, len(devices))


def block(ref_dim, size):
    return pl.ds(pl.multiple_of(ref_dim * size, size), size)


def group_of(q, slots):
    return lax.shift_right_logical(q * (2048 // slots + 1), 11)


def shuffle_base(count, total, slots, others):
    q = lax.broadcasted_iota(jnp.int32, (count, total), 0)
    col = lax.broadcasted_iota(jnp.int32, (count, total), 1)
    return col - q - group_of(q, slots) * ((others - 1) * slots)


def picked_rows(base, target, slots, rows):
    chosen = jnp.where(base == target * slots, 1.0, 0.0).astype(BF)
    return jnp.dot(chosen, rows, preferred_element_type=F32).astype(BF)


def minus_expm1(x):
    near = 1.0 + x * (1.0 / 7.0)
    for n in (6.0, 5.0, 4.0, 3.0, 2.0):
        near = 1.0 + x * (1.0 / n) * near
    return jnp.where(x > -0.25, -x * near, 1.0 - jnp.exp(x))


def split_dot(value, matrix, dims):
    high = value.astype(BF)
    low = (value - high.astype(F32)).astype(BF)
    return lax.dot_general(high, matrix, (dims, ((), ())), preferred_element_type=F32) + lax.dot_general(
        low, matrix, (dims, ((), ())), preferred_element_type=F32
    )


def scan_rows(coef, drive, reverse):
    length = coef.shape[0]
    row = lax.broadcasted_iota(jnp.int32, coef.shape, 0)
    step = 1
    while step < length:
        if reverse:
            shift, inside = length - step, row < length - step
        else:
            shift, inside = step, row >= step
        near = jnp.where(inside, pltpu.roll(drive, shift, 0), 0.0)
        drive = coef * near + drive
        coef = coef * jnp.where(inside, pltpu.roll(coef, shift, 0), 1.0)
        step *= 2
    return coef, drive


GELU_C = 0.7978845608028654


def gelu_parts(x):
    inner = GELU_C * (x + 0.044715 * (x * x * x))
    t = jnp.tanh(inner)
    value = 0.5 * x * (1.0 + t)
    slope = 0.5 * (1.0 + t) + 0.5 * x * (1.0 - t * t) * (GELU_C * (1.0 + 3.0 * 0.044715 * (x * x)))
    return value, slope


class Carries:
    def __init__(self, geo, own, near, far, total, sems):
        self.geo, self.own, self.near, self.far, self.total = geo, own, near, far, total
        self.s1, self.r1, self.s2, self.r2 = sems
        self.sp, self.z, self.c, self.j = geo.place()
        self.y_order, self.z_order = nearest_first(geo.nyc), nearest_first(geo.nz)

    def y_peer(self, k):
        return (self.z * self.geo.nyc + lax.rem(self.c + k, self.geo.nyc), self.j)

    def z_peer(self, k):
        return (lax.rem(self.z + k, self.geo.nz) * self.geo.nyc + self.c, self.j)

    def start(self):
        self.near[self.c] = self.own[...]
        return [
            send(self.own, self.near.at[self.c], self.s1.at[k], self.r1.at[k], self.y_peer(k)) for k in self.y_order
        ]

    def combined(self, ref, count, place):
        results = []
        for side in range(2):
            shape = (2, self.own.shape[1])
            a, b = jnp.ones(shape, F32), jnp.zeros(shape, F32)
            ta, tb = a, b
            for i in range(count):
                at = i if side == 0 else count - 1 - i
                na, nb = ref[at, 2 * side : 2 * side + 2], ref[at, 4 + 2 * side : 6 + 2 * side]
                ta, tb = ta * na, na * tb + nb
                inside = (at < place) if side == 0 else (at > place)
                ma, mb = jnp.where(inside, na, 1.0), jnp.where(inside, nb, 0.0)
                a, b = a * ma, ma * b + mb
            results.append((a, b, ta, tb))
        return results

    def middle(self):
        nyc = self.geo.nyc
        for k in self.y_order:
            source = lax.rem(self.c + nyc - k, nyc)
            arrival(self.near.at[source], self.s1.at[k], self.r1.at[k], self.y_peer(k)).wait_recv()
        self.first = self.combined(self.near, nyc, self.c)
        for side in range(2):
            self.total[2 * side : 2 * side + 2] = self.first[side][2]
            self.total[4 + 2 * side : 6 + 2 * side] = self.first[side][3]
        self.far[self.z] = self.total[...]
        return [
            send(self.total, self.far.at[self.z], self.s2.at[k], self.r2.at[k], self.z_peer(k)) for k in self.z_order
        ]

    def end(self):
        nz = self.geo.nz
        for k in self.z_order:
            source = lax.rem(self.z + nz - k, nz)
            arrival(self.far.at[source], self.s2.at[k], self.r2.at[k], self.z_peer(k)).wait_recv()
        second = self.combined(self.far, nz, self.z)
        return [self.first[side][0] * second[side][1] + self.first[side][1] for side in range(2)]


def wire(src, dst, send_sem, recv_sem, device):
    return pltpu.make_async_remote_copy(
        src_ref=src, dst_ref=dst, send_sem=send_sem, recv_sem=recv_sem, device_id=device, device_id_type=MESH
    )


def across(a, b):
    return lax.dot_general(a, b, (((1,), (1,)), ((), ())), preferred_element_type=F32)


def slot_rows(geo, cot_ref, x_ref, routes_ref, weight_ref, s_ref, pt_ref):
    length, width = x_ref.shape
    fourth = width // 4
    x32 = x_ref[...].astype(F32)
    inv_rms = lax.rsqrt(jnp.mean(x32 * x32, axis=1, keepdims=True) + EPS)
    first = pl.multiple_of(lax.axis_index("tp") * fourth, fourth)
    own_x = (x_ref[:, pl.ds(first, fourth)].astype(F32) * inv_rms).astype(BF)
    own_cot = cot_ref[:, pl.ds(first, fourth)].astype(F32)
    row = lax.broadcasted_iota(jnp.int32, (length, length), 0)
    col = lax.broadcasted_iota(jnp.int32, (length, length), 1)
    before = jnp.where(row < col, 1.0, 0.0).astype(BF)
    expert = lax.broadcasted_iota(jnp.int32, (geo.n, length), 0)
    place_row = lax.broadcasted_iota(jnp.int32, (geo.rows, length), 0).astype(F32)
    place_col = lax.broadcasted_iota(jnp.int32, (length, geo.rows), 1).astype(F32)
    shift = geo.nyc.bit_length() - 1

    def upright(line):
        return jnp.sum(jnp.where(row == col, line, 0.0), axis=1, keepdims=True)

    count = jnp.zeros((geo.n, 1), F32)
    sums = None
    for k in range(2):
        routes = routes_ref[k : k + 1, :]
        named = jnp.where(expert == routes, 1.0, 0.0)
        earlier = jnp.dot(named.astype(BF), before, preferred_element_type=F32) + count
        count = count + jnp.sum(named, axis=1, keepdims=True)
        rank = jnp.sum(earlier * named, axis=0, keepdims=True)
        seat = (routes & (geo.nyc - 1)) * geo.nz + lax.shift_right_logical(routes, shift)
        target = (seat * geo.slots).astype(F32) + rank
        chosen = jnp.where(place_row == target, 1.0, 0.0).astype(BF)
        pt_ref[k * length : (k + 1) * length, :] = jnp.where(place_col == upright(target), 1.0, 0.0).astype(BF)
        scaled = (upright(weight_ref[k : k + 1, :]) * own_cot).astype(BF)
        part = (
            jnp.dot(chosen, own_x, preferred_element_type=F32),
            jnp.dot(chosen, scaled, preferred_element_type=F32),
        )
        sums = part if sums is None else (sums[0] + part[0], sums[1] + part[1])
    s_ref[:, :fourth] = sums[0].astype(BF)
    s_ref[:, fourth:] = sums[1].astype(BF)


def softplus_of_minus(p):
    u = jnp.exp(-p)
    series = u * (1.0 - u * (0.5 - u * (1.0 / 3.0 - u * (0.25 - u * (0.2 - u * (1.0 / 6.0))))))
    return jnp.where(u < 0.03, series, jnp.log(1.0 + u))


def spread_blocks(map_value):
    size = map_value.shape[0]
    row = lax.broadcasted_iota(jnp.int32, (64, size), 0)
    col = lax.broadcasted_iota(jnp.int32, (64, size), 1)
    tiled = jnp.dot(map_value, jnp.where((col & 63) == row, 1.0, 0.0).astype(BF), preferred_element_type=F32)
    row = lax.shift_right_logical(lax.broadcasted_iota(jnp.int32, (size, size), 0), 6)
    col = lax.shift_right_logical(lax.broadcasted_iota(jnp.int32, (size, size), 1), 6)
    return jnp.where(row == col, tiled, 0.0).astype(BF)


SAVED = 15


def layer_kernel(
    geo, cot_ref, x_ref, routes_ref, weight_ref, ci_ref, gb_ref, taps_ref, recur_ref, input_ref, decay_ref, shift_ref,
    wg_hbm, wu_hbm, wd_hbm, op_hbm,
    xin_hbm, xsc_hbm, hid_ref, gg_ref, ug_ref, out_ref, ig_ref, bg_ref,
    s_ref, pt_ref, wg_ref, wu_ref, wd_ref, op_ref, xin_ref, xsc_ref, halo_ref, ng_ref,
    got, mid, p_ref, thru, direct, comb, fin, share, z_got, y_out, back,
    sv, maps_ref, big, mo_ref, mgb_ref, go_ref, cgb_ref, half, quarter, r1, r2, r3, halo, car, near, far, total,
    load, store, sa, ra, sb, rb, sc, rc, sh, rh, sx, rx, sz, rz, sy, ry, sg, rg,
    s1, q1, s2, q2, s3, q3, su, ru, e1, f1, e2, f2,
):
    nz, ny, nyc, slots, row_a, row_b = geo.nz, geo.ny, geo.nyc, geo.slots, geo.row_a, geo.row_b
    sp, z, c, j = geo.place()
    w = s_ref.shape[1] // 2
    hw = w // 2
    right, left, opposite = lax.rem(j + 1, 4), lax.rem(j + 3, 4), lax.rem(j + 2, 4)
    length = ci_ref.shape[0]
    last = length - 1
    full = (xin_ref, xsc_ref)
    after, ahead = lax.rem(sp + 1, geo.n), lax.rem(sp + geo.n - 1, geo.n)
    y_order, z_order = nearest_first(nyc), nearest_first(nz)
    has_low = jnp.where(sp > 0, 1.0, 0.0)
    has_high = jnp.where(sp < geo.n - 1, 1.0, 0.0)

    def turn(i):
        if isinstance(i, int):
            return ([0] + z_order)[i]
        return jnp.where(lax.rem(i, 2) == 1, lax.div(i + 1, 2), lax.rem(nz - lax.div(i, 2), nz))

    def y_peer(k):
        return (z * nyc + lax.rem(c + k, nyc), j)

    def z_at(k):
        return lax.rem(z + k, nz)

    def z_from(k):
        return lax.rem(z + nz - k, nz)

    def z_peer(k):
        return (z_at(k) * nyc + c, j)

    def columns(column, offset=0):
        return pl.multiple_of(column * w + offset, hw)

    met = greet(
        [y_peer(k) for k in y_order]
        + [z_peer(k) for k in z_order]
        + [(sp, right), (sp, left), (after, j), (ahead, j)]
    )
    loads = [
        pltpu.make_async_copy(src, dst, load.at[n])
        for n, (src, dst) in enumerate(((wg_hbm, wg_ref), (wu_hbm, wu_ref), (wd_hbm, wd_ref), (op_hbm, op_ref)))
    ]
    for copy in loads:
        copy.start()
    slot_rows(geo, cot_ref, x_ref, routes_ref, weight_ref, s_ref, pt_ref)
    base = shuffle_base(row_b, geo.rows, slots, nz)
    edges = [
        wire(ci_ref.at[pl.ds(length - EDGE, EDGE)], halo_ref.at[pl.ds(0, EDGE)], sh.at[0], rh.at[0], (after, j)),
        wire(ci_ref.at[pl.ds(0, EDGE)], halo_ref.at[pl.ds(EDGE, EDGE)], sh.at[1], rh.at[1], (ahead, j)),
    ]

    def y_copy(h, k):
        return wire(
            s_ref.at[block(lax.rem(c + k, nyc), row_a), pl.ds(h * w, w)],
            got.at[block(c, row_a), pl.ds(h * w, w)],
            sa.at[h, k],
            ra.at[h, k],
            y_peer(k),
        )

    met()
    for copy in edges:
        copy.start()
    for h in range(2):
        for k in y_order:
            y_copy(h, k).start()
    got[block(c, row_a), :] = s_ref[block(c, row_a), :]

    def surround(low, middle, high):
        big[0:EDGE] = low.astype(F32) * has_low
        big[EDGE : EDGE + length] = middle
        big[EDGE + length :] = high.astype(F32) * has_high

    taps = taps_ref[...].astype(F32)
    rate = softplus_of_minus(decay_ref[...])
    for d in range(2):
        maps_ref[2 * d] = spread_blocks(recur_ref[d])
        maps_ref[2 * d + 1] = spread_blocks(input_ref[d])
    value, slope = gelu_parts(gb_ref[...].astype(F32))
    sv[13] = value
    sv[14] = slope
    for e in range(2):
        arrival(halo_ref.at[pl.ds(e * EDGE, EDGE)], sh.at[e], rh.at[e], (after, j)).wait_recv()
    surround(halo_ref[0:EDGE], ci_ref[...].astype(F32), halo_ref[EDGE:])
    conv = jnp.zeros(ci_ref.shape, F32)
    for o in range(4):
        conv = conv + big[EDGE - 2 + o : EDGE - 2 + o + length] * taps[o : o + 1, :]
    sv[0] = conv
    forward, backward = [
        Carries(geo, car.at[i], near.at[i], far.at[i], total.at[i], (e1.at[i], f1.at[i], e2.at[i], f2.at[i]))
        for i in range(2)
    ]
    for d in range(2):
        recur = jax.nn.sigmoid(split_dot(conv, maps_ref[2 * d], ((1,), (0,))))
        inputs = jax.nn.sigmoid(split_dot(conv, maps_ref[2 * d + 1], ((1,), (0,))))
        log_decay = -DECAY_SCALE * recur * rate[d : d + 1, :] + shift_ref[d]
        coef = jnp.exp(log_decay)
        root = jnp.sqrt(minus_expm1(2.0 * log_decay))
        for n, item in enumerate((recur, inputs, coef, root)):
            sv[1 + 4 * d + n] = item
        cum, state = scan_rows(coef, root * (inputs * conv), d == 1)
        sv[9 + 2 * d] = cum
        sv[10 + 2 * d] = state

    def fill(ref, sums):
        products = (sv[9, last:], sv[11, 0:1], sv[11, 0:1], sv[9, last:])
        for n, item in enumerate(products + sums):
            ref[n : n + 1, :] = item

    zero = jnp.zeros((1, ci_ref.shape[1]), F32)
    fill(car.at[0], (sv[10, last:], zero, sv[12, 0:1], zero))

    def z_copy(h, k):
        own = full[h].at[block(z, row_b), pl.ds(columns(j), w)]
        return wire(mid.at[h, k], own, sb.at[h, k], rb.at[h, k], z_peer(k))

    def exchange_z(h, ready):
        for k in y_order:
            source = lax.rem(c + nyc - k, nyc)
            arrival(got.at[block(source, row_a), pl.ds(h * w, w)], sa.at[h, k], ra.at[h, k], y_peer(k)).wait_recv()
        rows = got[:, h * w : (h + 1) * w]
        for n, k in enumerate(z_order):
            mid[h, k] = picked_rows(base, z_at(k), slots, rows)
            if 0 < n <= len(ready):
                z_copy(h, ready[n - 1]).start()
        full[h][block(z, row_b), pl.ds(columns(j), w)] = picked_rows(base, z, slots, rows)
        for k in ready[len(z_order) - 1 :]:
            z_copy(h, k).start()

    def part(h, i, column, size, offset=0):
        return full[h].at[block(z_from(turn(i)), row_b), pl.ds(columns(column, offset), size)]

    def x_copy(h, i, kind):
        ref = (
            lambda: part(h, i, j, w),
            lambda: part(h, i, j, w),
            lambda: part(h, i, left, hw),
            lambda: part(h, i, right, hw, hw),
        )[kind]()
        return wire(ref, ref, sc.at[h, i, kind], rc.at[h, i, kind], (sp, left if kind % 2 else right))

    def x_landed(h, i, kind):
        ref = (
            lambda: part(h, i, left, w),
            lambda: part(h, i, right, w),
            lambda: part(h, i, opposite, hw),
            lambda: part(h, i, opposite, hw, hw),
        )[kind]()
        arrival(ref, sc.at[h, i, kind], rc.at[h, i, kind], (sp, right)).wait_recv()

    def first_hop(h, i):
        if not (isinstance(i, int) and i == 0):
            k = turn(i)
            arrival(part(h, i, j, w), sb.at[h, k], rb.at[h, k], z_peer(k)).wait_recv()
        x_copy(h, i, 0).start()
        x_copy(h, i, 1).start()

    def second_hop(h, i):
        for side in range(2):
            x_landed(h, i, side)
            x_copy(h, i, 2 + side).start()

    def compute(i):
        for h in range(2):
            for kind in (2, 3):
                x_landed(h, i, kind)
        rows = block(z_from(turn(i)), row_b)
        x = xin_ref[rows, :]
        gate_pre = jnp.dot(x, wg_ref[...], preferred_element_type=F32)
        up_pre = jnp.dot(x, wu_ref[...], preferred_element_type=F32)
        hidden_grad = across(xsc_ref[rows, :], wd_ref[...])
        gate_sig = jax.nn.sigmoid(gate_pre)
        gate_act = gate_pre * gate_sig
        hid_ref[rows, :] = (gate_act * up_pre).astype(BF)
        gate_grad = (hidden_grad * up_pre * gate_sig * (1.0 + gate_pre * (1.0 - gate_sig))).astype(BF)
        up_grad = (hidden_grad * gate_act).astype(BF)
        gg_ref[rows, :] = gate_grad
        ug_ref[rows, :] = up_grad
        for q in range(4):
            cut = pl.ds(q * w, w)
            p_ref[i, :, cut] = (across(gate_grad, wg_ref[cut, :]) + across(up_grad, wu_ref[cut, :])).astype(BF)

    def piece(i, column, offset):
        return p_ref.at[i, :, pl.ds(columns(column, offset), hw)]

    def s_copy(i, kind):
        src, dst = (
            lambda: (piece(i, opposite, 0), thru.at[i, 0]),
            lambda: (piece(i, opposite, hw), thru.at[i, 1]),
            lambda: (piece(i, right, hw), direct.at[i, 0]),
            lambda: (piece(i, left, 0), direct.at[i, 1]),
            lambda: (comb.at[i, 0], fin.at[i, 0]),
            lambda: (comb.at[i, 1], fin.at[i, 1]),
        )[kind]()
        return wire(src, dst, sx.at[i, kind], rx.at[i, kind], (sp, left if kind % 2 else right))

    def s_landed(ref, i, kind):
        arrival(ref, sx.at[i, kind], rx.at[i, kind], (sp, left)).wait_recv()

    def spread(i):
        for kind in range(4):
            s_copy(i, kind).start()

    def combine(i):
        s_landed(thru.at[i, 0], i, 0)
        comb[i, 0] = (piece(i, right, 0)[...].astype(F32) + thru[i, 0].astype(F32)).astype(BF)
        s_landed(thru.at[i, 1], i, 1)
        comb[i, 1] = (piece(i, left, hw)[...].astype(F32) + thru[i, 1].astype(F32)).astype(BF)

    def pass_on(i):
        s_copy(i, 4).start()
        s_copy(i, 5).start()

    def finish(i):
        for side in range(2):
            s_landed(direct.at[i, 1 - side], i, 3 - side)
            s_landed(fin.at[i, side], i, 4 + side)
            total = (
                piece(i, j, side * hw)[...].astype(F32)
                + fin[i, side].astype(F32)
                + direct[i, 1 - side].astype(F32)
            )
            share[i, :, side * hw : (side + 1) * hw] = total.astype(BF)

    def r_copy(i):
        k = turn(i)
        return wire(
            share.at[i], z_got.at[block(z, row_b)], sz.at[k], rz.at[k], (z_from(k) * nyc + c, j)
        )

    close, distant = z_order[:4], z_order[4:]
    exchange_z(0, close)
    sent = forward.start()
    for i in range(min(3, nz)):
        first_hop(0, i)
    exchange_z(1, close)
    for n in range(0, len(distant), 2):
        for h in range(2):
            for k in distant[n : n + 2]:
                z_copy(h, k).start()
    first_hop(1, 0)
    for i in range(3, min(5, nz)):
        first_hop(0, i)
    sent += forward.middle()
    for copy in loads:
        copy.wait()
    for h, i, hop in (
        (0, 0, second_hop), (0, 1, second_hop), (1, 1, first_hop), (1, 2, first_hop), (0, 2, second_hop),
        (1, 3, first_hop), (1, 0, second_hop), (1, 1, second_hop),
    ):
        if i < nz:
            hop(h, i)

    def step(t, _):
        for lead, hop, h in ((5, first_hop, 0), (4, first_hop, 1), (3, second_hop, 0), (2, second_hop, 1)):

            @pl.when(t + lead < nz)
            def _(lead=lead, hop=hop, h=h):
                hop(h, t + lead)

        @pl.when(t < nz)
        def _():
            compute(t)

        @pl.when((t >= 1) & (t < nz + 1))
        def _():
            combine(t - 1)

        @pl.when(t < nz)
        def _():
            spread(t)

        @pl.when(t >= 2)
        def _():
            finish(t - 2)

        @pl.when((t >= 1) & (t < nz + 1))
        def _():
            pass_on(t - 1)

        @pl.when(t >= 3)
        def _():
            r_copy(t - 2).start()

        return 0

    lax.fori_loop(0, nz + 2, step, 0)
    z_got[block(z, row_b), :] = share[0]
    stores = [
        pltpu.make_async_copy(src, dst, store.at[n]) for n, (src, dst) in enumerate(((xin_ref, xin_hbm), (xsc_ref, xsc_hbm)))
    ]
    for copy in stores:
        copy.start()
    low, high = forward.end()
    low_f, up_b = low[0:1], high[0:1]
    state_f = sv[10] + sv[9] * low_f
    state_b = sv[12] + sv[11] * up_b
    sv[10] = state_f
    sv[12] = state_b
    mo_ref[...] = (sv[13] * (state_f + state_b)).astype(BF)
    base = shuffle_base(row_a, geo.rows, slots, nyc)
    for k in z_order:
        arrival(z_got.at[block(z_at(k), row_b)], sz.at[k], rz.at[k], z_peer(k)).wait_recv()
    rows = z_got[...]

    def b_copy(k):
        return wire(y_out.at[k], back.at[block(c, row_a)], sy.at[k], ry.at[k], y_peer(k))

    held = None
    for k in y_order:
        y_out[k] = picked_rows(base, lax.rem(c + k, nyc), slots, rows)
        if held is not None:
            b_copy(held).start()
        held = k
    back[block(c, row_a), :] = picked_rows(base, c, slots, rows)
    b_copy(held).start()
    for k in y_order:
        source = lax.rem(c + nyc - k, nyc)
        arrival(back.at[block(source, row_a)], sy.at[k], ry.at[k], y_peer(k)).wait_recv()
    picked = jnp.dot(pt_ref[...], back[...], preferred_element_type=F32)
    ng_ref[:, pl.ds(columns(j), w)] = (picked[:length] + picked[length : 2 * length]).astype(BF)

    def g_part(column, size, offset=0):
        return ng_ref.at[:, pl.ds(columns(column, offset), size)]

    gathers = [
        wire(g_part(j, w), g_part(j, w), sg.at[0], rg.at[0], (sp, right)),
        wire(g_part(j, w), g_part(j, w), sg.at[1], rg.at[1], (sp, left)),
        wire(g_part(left, hw), g_part(left, hw), sg.at[2], rg.at[2], (sp, right)),
        wire(g_part(right, hw, hw), g_part(right, hw, hw), sg.at[3], rg.at[3], (sp, left)),
    ]
    gathers[0].start()
    gathers[1].start()
    arrival(g_part(left, w), sg.at[0], rg.at[0], (sp, left)).wait_recv()
    gathers[2].start()
    arrival(g_part(right, w), sg.at[1], rg.at[1], (sp, right)).wait_recv()
    gathers[3].start()
    arrival(g_part(opposite, hw), sg.at[2], rg.at[2], (sp, left)).wait_recv()
    arrival(g_part(opposite, hw, hw), sg.at[3], rg.at[3], (sp, right)).wait_recv()

    x32 = x_ref[...].astype(F32)
    inv_rms = lax.rsqrt(jnp.mean(x32 * x32, axis=1, keepdims=True) + EPS)
    normed = x32 * inv_rms
    ng = ng_ref[...].astype(F32)
    mean = jnp.mean(ng * normed, axis=1, keepdims=True)
    mgb_ref[...] = (cot_ref[...].astype(F32) + inv_rms * (ng - normed * mean)).astype(BF)
    go = lax.dot_general(mgb_ref[...], mo_ref[...], (((0,), (0,)), ((), ())), preferred_element_type=F32)
    go_ref[...] = go.astype(BF).reshape(go_ref.shape)
    out_grad = jnp.dot(mgb_ref[...], op_ref[...], preferred_element_type=F32)
    carried = out_grad * sv[13]
    cum_bf, after_b = scan_rows(sv[7], sv[7] * carried, False)
    y, core = lax.div(c, 2), lax.rem(c, 2)
    partner = (z * nyc + y * 2 + (1 - core), j)
    yy_order = nearest_first(ny)

    def yy_peer(k):
        return (z * nyc + lax.rem(y + k, ny) * 2 + core, j)

    sent.append(send(go_ref.at[:, :, 1 - core], r1, s1, q1, partner))
    cum_fr, after_f = scan_rows(sv[3], sv[3] * carried, True)
    fill(car.at[1], (zero, after_b[last:], zero, after_f[0:1]))
    states = sv[10] + sv[12]
    bg_ref[...] = (out_grad * states * sv[14]).astype(BF)
    sent += backward.start()
    arrival(r1, s1, q1, partner).wait_recv()
    for k in yy_order + [0]:
        at = lax.rem(y + k, ny)
        half[k] = (go_ref[:, at, core].astype(F32) + r1[:, at].astype(F32)).astype(BF)
    sent += backward.middle()
    for k in yy_order:
        sent.append(send(half.at[k], r2.at[k], s2.at[k], q2.at[k], yy_peer(k)))
    row = lax.broadcasted_iota(jnp.int32, ci_ref.shape, 0)

    def from_before(item, carry):
        return jnp.where(row == 0, carry, pltpu.roll(item, 1, 0))

    def from_after(item, carry):
        return jnp.where(row == last, carry, pltpu.roll(item, length - 1, 0))

    others = (from_before(sv[10], low_f), from_after(sv[12], up_b))
    low, high = backward.end()
    low_b, up_f = low[1:2], high[1:2]
    after_b = after_b + cum_bf * low_b
    after_f = after_f + cum_fr * up_f
    adjoints = (carried + from_after(after_f, up_f), carried + from_before(after_b, low_b))
    conv = sv[0]
    conv_grad = jnp.zeros(ci_ref.shape, F32)
    for d in range(2):
        recur, inputs, coef, root = [sv[1 + 4 * d + n] for n in range(4)]
        adjoint = adjoints[d]
        log_grad = adjoint * others[d] * coef - adjoint * (inputs * conv) * (coef * coef) / root
        recur_grad = log_grad * (-DECAY_SCALE * rate[d : d + 1, :]) * recur * (1.0 - recur)
        input_grad = adjoint * root * conv * inputs * (1.0 - inputs)
        conv_grad = conv_grad + adjoint * root * inputs
        conv_grad = conv_grad + split_dot(recur_grad, maps_ref[2 * d], ((1,), (1,)))
        conv_grad = conv_grad + split_dot(input_grad, maps_ref[2 * d + 1], ((1,), (1,)))
    cgb_ref[...] = conv_grad.astype(BF)
    for k in yy_order:
        arrival(r2.at[k], s2.at[k], q2.at[k], yy_peer(k)).wait_recv()
    sent.append(send(cgb_ref.at[pl.ds(length - EDGE, EDGE)], halo.at[pl.ds(0, EDGE)], su.at[0], ru.at[0], (after, j)))
    sent.append(send(cgb_ref.at[pl.ds(0, EDGE)], halo.at[pl.ds(EDGE, EDGE)], su.at[1], ru.at[1], (ahead, j)))
    for k in z_order + [0]:
        at = z_at(k)
        summed = half[0, at].astype(F32)
        for m in yy_order:
            summed = summed + r2[m, at].astype(F32)
        quarter[k] = summed.astype(BF)
    for k in z_order:
        sent.append(send(quarter.at[k], r3.at[k], s3.at[k], q3.at[k], z_peer(k)))
    for e in range(2):
        arrival(halo.at[pl.ds(e * EDGE, EDGE)], su.at[e], ru.at[e], (after, j)).wait_recv()
    surround(halo[0:EDGE], conv_grad, halo[EDGE:])
    grad = jnp.zeros(ci_ref.shape, F32)
    for o in range(4):
        grad = grad + big[EDGE + 2 - o : EDGE + 2 - o + length] * taps[o : o + 1, :]
    ig_ref[...] = grad.astype(BF)
    result = quarter[0].astype(F32)
    for k in z_order:
        arrival(r3.at[k], s3.at[k], q3.at[k], z_peer(k)).wait_recv()
        result = result + r3[k].astype(F32)
    out_ref[...] = result

    def drain(i, _):
        for h in range(2):
            for kind in range(4):
                x_copy(h, i, kind).wait_send()
        for kind in range(6):
            s_copy(i, kind).wait_send()
        return 0

    lax.fori_loop(0, nz, drain, 0)
    for k in y_order:
        y_copy(0, k).wait_send()
        y_copy(1, k).wait_send()
        b_copy(k).wait_send()
    for i in range(1, nz):
        r_copy(i).wait_send()
        z_copy(0, z_order[i - 1]).wait_send()
        z_copy(1, z_order[i - 1]).wait_send()
    for copy in edges + gathers + sent:
        copy.wait_send()
    for copy in stores:
        copy.wait()


def shards(
    cotangent,
    saved_input,
    routes,
    route_weight,
    gate_proj,
    up_proj,
    down_proj,
    out_proj,
    conv_input,
    gate_branch,
    conv_taps,
    recur_map,
    input_map,
    decay_param,
    decay_shift,
):
    length, width = cotangent.shape
    n_sp = lax.axis_size("sp")
    geo = Geometry(n_sp, 4 * length // n_sp)
    nz, ny, nyc, rows = geo.nz, geo.ny, geo.nyc, geo.rows
    w = width // 4
    hidden_units = gate_proj.shape[2]
    channels = conv_input.shape[1]
    part = width // n_sp
    own = (length, channels)
    half = (nz, 2, geo.row_b, w // 2)
    carry = (8, channels)
    shape = jax.ShapeDtypeStruct
    wide, narrow = shape((rows, width), BF), shape((rows, hidden_units), BF)
    anywhere = pl.BlockSpec(memory_space=pl.ANY)

    def vmem(dims, kind=BF):
        return pltpu.VMEM(dims, kind)

    rows_input, rows_scaled, hidden, gate_grad, up_grad, grad_out, input_grad, branch_grad = pl.pallas_call(
        functools.partial(layer_kernel, geo),
        out_shape=(wide, wide, narrow, narrow, narrow, shape((part, channels), F32), shape(own, BF), shape(own, BF)),
        in_specs=[VM] * 11 + [anywhere] * 4,
        out_specs=(anywhere,) * 2 + (VM,) * 6,
        scratch_shapes=[
            vmem((rows, 2 * w)),
            vmem((2 * length, rows)),
            vmem(gate_proj.shape[1:]),
            vmem(up_proj.shape[1:]),
            vmem(down_proj.shape[1:]),
            vmem(out_proj.shape),
            vmem((rows, width)),
            vmem((rows, width)),
            vmem((2 * EDGE, channels)),
            vmem((length, width)),
            vmem((rows, 2 * w)),
            vmem((2, nz, geo.row_b, w)),
            vmem((nz, geo.row_b, width)),
            vmem(half),
            vmem(half),
            vmem(half),
            vmem(half),
            vmem((nz, geo.row_b, w)),
            vmem((rows, w)),
            vmem((nyc, geo.row_a, w)),
            vmem((rows, w)),
            vmem((SAVED, *own), F32),
            vmem((4, channels, channels)),
            vmem((length + 2 * EDGE, channels), F32),
            vmem(own),
            vmem((length, width)),
            vmem((nz, ny, 2, part, channels)),
            vmem(own),
            vmem((ny, nz, part, channels)),
            vmem((nz, part, channels)),
            vmem((nz, ny, part, channels)),
            vmem((ny, nz, part, channels)),
            vmem((nz, part, channels)),
            vmem((2 * EDGE, channels)),
            vmem((2, *carry), F32),
            vmem((2, nyc, *carry), F32),
            vmem((2, nz, *carry), F32),
            vmem((2, *carry), F32),
            DMA((4,)),
            DMA((2,)),
            DMA((2, nyc)),
            DMA((2, nyc)),
            DMA((2, nz)),
            DMA((2, nz)),
            DMA((2, nz, 4)),
            DMA((2, nz, 4)),
            DMA((2,)),
            DMA((2,)),
            DMA((nz, 6)),
            DMA((nz, 6)),
            DMA((nz,)),
            DMA((nz,)),
            DMA((nyc,)),
            DMA((nyc,)),
            DMA((4,)),
            DMA((4,)),
            DMA,
            DMA,
            DMA((ny,)),
            DMA((ny,)),
            DMA((nz,)),
            DMA((nz,)),
            DMA((2,)),
            DMA((2,)),
            DMA((2, nyc)),
            DMA((2, nyc)),
            DMA((2, nz)),
            DMA((2, nz)),
        ],
        compiler_params=pltpu.CompilerParams(
            collective_id=1, has_side_effects=True, vmem_limit_bytes=60 * 2**20
        ),
    )(
        cotangent,
        saved_input,
        routes.T,
        route_weight.T,
        conv_input,
        gate_branch,
        conv_taps,
        recur_map.reshape(2, channels, 64),
        input_map.reshape(2, channels, 64),
        decay_param,
        decay_shift,
        gate_proj[0],
        up_proj[0],
        down_proj[0],
        out_proj,
    )
    over_rows = (((0,), (0,)), ((), ()))
    grad_down = lax.dot_general(hidden, rows_scaled, over_rows, preferred_element_type=F32)
    grad_gate = lax.dot_general(rows_input, gate_grad, over_rows, preferred_element_type=F32)
    grad_up = lax.dot_general(rows_input, up_grad, over_rows, preferred_element_type=F32)
    return (grad_gate[None], grad_up[None], grad_down[None], grad_out, input_grad, branch_grad)


def solution(mesh):
    in_specs = (
        P("sp", None),
        P("sp", None),
        P("sp", None),
        P("sp", None),
        P("sp", None, "tp"),
        P("sp", None, "tp"),
        P("sp", "tp", None),
        P(None, "tp"),
        P("sp", "tp"),
        P("sp", "tp"),
        P(None, "tp"),
        P(None, "tp", None, None),
        P(None, "tp", None, None),
        P(None, "tp"),
        P(None, "sp", "tp"),
    )
    out_specs = (
        P("sp", None, "tp"),
        P("sp", None, "tp"),
        P("sp", "tp", None),
        P("sp", "tp"),
        P("sp", "tp"),
        P("sp", "tp"),
    )
    return jax.shard_map(shards, mesh=mesh, in_specs=in_specs, out_specs=out_specs, check_vma=False)
```

```python
import functools

import jax
import jax.numpy as jnp
from jax import lax
from jax.experimental import pallas as pl
from jax.experimental.pallas import tpu as pltpu
from jax.sharding import PartitionSpec as P

EPS = 1e-06
DECAY_SCALE = 8.0
MESH = pl.DeviceIdType.MESH
EDGE = 16
BF = jnp.bfloat16
F32 = jnp.float32
VM = pl.BlockSpec(memory_space=pltpu.VMEM)
DMA = pltpu.SemaphoreType.DMA


class Geometry:
    def __init__(self, n_sp, slots):
        self.n = n_sp
        self.nyc = 8 if n_sp == 64 else 2
        self.nz = n_sp // self.nyc
        self.ny = self.nyc // 2
        self.slots = slots
        self.row_a = self.nz * slots
        self.row_b = self.nyc * slots
        self.rows = n_sp * slots

    def place(self):
        sp = lax.axis_index("sp")
        return sp, lax.div(sp, self.nyc), lax.rem(sp, self.nyc), lax.axis_index("tp")


def nearest_first(n):
    order = []
    for k in range(1, n):
        for step in (k, n - k):
            if step not in order and 0 < step < n:
                order.append(step)
    return order


def send(src, dst, send_sem, recv_sem, device):
    copy = pltpu.make_async_remote_copy(
        src_ref=src,
        dst_ref=dst,
        send_sem=send_sem,
        recv_sem=recv_sem,
        device_id=device,
        device_id_type=MESH,
    )
    copy.start()
    return copy


def arrival(dst, send_sem, recv_sem, device):
    return pltpu.make_async_remote_copy(
        src_ref=dst,
        dst_ref=dst,
        send_sem=send_sem,
        recv_sem=recv_sem,
        device_id=device,
        device_id_type=MESH,
    )


def greet(devices):
    barrier = pltpu.get_barrier_semaphore()
    for device in devices:
        pl.semaphore_signal(barrier, inc=1, device_id=device, device_id_type=MESH)
    return lambda: pl.semaphore_wait(barrier, len(devices))


def block(ref_dim, size):
    return pl.ds(pl.multiple_of(ref_dim * size, size), size)


def group_of(q, slots):
    return lax.shift_right_logical(q * (2048 // slots + 1), 11)


def shuffle_base(count, total, slots, others):
    q = lax.broadcasted_iota(jnp.int32, (count, total), 0)
    col = lax.broadcasted_iota(jnp.int32, (count, total), 1)
    return col - q - group_of(q, slots) * ((others - 1) * slots)


def picked_rows(base, target, slots, rows):
    chosen = jnp.where(base == target * slots, 1.0, 0.0).astype(BF)
    return jnp.dot(chosen, rows, preferred_element_type=F32).astype(BF)


def minus_expm1(x):
    near = 1.0 + x * (1.0 / 7.0)
    for n in (6.0, 5.0, 4.0, 3.0, 2.0):
        near = 1.0 + x * (1.0 / n) * near
    return jnp.where(x > -0.25, -x * near, 1.0 - jnp.exp(x))


def split_dot(value, matrix, dims):
    high = value.astype(BF)
    low = (value - high.astype(F32)).astype(BF)
    return lax.dot_general(high, matrix, (dims, ((), ())), preferred_element_type=F32) + lax.dot_general(
        low, matrix, (dims, ((), ())), preferred_element_type=F32
    )


def scan_rows(coef, drive, reverse):
    length = coef.shape[0]
    row = lax.broadcasted_iota(jnp.int32, coef.shape, 0)
    step = 1
    while step < length:
        if reverse:
            shift, inside = length - step, row < length - step
        else:
            shift, inside = step, row >= step
        near = jnp.where(inside, pltpu.roll(drive, shift, 0), 0.0)
        drive = coef * near + drive
        coef = coef * jnp.where(inside, pltpu.roll(coef, shift, 0), 1.0)
        step *= 2
    return coef, drive


GELU_C = 0.7978845608028654


def gelu_parts(x):
    inner = GELU_C * (x + 0.044715 * (x * x * x))
    t = jnp.tanh(inner)
    value = 0.5 * x * (1.0 + t)
    slope = 0.5 * (1.0 + t) + 0.5 * x * (1.0 - t * t) * (GELU_C * (1.0 + 3.0 * 0.044715 * (x * x)))
    return value, slope


class Carries:
    def __init__(self, geo, own, near, far, total, sems):
        self.geo, self.own, self.near, self.far, self.total = geo, own, near, far, total
        self.s1, self.r1, self.s2, self.r2 = sems
        self.sp, self.z, self.c, self.j = geo.place()
        self.y_order, self.z_order = nearest_first(geo.nyc), nearest_first(geo.nz)

    def y_peer(self, k):
        return (self.z * self.geo.nyc + lax.rem(self.c + k, self.geo.nyc), self.j)

    def z_peer(self, k):
        return (lax.rem(self.z + k, self.geo.nz) * self.geo.nyc + self.c, self.j)

    def start(self):
        self.near[self.c] = self.own[...]
        return [
            send(self.own, self.near.at[self.c], self.s1.at[k], self.r1.at[k], self.y_peer(k)) for k in self.y_order
        ]

    def combined(self, ref, count, place):
        results = []
        for side in range(2):
            shape = (2, self.own.shape[1])
            a, b = jnp.ones(shape, F32), jnp.zeros(shape, F32)
            ta, tb = a, b
            for i in range(count):
                at = i if side == 0 else count - 1 - i
                na, nb = ref[at, 2 * side : 2 * side + 2], ref[at, 4 + 2 * side : 6 + 2 * side]
                ta, tb = ta * na, na * tb + nb
                inside = (at < place) if side == 0 else (at > place)
                ma, mb = jnp.where(inside, na, 1.0), jnp.where(inside, nb, 0.0)
                a, b = a * ma, ma * b + mb
            results.append((a, b, ta, tb))
        return results

    def middle(self):
        nyc = self.geo.nyc
        for k in self.y_order:
            source = lax.rem(self.c + nyc - k, nyc)
            arrival(self.near.at[source], self.s1.at[k], self.r1.at[k], self.y_peer(k)).wait_recv()
        self.first = self.combined(self.near, nyc, self.c)
        for side in range(2):
            self.total[2 * side : 2 * side + 2] = self.first[side][2]
            self.total[4 + 2 * side : 6 + 2 * side] = self.first[side][3]
        self.far[self.z] = self.total[...]
        return [
            send(self.total, self.far.at[self.z], self.s2.at[k], self.r2.at[k], self.z_peer(k)) for k in self.z_order
        ]

    def end(self):
        nz = self.geo.nz
        for k in self.z_order:
            source = lax.rem(self.z + nz - k, nz)
            arrival(self.far.at[source], self.s2.at[k], self.r2.at[k], self.z_peer(k)).wait_recv()
        second = self.combined(self.far, nz, self.z)
        return [self.first[side][0] * second[side][1] + self.first[side][1] for side in range(2)]


def wire(src, dst, send_sem, recv_sem, device):
    return pltpu.make_async_remote_copy(
        src_ref=src, dst_ref=dst, send_sem=send_sem, recv_sem=recv_sem, device_id=device, device_id_type=MESH
    )


def across(a, b):
    return lax.dot_general(a, b, (((1,), (1,)), ((), ())), preferred_element_type=F32)


def slot_rows(geo, cot_ref, x_ref, routes_ref, weight_ref, s_ref, pt_ref):
    length, width = x_ref.shape
    fourth = width // 4
    x32 = x_ref[...].astype(F32)
    inv_rms = lax.rsqrt(jnp.mean(x32 * x32, axis=1, keepdims=True) + EPS)
    first = pl.multiple_of(lax.axis_index("tp") * fourth, fourth)
    own_x = (x_ref[:, pl.ds(first, fourth)].astype(F32) * inv_rms).astype(BF)
    own_cot = cot_ref[:, pl.ds(first, fourth)].astype(F32)
    row = lax.broadcasted_iota(jnp.int32, (length, length), 0)
    col = lax.broadcasted_iota(jnp.int32, (length, length), 1)
    before = jnp.where(row < col, 1.0, 0.0).astype(BF)
    expert = lax.broadcasted_iota(jnp.int32, (geo.n, length), 0)
    place_row = lax.broadcasted_iota(jnp.int32, (geo.rows, length), 0).astype(F32)
    place_col = lax.broadcasted_iota(jnp.int32, (length, geo.rows), 1).astype(F32)
    shift = geo.nyc.bit_length() - 1

    def upright(line):
        return jnp.sum(jnp.where(row == col, line, 0.0), axis=1, keepdims=True)

    count = jnp.zeros((geo.n, 1), F32)
    sums = None
    for k in range(2):
        routes = routes_ref[k : k + 1, :]
        named = jnp.where(expert == routes, 1.0, 0.0)
        earlier = jnp.dot(named.astype(BF), before, preferred_element_type=F32) + count
        count = count + jnp.sum(named, axis=1, keepdims=True)
        rank = jnp.sum(earlier * named, axis=0, keepdims=True)
        seat = (routes & (geo.nyc - 1)) * geo.nz + lax.shift_right_logical(routes, shift)
        target = (seat * geo.slots).astype(F32) + rank
        chosen = jnp.where(place_row == target, 1.0, 0.0).astype(BF)
        pt_ref[k * length : (k + 1) * length, :] = jnp.where(place_col == upright(target), 1.0, 0.0).astype(BF)
        scaled = (upright(weight_ref[k : k + 1, :]) * own_cot).astype(BF)
        part = (
            jnp.dot(chosen, own_x, preferred_element_type=F32),
            jnp.dot(chosen, scaled, preferred_element_type=F32),
        )
        sums = part if sums is None else (sums[0] + part[0], sums[1] + part[1])
    s_ref[:, :fourth] = sums[0].astype(BF)
    s_ref[:, fourth:] = sums[1].astype(BF)


def softplus_of_minus(p):
    u = jnp.exp(-p)
    series = u * (1.0 - u * (0.5 - u * (1.0 / 3.0 - u * (0.25 - u * (0.2 - u * (1.0 / 6.0))))))
    return jnp.where(u < 0.03, series, jnp.log(1.0 + u))


def spread_blocks(map_value):
    size = map_value.shape[0]
    row = lax.broadcasted_iota(jnp.int32, (64, size), 0)
    col = lax.broadcasted_iota(jnp.int32, (64, size), 1)
    tiled = jnp.dot(map_value, jnp.where((col & 63) == row, 1.0, 0.0).astype(BF), preferred_element_type=F32)
    row = lax.shift_right_logical(lax.broadcasted_iota(jnp.int32, (size, size), 0), 6)
    col = lax.shift_right_logical(lax.broadcasted_iota(jnp.int32, (size, size), 1), 6)
    return jnp.where(row == col, tiled, 0.0).astype(BF)


SAVED = 15


def layer_kernel(
    geo, cot_ref, x_ref, routes_ref, weight_ref, ci_ref, gb_ref, taps_ref, recur_ref, input_ref, decay_ref, shift_ref,
    wg_hbm, wu_hbm, wd_hbm, op_hbm,
    xin_hbm, xsc_hbm, hid_hbm, gg_hbm, ug_hbm, out_ref, ig_ref, bg_ref,
    s_ref, pt_ref, wg_ref, wu_ref, wd_ref, op_ref, xin_ref, xsc_ref, hid_ref, gg_ref, ug_ref, halo_ref, ng_ref,
    got, mid, p_ref, thru, direct, comb, fin, share, z_got, y_out, back,
    sv, maps_ref, big, mo_ref, mgb_ref, go_ref, cgb_ref, half, quarter, r1, r2, r3, halo, car, near, far, total,
    load, store, sa, ra, sb, rb, sc, rc, sh, rh, sx, rx, sz, rz, sy, ry, sg, rg,
    s1, q1, s2, q2, s3, q3, su, ru, e1, f1, e2, f2,
):
    nz, ny, nyc, slots, row_a, row_b = geo.nz, geo.ny, geo.nyc, geo.slots, geo.row_a, geo.row_b
    sp, z, c, j = geo.place()
    w = s_ref.shape[1] // 2
    hw = w // 2
    right, left, opposite = lax.rem(j + 1, 4), lax.rem(j + 3, 4), lax.rem(j + 2, 4)
    length = ci_ref.shape[0]
    last = length - 1
    full = (xin_ref, xsc_ref)
    after, ahead = lax.rem(sp + 1, geo.n), lax.rem(sp + geo.n - 1, geo.n)
    y_order, z_order = nearest_first(nyc), nearest_first(nz)
    has_low = jnp.where(sp > 0, 1.0, 0.0)
    has_high = jnp.where(sp < geo.n - 1, 1.0, 0.0)

    def turn(i):
        if isinstance(i, int):
            return ([0] + z_order)[i]
        return jnp.where(lax.rem(i, 2) == 1, lax.div(i + 1, 2), lax.rem(nz - lax.div(i, 2), nz))

    def y_peer(k):
        return (z * nyc + lax.rem(c + k, nyc), j)

    def z_at(k):
        return lax.rem(z + k, nz)

    def z_from(k):
        return lax.rem(z + nz - k, nz)

    def z_peer(k):
        return (z_at(k) * nyc + c, j)

    def columns(column, offset=0):
        return pl.multiple_of(column * w + offset, hw)

    met = greet(
        [y_peer(k) for k in y_order]
        + [z_peer(k) for k in z_order]
        + [(sp, right), (sp, left), (after, j), (ahead, j)]
    )
    loads = [
        pltpu.make_async_copy(src, dst, load.at[n])
        for n, (src, dst) in enumerate(((wg_hbm, wg_ref), (wu_hbm, wu_ref), (wd_hbm, wd_ref), (op_hbm, op_ref)))
    ]
    for copy in loads:
        copy.start()
    slot_rows(geo, cot_ref, x_ref, routes_ref, weight_ref, s_ref, pt_ref)
    base = shuffle_base(row_b, geo.rows, slots, nz)
    edges = [
        wire(ci_ref.at[pl.ds(length - EDGE, EDGE)], halo_ref.at[pl.ds(0, EDGE)], sh.at[0], rh.at[0], (after, j)),
        wire(ci_ref.at[pl.ds(0, EDGE)], halo_ref.at[pl.ds(EDGE, EDGE)], sh.at[1], rh.at[1], (ahead, j)),
    ]

    def y_copy(h, k):
        return wire(
            s_ref.at[block(lax.rem(c + k, nyc), row_a), pl.ds(h * w, w)],
            got.at[block(c, row_a), pl.ds(h * w, w)],
            sa.at[h, k],
            ra.at[h, k],
            y_peer(k),
        )

    met()
    for copy in edges:
        copy.start()
    for k in y_order:
        y_copy(0, k).start()
    got[block(c, row_a), :] = s_ref[block(c, row_a), :]

    def surround(low, middle, high):
        big[0:EDGE] = low.astype(F32) * has_low
        big[EDGE : EDGE + length] = middle
        big[EDGE + length :] = high.astype(F32) * has_high

    taps = taps_ref[...].astype(F32)
    rate = softplus_of_minus(decay_ref[...])
    for d in range(2):
        maps_ref[2 * d] = spread_blocks(recur_ref[d])
        maps_ref[2 * d + 1] = spread_blocks(input_ref[d])
    value, slope = gelu_parts(gb_ref[...].astype(F32))
    sv[13] = value
    sv[14] = slope
    for e in range(2):
        arrival(halo_ref.at[pl.ds(e * EDGE, EDGE)], sh.at[e], rh.at[e], (after, j)).wait_recv()
    surround(halo_ref[0:EDGE], ci_ref[...].astype(F32), halo_ref[EDGE:])
    conv = jnp.zeros(ci_ref.shape, F32)
    for o in range(4):
        conv = conv + big[EDGE - 2 + o : EDGE - 2 + o + length] * taps[o : o + 1, :]
    sv[0] = conv
    forward, backward = [
        Carries(geo, car.at[i], near.at[i], far.at[i], total.at[i], (e1.at[i], f1.at[i], e2.at[i], f2.at[i]))
        for i in range(2)
    ]
    for d in range(2):
        recur = jax.nn.sigmoid(split_dot(conv, maps_ref[2 * d], ((1,), (0,))))
        inputs = jax.nn.sigmoid(split_dot(conv, maps_ref[2 * d + 1], ((1,), (0,))))
        log_decay = -DECAY_SCALE * recur * rate[d : d + 1, :] + shift_ref[d]
        coef = jnp.exp(log_decay)
        root = jnp.sqrt(minus_expm1(2.0 * log_decay))
        for n, item in enumerate((recur, inputs, coef, root)):
            sv[1 + 4 * d + n] = item
        cum, state = scan_rows(coef, root * (inputs * conv), d == 1)
        sv[9 + 2 * d] = cum
        sv[10 + 2 * d] = state

    def fill(ref, sums):
        products = (sv[9, last:], sv[11, 0:1], sv[11, 0:1], sv[9, last:])
        for n, item in enumerate(products + sums):
            ref[n : n + 1, :] = item

    for k in y_order:
        y_copy(1, k).start()
    zero = jnp.zeros((1, ci_ref.shape[1]), F32)
    fill(car.at[0], (sv[10, last:], zero, sv[12, 0:1], zero))

    def z_copy(h, k):
        own = full[h].at[block(z, row_b), pl.ds(columns(j), w)]
        return wire(mid.at[h, k], own, sb.at[h, k], rb.at[h, k], z_peer(k))

    def exchange_z(h, ready):
        for k in y_order:
            source = lax.rem(c + nyc - k, nyc)
            arrival(got.at[block(source, row_a), pl.ds(h * w, w)], sa.at[h, k], ra.at[h, k], y_peer(k)).wait_recv()
        rows = got[:, h * w : (h + 1) * w]
        for n, k in enumerate(z_order):
            mid[h, k] = picked_rows(base, z_at(k), slots, rows)
            if 0 < n <= len(ready):
                z_copy(h, ready[n - 1]).start()
        full[h][block(z, row_b), pl.ds(columns(j), w)] = picked_rows(base, z, slots, rows)
        for k in ready[len(z_order) - 1 :]:
            z_copy(h, k).start()

    def part(h, i, column, size, offset=0):
        return full[h].at[block(z_from(turn(i)), row_b), pl.ds(columns(column, offset), size)]

    def x_copy(h, i, kind):
        ref = (
            lambda: part(h, i, j, w),
            lambda: part(h, i, j, w),
            lambda: part(h, i, left, hw),
            lambda: part(h, i, right, hw, hw),
        )[kind]()
        return wire(ref, ref, sc.at[h, i, kind], rc.at[h, i, kind], (sp, left if kind % 2 else right))

    def x_landed(h, i, kind):
        ref = (
            lambda: part(h, i, left, w),
            lambda: part(h, i, right, w),
            lambda: part(h, i, opposite, hw),
            lambda: part(h, i, opposite, hw, hw),
        )[kind]()
        arrival(ref, sc.at[h, i, kind], rc.at[h, i, kind], (sp, right)).wait_recv()

    def first_hop(h, i):
        if not (isinstance(i, int) and i == 0):
            k = turn(i)
            arrival(part(h, i, j, w), sb.at[h, k], rb.at[h, k], z_peer(k)).wait_recv()
        x_copy(h, i, 0).start()
        x_copy(h, i, 1).start()

    def second_hop(h, i):
        for side in range(2):
            x_landed(h, i, side)
            x_copy(h, i, 2 + side).start()

    def compute(i):
        for h in range(2):
            for kind in (2, 3):
                x_landed(h, i, kind)
        rows = block(z_from(turn(i)), row_b)
        x = xin_ref[rows, :]
        gate_pre = jnp.dot(x, wg_ref[...], preferred_element_type=F32)
        up_pre = jnp.dot(x, wu_ref[...], preferred_element_type=F32)
        hidden_grad = across(xsc_ref[rows, :], wd_ref[...])
        gate_sig = jax.nn.sigmoid(gate_pre)
        gate_act = gate_pre * gate_sig
        hid_ref[rows, :] = (gate_act * up_pre).astype(BF)
        gate_grad = (hidden_grad * up_pre * gate_sig * (1.0 + gate_pre * (1.0 - gate_sig))).astype(BF)
        up_grad = (hidden_grad * gate_act).astype(BF)
        gg_ref[rows, :] = gate_grad
        ug_ref[rows, :] = up_grad
        for q in range(4):
            cut = pl.ds(q * w, w)
            p_ref[i, :, cut] = (across(gate_grad, wg_ref[cut, :]) + across(up_grad, wu_ref[cut, :])).astype(BF)

    def stores(i):
        rows = block(z_from(turn(i)), row_b)
        pairs = ((xin_ref, xin_hbm), (xsc_ref, xsc_hbm), (hid_ref, hid_hbm), (gg_ref, gg_hbm), (ug_ref, ug_hbm))
        return [
            pltpu.make_async_copy(src.at[rows], dst.at[rows], store.at[i, n]) for n, (src, dst) in enumerate(pairs)
        ]

    def piece(i, column, offset):
        return p_ref.at[i, :, pl.ds(columns(column, offset), hw)]

    def s_copy(i, kind):
        src, dst = (
            lambda: (piece(i, opposite, 0), thru.at[i, 0]),
            lambda: (piece(i, opposite, hw), thru.at[i, 1]),
            lambda: (piece(i, right, hw), direct.at[i, 0]),
            lambda: (piece(i, left, 0), direct.at[i, 1]),
            lambda: (comb.at[i, 0], fin.at[i, 0]),
            lambda: (comb.at[i, 1], fin.at[i, 1]),
        )[kind]()
        return wire(src, dst, sx.at[i, kind], rx.at[i, kind], (sp, left if kind % 2 else right))

    def s_landed(ref, i, kind):
        arrival(ref, sx.at[i, kind], rx.at[i, kind], (sp, left)).wait_recv()

    def spread(i):
        for kind in range(4):
            s_copy(i, kind).start()

    def combine(i):
        s_landed(thru.at[i, 0], i, 0)
        comb[i, 0] = (piece(i, right, 0)[...].astype(F32) + thru[i, 0].astype(F32)).astype(BF)
        s_landed(thru.at[i, 1], i, 1)
        comb[i, 1] = (piece(i, left, hw)[...].astype(F32) + thru[i, 1].astype(F32)).astype(BF)

    def pass_on(i):
        s_copy(i, 4).start()
        s_copy(i, 5).start()

    def finish(i):
        for side in range(2):
            s_landed(direct.at[i, 1 - side], i, 3 - side)
            s_landed(fin.at[i, side], i, 4 + side)
            total = (
                piece(i, j, side * hw)[...].astype(F32)
                + fin[i, side].astype(F32)
                + direct[i, 1 - side].astype(F32)
            )
            share[i, :, side * hw : (side + 1) * hw] = total.astype(BF)

    def r_copy(i):
        k = turn(i)
        return wire(
            share.at[i], z_got.at[block(z, row_b)], sz.at[k], rz.at[k], (z_from(k) * nyc + c, j)
        )

    close, distant = z_order[:4], z_order[4:]
    exchange_z(0, close)
    sent = forward.start()
    for i in range(min(3, nz)):
        first_hop(0, i)
    exchange_z(1, close)
    for n in range(0, len(distant), 2):
        for h in range(2):
            for k in distant[n : n + 2]:
                z_copy(h, k).start()
    first_hop(1, 0)
    for i in range(3, min(5, nz)):
        first_hop(0, i)
    sent += forward.middle()
    for copy in loads:
        copy.wait()
    for h, i, hop in (
        (0, 0, second_hop), (0, 1, second_hop), (1, 1, first_hop), (1, 2, first_hop), (0, 2, second_hop),
        (1, 3, first_hop), (1, 0, second_hop), (1, 1, second_hop),
    ):
        if i < nz:
            hop(h, i)

    def step(t, _):
        for lead, hop, h in ((5, first_hop, 0), (4, first_hop, 1), (3, second_hop, 0), (2, second_hop, 1)):

            @pl.when(t + lead < nz)
            def _(lead=lead, hop=hop, h=h):
                hop(h, t + lead)

        @pl.when(t < nz)
        def _():
            compute(t)

        @pl.when((t >= 1) & (t < nz + 1))
        def _():
            combine(t - 1)

        @pl.when(t < nz)
        def _():
            spread(t)
            for copy in stores(t):
                copy.start()

        @pl.when(t >= 2)
        def _():
            finish(t - 2)

        @pl.when((t >= 1) & (t < nz + 1))
        def _():
            pass_on(t - 1)

        @pl.when(t >= 3)
        def _():
            r_copy(t - 2).start()

        return 0

    lax.fori_loop(0, nz + 2, step, 0)
    z_got[block(z, row_b), :] = share[0]
    low, high = forward.end()
    low_f, up_b = low[0:1], high[0:1]
    state_f = sv[10] + sv[9] * low_f
    state_b = sv[12] + sv[11] * up_b
    sv[10] = state_f
    sv[12] = state_b
    mo_ref[...] = (sv[13] * (state_f + state_b)).astype(BF)
    base = shuffle_base(row_a, geo.rows, slots, nyc)
    for k in z_order:
        arrival(z_got.at[block(z_at(k), row_b)], sz.at[k], rz.at[k], z_peer(k)).wait_recv()
    rows = z_got[...]

    def b_copy(k):
        return wire(y_out.at[k], back.at[block(c, row_a)], sy.at[k], ry.at[k], y_peer(k))

    held = None
    for k in y_order:
        y_out[k] = picked_rows(base, lax.rem(c + k, nyc), slots, rows)
        if held is not None:
            b_copy(held).start()
        held = k
    back[block(c, row_a), :] = picked_rows(base, c, slots, rows)
    b_copy(held).start()
    for k in y_order:
        source = lax.rem(c + nyc - k, nyc)
        arrival(back.at[block(source, row_a)], sy.at[k], ry.at[k], y_peer(k)).wait_recv()
    picked = jnp.dot(pt_ref[...], back[...], preferred_element_type=F32)
    ng_ref[:, pl.ds(columns(j), w)] = (picked[:length] + picked[length : 2 * length]).astype(BF)

    def g_part(column, size, offset=0):
        return ng_ref.at[:, pl.ds(columns(column, offset), size)]

    gathers = [
        wire(g_part(j, w), g_part(j, w), sg.at[0], rg.at[0], (sp, right)),
        wire(g_part(j, w), g_part(j, w), sg.at[1], rg.at[1], (sp, left)),
        wire(g_part(left, hw), g_part(left, hw), sg.at[2], rg.at[2], (sp, right)),
        wire(g_part(right, hw, hw), g_part(right, hw, hw), sg.at[3], rg.at[3], (sp, left)),
    ]
    gathers[0].start()
    gathers[1].start()
    arrival(g_part(left, w), sg.at[0], rg.at[0], (sp, left)).wait_recv()
    gathers[2].start()
    arrival(g_part(right, w), sg.at[1], rg.at[1], (sp, right)).wait_recv()
    gathers[3].start()
    arrival(g_part(opposite, hw), sg.at[2], rg.at[2], (sp, left)).wait_recv()
    arrival(g_part(opposite, hw, hw), sg.at[3], rg.at[3], (sp, right)).wait_recv()

    x32 = x_ref[...].astype(F32)
    inv_rms = lax.rsqrt(jnp.mean(x32 * x32, axis=1, keepdims=True) + EPS)
    normed = x32 * inv_rms
    ng = ng_ref[...].astype(F32)
    mean = jnp.mean(ng * normed, axis=1, keepdims=True)
    mgb_ref[...] = (cot_ref[...].astype(F32) + inv_rms * (ng - normed * mean)).astype(BF)
    go = lax.dot_general(mgb_ref[...], mo_ref[...], (((0,), (0,)), ((), ())), preferred_element_type=F32)
    go_ref[...] = go.astype(BF).reshape(go_ref.shape)
    out_grad = jnp.dot(mgb_ref[...], op_ref[...], preferred_element_type=F32)
    carried = out_grad * sv[13]
    cum_bf, after_b = scan_rows(sv[7], sv[7] * carried, False)
    y, core = lax.div(c, 2), lax.rem(c, 2)
    partner = (z * nyc + y * 2 + (1 - core), j)
    yy_order = nearest_first(ny)

    def yy_peer(k):
        return (z * nyc + lax.rem(y + k, ny) * 2 + core, j)

    sent.append(send(go_ref.at[:, :, 1 - core], r1, s1, q1, partner))
    cum_fr, after_f = scan_rows(sv[3], sv[3] * carried, True)
    fill(car.at[1], (zero, after_b[last:], zero, after_f[0:1]))
    states = sv[10] + sv[12]
    bg_ref[...] = (out_grad * states * sv[14]).astype(BF)
    sent += backward.start()
    arrival(r1, s1, q1, partner).wait_recv()
    for k in yy_order + [0]:
        at = lax.rem(y + k, ny)
        half[k] = (go_ref[:, at, core].astype(F32) + r1[:, at].astype(F32)).astype(BF)
    sent += backward.middle()
    for k in yy_order:
        sent.append(send(half.at[k], r2.at[k], s2.at[k], q2.at[k], yy_peer(k)))
    row = lax.broadcasted_iota(jnp.int32, ci_ref.shape, 0)

    def from_before(item, carry):
        return jnp.where(row == 0, carry, pltpu.roll(item, 1, 0))

    def from_after(item, carry):
        return jnp.where(row == last, carry, pltpu.roll(item, length - 1, 0))

    others = (from_before(sv[10], low_f), from_after(sv[12], up_b))
    low, high = backward.end()
    low_b, up_f = low[1:2], high[1:2]
    after_b = after_b + cum_bf * low_b
    after_f = after_f + cum_fr * up_f
    adjoints = (carried + from_after(after_f, up_f), carried + from_before(after_b, low_b))
    conv = sv[0]
    conv_grad = jnp.zeros(ci_ref.shape, F32)
    for d in range(2):
        recur, inputs, coef, root = [sv[1 + 4 * d + n] for n in range(4)]
        adjoint = adjoints[d]
        log_grad = adjoint * others[d] * coef - adjoint * (inputs * conv) * (coef * coef) / root
        recur_grad = log_grad * (-DECAY_SCALE * rate[d : d + 1, :]) * recur * (1.0 - recur)
        input_grad = adjoint * root * conv * inputs * (1.0 - inputs)
        conv_grad = conv_grad + adjoint * root * inputs
        conv_grad = conv_grad + split_dot(recur_grad, maps_ref[2 * d], ((1,), (1,)))
        conv_grad = conv_grad + split_dot(input_grad, maps_ref[2 * d + 1], ((1,), (1,)))
    cgb_ref[...] = conv_grad.astype(BF)
    big[EDGE : EDGE + length] = conv_grad
    inner = jnp.zeros((length - 2 * EDGE, ci_ref.shape[1]), F32)
    for o in range(4):
        inner = inner + big[2 * EDGE + 2 - o : 2 + length - o] * taps[o : o + 1, :]
    ig_ref[EDGE : length - EDGE] = inner.astype(BF)
    sent.append(send(cgb_ref.at[pl.ds(length - EDGE, EDGE)], halo.at[pl.ds(0, EDGE)], su.at[0], ru.at[0], (after, j)))
    sent.append(send(cgb_ref.at[pl.ds(0, EDGE)], halo.at[pl.ds(EDGE, EDGE)], su.at[1], ru.at[1], (ahead, j)))
    for k in yy_order:
        arrival(r2.at[k], s2.at[k], q2.at[k], yy_peer(k)).wait_recv()
    for k in z_order + [0]:
        at = z_at(k)
        summed = half[0, at].astype(F32)
        for m in yy_order:
            summed = summed + r2[m, at].astype(F32)
        quarter[k] = summed.astype(BF)
    for k in z_order:
        sent.append(send(quarter.at[k], r3.at[k], s3.at[k], q3.at[k], z_peer(k)))
    for e in range(2):
        arrival(halo.at[pl.ds(e * EDGE, EDGE)], su.at[e], ru.at[e], (after, j)).wait_recv()
    big[0:EDGE] = halo[0:EDGE].astype(F32) * has_low
    big[EDGE + length :] = halo[EDGE:].astype(F32) * has_high
    for start in (0, length - EDGE):
        grad = jnp.zeros((EDGE, ci_ref.shape[1]), F32)
        for o in range(4):
            at = EDGE + 2 - o + start
            grad = grad + big[at : at + EDGE] * taps[o : o + 1, :]
        ig_ref[start : start + EDGE] = grad.astype(BF)
    result = quarter[0].astype(F32)
    for k in z_order:
        arrival(r3.at[k], s3.at[k], q3.at[k], z_peer(k)).wait_recv()
        result = result + r3[k].astype(F32)
    out_ref[...] = result

    def drain(i, _):
        for h in range(2):
            for kind in range(4):
                x_copy(h, i, kind).wait_send()
        for kind in range(6):
            s_copy(i, kind).wait_send()
        for copy in stores(i):
            copy.wait()
        return 0

    lax.fori_loop(0, nz, drain, 0)
    for k in y_order:
        y_copy(0, k).wait_send()
        y_copy(1, k).wait_send()
        b_copy(k).wait_send()
    for i in range(1, nz):
        r_copy(i).wait_send()
        z_copy(0, z_order[i - 1]).wait_send()
        z_copy(1, z_order[i - 1]).wait_send()
    for copy in edges + gathers + sent:
        copy.wait_send()


def weights_kernel(xin_ref, xsc_ref, hid_ref, gg_ref, ug_ref, a_ref, b_ref, c_ref, gate_ref, up_ref, down_ref, ao_ref, bo_ref, co_ref, ht):
    @pl.when(pl.program_id(0) == 0)
    def _():
        ht[...] = hid_ref[...].T
        ao_ref[...] = a_ref[...]
        bo_ref[...] = b_ref[...]
        co_ref[...] = c_ref[...]

    xt = xin_ref[...].T
    gate_ref[...] = jnp.dot(xt, gg_ref[...], preferred_element_type=F32)
    up_ref[...] = jnp.dot(xt, ug_ref[...], preferred_element_type=F32)
    down_ref[...] = jnp.dot(ht[...], xsc_ref[...], preferred_element_type=F32)


def shards(
    cotangent,
    saved_input,
    routes,
    route_weight,
    gate_proj,
    up_proj,
    down_proj,
    out_proj,
    conv_input,
    gate_branch,
    conv_taps,
    recur_map,
    input_map,
    decay_param,
    decay_shift,
):
    length, width = cotangent.shape
    n_sp = lax.axis_size("sp")
    geo = Geometry(n_sp, 4 * length // n_sp)
    nz, ny, nyc, rows = geo.nz, geo.ny, geo.nyc, geo.rows
    w = width // 4
    hidden_units = gate_proj.shape[2]
    channels = conv_input.shape[1]
    part = width // n_sp
    own = (length, channels)
    half = (nz, 2, geo.row_b, w // 2)
    carry = (8, channels)
    shape = jax.ShapeDtypeStruct
    wide, narrow = shape((rows, width), BF), shape((rows, hidden_units), BF)
    anywhere = pl.BlockSpec(memory_space=pl.ANY)

    def vmem(dims, kind=BF):
        return pltpu.VMEM(dims, kind)

    rows_input, rows_scaled, hidden, gate_grad, up_grad, *small = pl.pallas_call(
        functools.partial(layer_kernel, geo),
        out_shape=(wide, wide, narrow, narrow, narrow, shape((part, channels), F32), shape(own, BF), shape(own, BF)),
        in_specs=[VM] * 11 + [anywhere] * 4,
        out_specs=(anywhere,) * 5 + (VM,) * 3,
        scratch_shapes=[
            vmem((rows, 2 * w)),
            vmem((2 * length, rows)),
            vmem(gate_proj.shape[1:]),
            vmem(up_proj.shape[1:]),
            vmem(down_proj.shape[1:]),
            vmem(out_proj.shape),
            vmem((rows, width)),
            vmem((rows, width)),
            vmem((rows, hidden_units)),
            vmem((rows, hidden_units)),
            vmem((rows, hidden_units)),
            vmem((2 * EDGE, channels)),
            vmem((length, width)),
            vmem((rows, 2 * w)),
            vmem((2, nz, geo.row_b, w)),
            vmem((nz, geo.row_b, width)),
            vmem(half),
            vmem(half),
            vmem(half),
            vmem(half),
            vmem((nz, geo.row_b, w)),
            vmem((rows, w)),
            vmem((nyc, geo.row_a, w)),
            vmem((rows, w)),
            vmem((SAVED, *own), F32),
            vmem((4, channels, channels)),
            vmem((length + 2 * EDGE, channels), F32),
            vmem(own),
            vmem((length, width)),
            vmem((nz, ny, 2, part, channels)),
            vmem(own),
            vmem((ny, nz, part, channels)),
            vmem((nz, part, channels)),
            vmem((nz, ny, part, channels)),
            vmem((ny, nz, part, channels)),
            vmem((nz, part, channels)),
            vmem((2 * EDGE, channels)),
            vmem((2, *carry), F32),
            vmem((2, nyc, *carry), F32),
            vmem((2, nz, *carry), F32),
            vmem((2, *carry), F32),
            DMA((4,)),
            DMA((nz, 5)),
            DMA((2, nyc)),
            DMA((2, nyc)),
            DMA((2, nz)),
            DMA((2, nz)),
            DMA((2, nz, 4)),
            DMA((2, nz, 4)),
            DMA((2,)),
            DMA((2,)),
            DMA((nz, 6)),
            DMA((nz, 6)),
            DMA((nz,)),
            DMA((nz,)),
            DMA((nyc,)),
            DMA((nyc,)),
            DMA((4,)),
            DMA((4,)),
            DMA,
            DMA,
            DMA((ny,)),
            DMA((ny,)),
            DMA((nz,)),
            DMA((nz,)),
            DMA((2,)),
            DMA((2,)),
            DMA((2, nyc)),
            DMA((2, nyc)),
            DMA((2, nz)),
            DMA((2, nz)),
        ],
        compiler_params=pltpu.CompilerParams(
            collective_id=1, has_side_effects=True, vmem_limit_bytes=60 * 2**20
        ),
    )(
        cotangent,
        saved_input,
        routes.T,
        route_weight.T,
        conv_input,
        gate_branch,
        conv_taps,
        recur_map.reshape(2, channels, 64),
        input_map.reshape(2, channels, 64),
        decay_param,
        decay_shift,
        gate_proj[0],
        up_proj[0],
        down_proj[0],
        out_proj,
    )
    tile = min(256, width)
    across_tile = pl.BlockSpec((rows, tile), lambda i: (0, i))
    down_tile = pl.BlockSpec((tile, hidden_units), lambda i: (i, 0))

    def whole(a):
        return pl.BlockSpec(a.shape, lambda i: (0, 0))

    grad_gate, grad_up, grad_down, grad_out, input_grad, branch_grad = pl.pallas_call(
        weights_kernel,
        grid=(width // tile,),
        out_shape=(
            shape((width, hidden_units), F32),
            shape((width, hidden_units), F32),
            shape((hidden_units, width), F32),
            *(shape(a.shape, a.dtype) for a in small),
        ),
        in_specs=[across_tile, across_tile, *(whole(a) for a in (hidden, gate_grad, up_grad, *small))],
        out_specs=(
            down_tile,
            down_tile,
            pl.BlockSpec((hidden_units, tile), lambda i: (0, i)),
            *(whole(a) for a in small),
        ),
        scratch_shapes=[vmem((hidden_units, rows))],
        compiler_params=pltpu.CompilerParams(vmem_limit_bytes=60 * 2**20),
    )(rows_input, rows_scaled, hidden, gate_grad, up_grad, *small)
    return (grad_gate[None], grad_up[None], grad_down[None], grad_out, input_grad, branch_grad)


def solution(mesh):
    in_specs = (
        P("sp", None),
        P("sp", None),
        P("sp", None),
        P("sp", None),
        P("sp", None, "tp"),
        P("sp", None, "tp"),
        P("sp", "tp", None),
        P(None, "tp"),
        P("sp", "tp"),
        P("sp", "tp"),
        P(None, "tp"),
        P(None, "tp", None, None),
        P(None, "tp", None, None),
        P(None, "tp"),
        P(None, "sp", "tp"),
    )
    out_specs = (
        P("sp", None, "tp"),
        P("sp", None, "tp"),
        P("sp", "tp", None),
        P("sp", "tp"),
        P("sp", "tp"),
        P("sp", "tp"),
    )
    return jax.shard_map(shards, mesh=mesh, in_specs=in_specs, out_specs=out_specs, check_vma=False)
```
